32 devices in a mesh: grp: 2 (over x), tp: 16 (over z, y, core).
Axes of the slice: x: 2, y: 2, z: 4, core: 2. Of those that a mesh axis runs over, the one named last changes fastest.
Arguments:
- stream_in: bfloat16 [64, 4, 4096], P('grp'), parts along dimension 0, may hold values from -6 to 6
- state_in: float32 [2, 64, 8, 256, 256], P(None, 'grp', None, 'tp'), parts along dimension 1, may hold values from -0.8 to 0.8
- norm_gain: bfloat16 [2, 4096], replicated, may hold values from 0.099609375 to 1.8984375
- query_weight: bfloat16 [2, 4096, 2048], P(None, None, 'tp'), may hold values from -0.09375 to 0.09375
- key_weight: bfloat16 [2, 4096, 2048], P(None, None, 'tp'), may hold values from -0.09375 to 0.09375
- value_weight: bfloat16 [2, 4096, 8, 256], P(None, None, None, 'tp'), as said below
- gate_weight: bfloat16 [2, 4096, 8, 256], P(None, None, None, 'tp'), may hold values from -0.09375 to 0.09375
- group_gain: bfloat16 [2, 8, 256], P(None, None, 'tp'), may hold values from 0.099609375 to 1.8984375
- output_weight: bfloat16 [2, 8, 256, 4096], P(None, None, 'tp'), may hold values from -0.375 to 0.375
Outputs:
- stream_out: bfloat16 [64, 4, 4096], P('grp', None, 'tp'), parts along dimension 0
- state_out: float32 [2, 64, 8, 256, 256], P(None, 'grp', None, 'tp'), parts along dimension 1
The draws below stay inside these ranges and needn't reach their ends.
There are 2 independent parts, one for each index of `grp`. The reference program is written for one: setup_inputs(seed, part) draws one part's arguments, and reference() takes and returns one part's arrays. A program takes and returns all parts, laid end to end along the dimension named above; an argument that names none is the same for every part. Nothing has to cross between parts.
Inputs may be any that keep to these rules, and one draw needn't show every extreme that they name: `value_weight`: real values; column scales of the value projection differ.
All inputs are finite; a program needn't handle non-finite values.
Results may differ from the reference program's by a relative error of at most 0.024.
Values may be sent and summed in bfloat16 or wider, within the bound.
A program may use at most 64 MiB of HBM per device.

```python
import jax
import jax.numpy as jnp
from jax import lax

D = 4096
HEADS = 8
HEAD_DIM = 256
SEQS = 32
NEW_TOK = 4
PAST = 1024
LAYERS = 2


def draw_value_weight(key, part):
    first_key, second_key = jax.random.split(jax.random.fold_in(key, 17))
    base = jax.random.normal(first_key, (LAYERS, D, HEADS, HEAD_DIM), jnp.float32) * D ** (-0.5)
    ramp = jnp.arange(HEAD_DIM, dtype=jnp.float32) / (HEAD_DIM - 1)
    rough = jax.random.uniform(second_key, (LAYERS, 1, HEADS, HEAD_DIM), jnp.float32, -0.4, 0.4)
    scales = jnp.power(3.0, ramp) * jnp.exp(rough)
    return (base * scales).astype(jnp.bfloat16)


def strengthened(drawn, key, source, target, shards_of, factor):
    def block_of(dim):
        return (jnp.arange(drawn.shape[dim]) // (drawn.shape[dim] // shards_of)).reshape((-1,) + (1,) * (drawn.ndim - 1 - dim))

    near = jax.random.permutation(key, shards_of)[block_of(target)]
    far = (block_of(target) + shards_of // 2) % shards_of
    return jnp.where((block_of(source) == near) | (block_of(source) == far), factor * drawn, drawn)


def level_of(own_key, dims, cuts, smallest, largest):
    loudness, own = 1.0, jax.random.fold_in(own_key, 6)
    for position, blocks in cuts:
        steps = jnp.exp(jax.random.uniform(jax.random.fold_in(own, position), (blocks,), jnp.float32, smallest / len(cuts), largest / len(cuts)))
        loudness = loudness * jnp.repeat(steps, dims[position] // blocks).reshape([-1 if axis == position else 1 for axis in range(len(dims))])
    return loudness


def bell_draw(own_key, shape, scale, most, pieces=(), held_as=jnp.bfloat16):
    factor_of = level_of(own_key, shape, pieces, -0.22, 0.18) if pieces else 1.0
    drawn = jax.random.normal(own_key, shape, jnp.float32) * scale * factor_of
    return jnp.minimum(jnp.maximum(drawn, -most), most).astype(held_as)


def heavy_noise(rng, dims, spread, most, shards, heavy, kind=jnp.bfloat16):
    array = spread * jax.random.normal(rng, dims, jnp.float32)
    if shards:
        array = array * level_of(rng, dims, shards, -0.22, 0.18)
    return jnp.clip(strengthened(array, jax.random.fold_in(rng, 3), *heavy), -most, most).astype(kind)


def setup_inputs(seed: int = 0, part: int = 0) -> dict:
    key_of = jax.random.split(jax.random.key(seed), 10)
    part_splits = jax.random.split(jax.random.fold_in(key_of[9], part), 10)
    return {
        "stream_in": bell_draw(part_splits[0], (SEQS, NEW_TOK, D), 1.0, 6.0),
        "state_in": bell_draw(part_splits[1], (LAYERS, SEQS, HEADS, HEAD_DIM, HEAD_DIM), 0.1, 0.8, ((3, 16),), jnp.float32),
        "norm_gain": jnp.clip(1.0 + 0.18 * jax.random.normal(key_of[2], (LAYERS, D), jnp.float32), 0.099609375, 1.8984375).astype(jnp.bfloat16),
        "query_weight": bell_draw(key_of[3], (LAYERS, D, HEADS * HEAD_DIM), D ** -0.5, 0.09375, ((2, 16),)),
        "key_weight": bell_draw(key_of[4], (LAYERS, D, HEADS * HEAD_DIM), D ** -0.5, 0.09375, ((2, 16),)),
        "value_weight": draw_value_weight(jax.random.fold_in(key_of[9], 71), part),
        "gate_weight": bell_draw(key_of[6], (LAYERS, D, HEADS, HEAD_DIM), D ** -0.5, 0.09375, ((3, 16),)),
        "group_gain": jnp.clip(1.0 + 0.18 * jax.random.normal(key_of[7], (LAYERS, HEADS, HEAD_DIM), jnp.float32), 0.099609375, 1.8984375).astype(jnp.bfloat16),
        "output_weight": heavy_noise(key_of[8], (LAYERS, HEADS, HEAD_DIM, D), (HEADS * HEAD_DIM // 4) ** -0.5, 0.375, ((2, 16),), (2, 3, 16, 2.0)),
    }


EPS_RMS = 1e-06
EPS_GROUP = 1e-05
ROTARY_BASE = 10000.0

def log_decays(count):
    return jnp.log(1.0 - jnp.power(2.0, -5.0 - jnp.arange(count, dtype=jnp.float32)))

def decay_tables(log_gamma, count):
    steps = jnp.arange(count, dtype=jnp.float32)
    gap = steps[:, None] - steps[None, :]
    intra = jnp.where(gap[None] >= 0, jnp.exp(log_gamma[:, None, None] * jnp.maximum(gap, 0.0)[None]), 0.0)
    q_decay = jnp.exp(log_gamma[None, :] * (steps[:, None] + 1.0))
    k_decay = jnp.exp(log_gamma[None, :] * (count - 1.0 - steps[:, None]))
    block_decay = jnp.exp(log_gamma * count)
    return (intra, q_decay, k_decay, block_decay)

def rotate(values, offset):
    half_dim = values.shape[-1] // 2
    freqs = jnp.power(ROTARY_BASE, -jnp.arange(half_dim, dtype=jnp.float32) * (2.0 / values.shape[-1]))
    places = (offset + jnp.arange(values.shape[1])).astype(jnp.float32)
    angles = places[:, None] * freqs[None, :]
    cosine = jnp.cos(angles)[None, :, None, :]
    sine = jnp.sin(angles)[None, :, None, :]
    first = values[..., :half_dim]
    second = values[..., half_dim:]
    return jnp.concatenate([first * cosine - second * sine, second * cosine + first * sine], axis=-1)

def reference(stream_in, state_in, norm_gain, query_weight, key_weight, value_weight, gate_weight, group_gain, output_weight):
    seqs, new_tok, width = stream_in.shape
    heads, head_dim = (value_weight.shape[2], value_weight.shape[3])
    log_gamma = log_decays(heads)
    intra, q_decay, k_decay, block_decay = decay_tables(log_gamma, new_tok)
    highest = lax.Precision.HIGHEST
    stream = stream_in
    new_states = []
    for layer_no in range(state_in.shape[0]):
        stream_f = stream.astype(jnp.float32)
        normed = stream_f * lax.rsqrt(lax.optimization_barrier(jnp.mean(stream_f * stream_f, axis=-1, keepdims=True)) + EPS_RMS)
        normed = (normed * norm_gain[layer_no].astype(jnp.float32)).astype(jnp.bfloat16)
        flat = normed.reshape(seqs * new_tok, width)

        def project(weight):
            result = jnp.dot(flat, weight.reshape(width, heads * head_dim), preferred_element_type=jnp.float32)
            result = lax.optimization_barrier(result.astype(jnp.bfloat16))
            return result.astype(jnp.float32).reshape(seqs, new_tok, heads, head_dim)
        queries = project(query_weight[layer_no])
        key_rows = project(key_weight[layer_no])
        values_f = project(value_weight[layer_no])
        gates_f = project(gate_weight[layer_no])
        rot_q = rotate(queries, PAST)
        rot_k = rotate(key_rows, PAST) * head_dim ** (-0.5)
        scores = jnp.einsum('bthd,bshd->bhts', rot_q, rot_k, precision=highest) * intra[None]
        inner = jnp.einsum('bhts,bshe->bthe', scores, values_f, precision=highest)
        state = state_in[layer_no]
        carried = jnp.einsum('bthd,bhed->bthe', rot_q, state, precision=highest) * q_decay[None, :, :, None]
        mixed = inner + carried
        new_state = state * block_decay[None, :, None, None] + jnp.einsum('bthe,bthd->bhed', values_f, rot_k * k_decay[None, :, :, None], precision=highest)
        mean_o = lax.optimization_barrier(jnp.mean(mixed, axis=-1, keepdims=True))
        var_o = lax.optimization_barrier(jnp.mean(jnp.square(mixed - mean_o), axis=-1, keepdims=True))
        normal = (mixed - mean_o) * lax.rsqrt(var_o + EPS_GROUP) * group_gain[layer_no].astype(jnp.float32)[None, None]
        gated = (jax.nn.silu(gates_f) * normal).astype(jnp.bfloat16)
        branch = jnp.dot(gated.reshape(seqs * new_tok, heads * head_dim), output_weight[layer_no].reshape(heads * head_dim, width), preferred_element_type=jnp.float32)
        stream = (stream.astype(jnp.float32) + branch.reshape(seqs, new_tok, width)).astype(jnp.bfloat16)
        new_states.append(new_state)
    return (stream, jnp.stack(new_states))
```

```python
import functools

import jax
import jax.numpy as jnp
import numpy as np
from jax import lax
from jax.experimental import pallas as pl
from jax.experimental.pallas import tpu as pltpu
from jax.sharding import PartitionSpec as P

HEAD_DIM = 256
PAST = 1024


EPS_RMS = 1e-06
EPS_GROUP = 1e-05
ROTARY_BASE = 10000.0


def log_decays(count):
    return jnp.log(1.0 - jnp.power(2.0, -5.0 - jnp.arange(count, dtype=jnp.float32)))


def decay_tables(log_gamma, count):
    steps = jnp.arange(count, dtype=jnp.float32)
    gap = steps[:, None] - steps[None, :]
    intra = jnp.where(
        gap[None] >= 0, jnp.exp(log_gamma[:, None, None] * jnp.maximum(gap, 0.0)[None]), 0.0
    )
    q_decay = jnp.exp(log_gamma[None, :] * (steps[:, None] + 1.0))
    k_decay = jnp.exp(log_gamma[None, :] * (count - 1.0 - steps[:, None]))
    block_decay = jnp.exp(log_gamma * count)
    return (intra, q_decay, k_decay, block_decay)


def rotate(values, offset):
    half_dim = values.shape[-1] // 2
    freqs = jnp.power(
        ROTARY_BASE, -jnp.arange(half_dim, dtype=jnp.float32) * (2.0 / values.shape[-1])
    )
    places = (offset + jnp.arange(values.shape[1])).astype(jnp.float32)
    angles = places[:, None] * freqs[None, :]
    cosine = jnp.cos(angles)[None, :, None, :]
    sine = jnp.sin(angles)[None, :, None, :]
    first = values[..., :half_dim]
    second = values[..., half_dim:]
    return jnp.concatenate(
        [first * cosine - second * sine, second * cosine + first * sine], axis=-1
    )


def plain_local(
    stream_in,
    state_in,
    norm_gain,
    query_weight,
    key_weight,
    value_weight,
    gate_weight,
    group_gain,
    output_weight,
):
    seqs, new_tok, width = stream_in.shape
    heads, local_dim = (value_weight.shape[2], value_weight.shape[3])
    head_dim = HEAD_DIM
    log_gamma = log_decays(heads)
    intra, q_decay, k_decay, block_decay = decay_tables(log_gamma, new_tok)
    highest = lax.Precision.HIGHEST
    share_cols = width // lax.axis_size("tp")
    col_start = lax.axis_index("tp") * share_cols
    layers = state_in.shape[0]
    stream = stream_in
    stream_share = stream_in
    new_states = []
    for layer_no in range(layers):
        stream_f = stream.astype(jnp.float32)
        normed = stream_f * lax.rsqrt(
            jnp.mean(stream_f * stream_f, axis=-1, keepdims=True) + EPS_RMS
        )
        normed = (normed * norm_gain[layer_no].astype(jnp.float32)).astype(jnp.bfloat16)
        flat = normed.reshape(seqs * new_tok, width)
        query_part = jnp.dot(flat, query_weight[layer_no], preferred_element_type=jnp.float32)
        query_part = query_part.astype(jnp.bfloat16).reshape(seqs, new_tok, -1)
        key_part = jnp.dot(flat, key_weight[layer_no], preferred_element_type=jnp.float32)
        key_part = key_part.astype(jnp.bfloat16).reshape(seqs, new_tok, -1)

        def project_local(weight):
            result = jnp.dot(
                flat, weight.reshape(width, heads * local_dim), preferred_element_type=jnp.float32
            )
            result = lax.optimization_barrier(result.astype(jnp.bfloat16))
            return result.astype(jnp.float32).reshape(seqs, new_tok, heads, local_dim)

        values_f = project_local(value_weight[layer_no])
        gates_f = project_local(gate_weight[layer_no])
        queries, key_rows = (
            lax.all_gather(query_part, "tp", axis=2, tiled=True),
            lax.all_gather(key_part, "tp", axis=2, tiled=True),
        )
        queries = queries.astype(jnp.float32).reshape(seqs, new_tok, heads, head_dim)
        key_rows = key_rows.astype(jnp.float32).reshape(seqs, new_tok, heads, head_dim)
        rot_q = rotate(queries, PAST)
        rot_k = rotate(key_rows, PAST) * head_dim ** (-0.5)
        scores = jnp.einsum("bthd,bshd->bhts", rot_q, rot_k, precision=highest) * intra[None]
        inner = jnp.einsum("bhts,bshe->bthe", scores, values_f, precision=highest)
        state = state_in[layer_no]
        carried = (
            jnp.einsum("bthd,bhed->bthe", rot_q, state, precision=highest)
            * q_decay[None, :, :, None]
        )
        mixed = inner + carried
        new_state = state * block_decay[None, :, None, None] + jnp.einsum(
            "bthe,bthd->bhed", values_f, rot_k * k_decay[None, :, :, None], precision=highest
        )
        new_states.append(new_state)
        totals, squares = lax.psum((jnp.sum(mixed, axis=-1), jnp.sum(mixed * mixed, axis=-1)), "tp")
        mean_o = (totals / head_dim)[..., None]
        var_o = (squares / head_dim)[..., None] - mean_o * mean_o
        normal = (
            (mixed - mean_o)
            * lax.rsqrt(var_o + EPS_GROUP)
            * group_gain[layer_no].astype(jnp.float32)[None, None]
        )
        gated = (jax.nn.silu(gates_f) * normal).astype(jnp.bfloat16)
        partial_out = jnp.dot(
            gated.reshape(seqs * new_tok, heads * local_dim),
            output_weight[layer_no].reshape(heads * local_dim, width),
            preferred_element_type=jnp.float32,
        ).reshape(seqs, new_tok, width)
        share_out = lax.psum_scatter(partial_out, "tp", scatter_dimension=2, tiled=True)
        own_cols = lax.dynamic_slice_in_dim(stream, col_start, share_cols, 2)
        stream_share = (own_cols.astype(jnp.float32) + share_out).astype(jnp.bfloat16)
        if layer_no + 1 < layers:
            stream = lax.all_gather(stream_share, "tp", axis=2, tiled=True)
    result = stream_share
    return (result, jnp.stack(new_states))


F32 = jnp.float32
BF16 = jnp.bfloat16
XPARTS = 4
scope = jax.named_scope


def nt_dot(a, b, precision=None):
    return lax.dot_general(
        a, b, (((1,), (1,)), ((), ())), preferred_element_type=F32, precision=precision
    )


def log2(value):
    return int(value).bit_length() - 1


def rotary_tables(heads, new_tok, head_dim):
    half = head_dim // 2
    freqs = np.power(
        np.float32(ROTARY_BASE), -np.arange(half, dtype=np.float32) * np.float32(2.0 / head_dim)
    ).astype(np.float32)
    tok = np.arange(8) % new_tok
    places = (PAST + tok).astype(np.float32)
    angles = (places[:, None] * freqs[None, :]).astype(np.float32).astype(np.float64)
    gamma = 1.0 - np.power(2.0, -5.0 - np.arange(heads))
    grow = np.power(gamma[:, None], tok[None, :] + 1.0)[:, :, None]
    shrink = head_dim ** (-0.5) / grow
    cosine, sine = np.cos(angles)[None], np.sin(angles)[None]
    block = np.broadcast_to(np.power(gamma, new_tok)[:, None, None], (heads, 8, half))
    return np.stack(
        [cosine * grow, sine * grow, cosine * shrink, sine * shrink, block]
    ).astype(np.float32)


def kernel(
    n, head_dim,
    x_hbm, st_hbm, ng_hbm, qw_hbm, kw_hbm, vw_hbm, gw_hbm, gg_hbm, ow_hbm, tab_hbm,
    y_ref, stv,
    ng_ref, gg_ref, tab_ref, xr, xs, nv, wqk, wvg, wo, qkg, kh, vts, sb, pbs, pbr, yss, ysr, rss, rsr, mkc, mks, fold, sqa, qka,
    lsem, ag_s, st_s, rs_s, aq_r, ax_r, st_r, pb_r, ys_r, rs_r,
):
    layers, seqs, heads, e_dim, _ = st_hbm.shape
    tok = x_hbm.shape[1]
    width = x_hbm.shape[2]
    rows = seqs * tok
    share = width // n
    cols = qw_hbm.shape[2]
    he = heads * e_dim
    half = head_dim // 2
    nc = n // 2
    me = lax.axis_index("tp")
    core = lax.rem(me, 2)
    chip = lax.div(me, 2)
    partner = chip * 2 + 1 - core

    nz = nc // 2
    yy = lax.rem(chip, 2)
    zz = lax.div(chip, 2)

    def chip_at(o, y):
        z, bit = zz, 1
        while bit < nz:
            if o & bit:
                z = z + bit - 2 * bit * lax.rem(lax.div(z, bit), 2)
            bit = 2 * bit
        return z * 2 + y

    def at_z(o, y, c):
        return chip_at(o, y) * 2 + c

    facing = at_z(0, 1 - yy, core)
    far = list(range(2, nz)) + [1]
    near = [1] + list(range(nz - 1, 1, -1))

    def remote(src, dst, ssem, rsem, device):
        return pltpu.make_async_remote_copy(
            src_ref=src, dst_ref=dst, send_sem=ssem, recv_sem=rsem,
            device_id={"tp": device}, device_id_type=pl.DeviceIdType.MESH,
        )

    loads = {}
    count = 0

    def load(name, src, dst):
        nonlocal count
        loads[name] = pltpu.make_async_copy(src, dst, lsem.at[count])
        loads[name].start()
        count += 1

    wide = width // XPARTS
    for j in range(XPARTS):
        at = pl.ds(j * wide, wide)
        load(("x", j), x_hbm.at[:, :, at], xr.at[:, :, at])
    load("ng", ng_hbm, ng_ref)

    barrier = pltpu.get_barrier_semaphore()
    for o in range(1, n):
        pl.semaphore_signal(
            barrier, inc=1, device_id={"tp": lax.rem(me + o, n)},
            device_id_type=pl.DeviceIdType.MESH,
        )

    for l in range(layers):
        load(("q", l), qw_hbm.at[l], wqk.at[l, :, pl.ds(0, cols)])
        load(("k", l), kw_hbm.at[l], wqk.at[l, :, pl.ds(cols, cols)])
        load(("v", l), vw_hbm.at[l], wvg.at[l, pl.ds(0, he)])
        load(("g", l), gw_hbm.at[l], wvg.at[l, pl.ds(he, he)])
        load(("s", l), st_hbm.at[l], stv.at[l])
        load(("o", l), ow_hbm.at[l], wo.at[l])
        if l == 0:
            load("tab", tab_hbm, tab_ref)
            load("gg", gg_hbm, gg_ref)

    be = seqs * e_dim

    def iota(shape, dim, shift=0):
        return jnp.right_shift(lax.broadcasted_iota(jnp.int32, shape, dim), shift)

    te, tt = log2(e_dim), log2(tok)
    low = e_dim - 1
    causal = (
        (iota((rows, rows), 0, tt) == iota((rows, rows), 1, tt))
        & (iota((rows, rows), 0) >= iota((rows, rows), 1))
    ).astype(F32)
    heads_of = (iota((heads, he), 0) == iota((heads, he), 1, te)).astype(F32)
    place = (
        iota((e_dim, he), 0) == jnp.bitwise_and(iota((e_dim, he), 1), low)
    ).astype(F32)
    highest = lax.Precision.HIGHEST

    def make_masks():
        mkc[...] = (iota((rows, be), 0, tt) == iota((rows, be), 1, te)).astype(F32).astype(BF16)
        mks[...] = (iota((be, rows), 0, te) == iota((be, rows), 1, tt)).astype(F32).astype(BF16)
        fold[...] = (
            jnp.bitwise_and(iota((be, he), 0), low) == jnp.bitwise_and(iota((be, he), 1), low)
        ).astype(F32).astype(BF16)

    drains = []

    def gather(name, buf, recv, send, after_start, on_chip):
        own = buf.at[me]

        def push(slot, k, device):
            remote(slot, slot, send, recv.at[k], device).start()

        def arrive(slot, k):
            remote(slot, slot, send, recv.at[k], partner).wait_recv()

        def from_z(o):
            with scope(f"{name}z{o}"):
                slot = buf.at[at_z(o, yy, core)]
                arrive(slot, o)
                push(slot, nz + o, facing)
                push(slot, nc + o, partner)

        def from_y(o):
            with scope(f"{name}y{o}"):
                slot = buf.at[at_z(o, 1 - yy, core)]
                arrive(slot, nz + o)
                push(slot, nc + nz + o, partner)

        def done(o, side):
            y = 1 - yy if side else yy
            with scope(f"{name}d{side}{o}"):
                arrive(buf.at[at_z(o, y, 1 - core)], nc + nz * side + o)
            with scope(f"{name}c{side}{o}"):
                on_chip(chip_at(o, y))

        push(own, nz, facing)
        for o in near:
            push(own, o, at_z(o, yy, core))
        push(own, nc, partner)
        with scope(name + "after"):
            after_start()
        done(0, 0)
        from_z(near[0])
        from_y(0)
        for o in near[1:]:
            from_z(o)
        done(near[0], 0)
        done(0, 1)
        from_y(near[0])
        for a, b in zip(near[1:], near[:-1]):
            done(a, 0)
            from_y(a)
            done(b, 1)
        done(near[-1], 1)
        drains.append((buf.at[pl.ds(0, n - 1)], send))

    def spread(table):
        return jnp.broadcast_to(table[None], (rows // 8, 8, half)).reshape(rows, half)

    def absorb(l, j, count):
        at = pl.ds(pl.multiple_of(j * share, share), share * count)
        parts = []
        for i in range(count):
            block = xs[l, j + i].astype(F32)
            sqa[...] += block * block
            one = pl.ds(pl.multiple_of((j + i) * share, share), share)
            gain = ng_ref[l : l + 1, one].astype(F32)
            scaled = (block * gain).astype(BF16)
            nv[:, one] = scaled
            parts.append(scaled)
        both = jnp.concatenate(parts, axis=1) if count > 1 else parts[0]
        qka[...] += jnp.dot(both, wqk[l, at, :], preferred_element_type=F32)

    def clear():
        sqa[...] = jnp.zeros_like(sqa)
        qka[...] = jnp.zeros_like(qka)

    for l in range(layers):
        if l == 0:
            with scope("unpack"):
                clear()
                per = n // XPARTS
                for p in range(XPARTS):
                    loads[("x", p)].wait()
                    for j in range(p * per, (p + 1) * per):
                        piece = xr[:, :, pl.ds(j * share, share)].astype(F32)
                        xs[0, j] = piece.reshape(rows, share).astype(BF16)
            with scope("wqk"):
                loads[("q", 0)].wait()
                loads[("k", 0)].wait()
                loads["ng"].wait()
            with scope("absorb"):
                lax.fori_loop(0, n // 4, lambda i, c: (absorb(0, i * 4, 4), c)[1], 0)

        with scope(f"qk{l}"):
            scale = lax.rsqrt(jnp.sum(sqa[...], axis=1, keepdims=True) / width + EPS_RMS)
            qkg[l, me] = (qka[...] * scale).astype(BF16)
        if l == 0:
            with scope("bar"):
                pl.semaphore_wait(barrier, n - 1)

        box = {}

        def project(l=l, scale=scale, box=box):
            if l == 0:
                make_masks()
            loads[("v", l)].wait()
            loads[("g", l)].wait()
            vg = nt_dot(nv[...], wvg[l]) * scale
            box["values"] = vg[:, :he].astype(BF16)
            box["gates"] = vg[:, he:].astype(BF16).astype(F32)
            vts[...] = jnp.transpose(box["values"].astype(F32)).astype(BF16)
            loads[("s", l)].wait()
            if l == 0:
                loads["tab"].wait()
                loads["gg"].wait()
            box["mixed"] = jnp.zeros((rows, he), F32)

        def mix(h, l=l, box=box):
            qk_a = qkg[l, 2 * h].astype(F32)
            qk_b = qkg[l, 2 * h + 1].astype(F32)
            qa, ka = qk_a[:, :half], qk_a[:, half:]
            qb, kb = qk_b[:, :half], qk_b[:, half:]
            cq, sq = spread(tab_ref[0, h]), spread(tab_ref[1, h])
            ck, sk = spread(tab_ref[2, h]), spread(tab_ref[3, h])
            rq = jnp.concatenate([qa * cq - qb * sq, qb * cq + qa * sq], axis=1).astype(BF16)
            rk = jnp.concatenate([ka * ck - kb * sk, kb * ck + ka * sk], axis=1).astype(BF16)
            kh[h] = rk
            state = stv[l, :, h].reshape(be, head_dim).astype(BF16)
            scores = (nt_dot(rq, rk) * causal).astype(BF16)
            carried = nt_dot(rq, state).astype(BF16) * mkc[...]
            part = jnp.dot(scores, box["values"], preferred_element_type=F32)
            part = part + jnp.dot(carried, fold[...], preferred_element_type=F32)
            own = (iota((1, he), 1, te) == h).astype(F32)
            box["mixed"] = box["mixed"] + part * own

        gather(f"q{l}", qkg.at[l], aq_r, ag_s.at[l], project, mix)
        mixed, gates = box["mixed"], box["gates"]

        with scope(f"sums{l}"):
            sums = nt_dot(heads_of, mixed, highest)
            squares = nt_dot(heads_of, mixed * mixed, highest)
            sb[l, me] = jnp.concatenate([sums, squares], axis=1)
            for o in range(1, n):
                remote(sb.at[l, me], sb.at[l, me], st_s.at[l], st_r.at[0], lax.rem(me + o, n)).start()
            drains.append((sb.at[l, pl.ds(0, n - 1)], st_s.at[l]))

        def update(h, carry, l=l):
            at = pl.ds(pl.multiple_of(h * e_dim, e_dim), e_dim)
            tall = jnp.broadcast_to(vts[at, :][None], (seqs, e_dim, rows)).reshape(be, rows)
            fresh = jnp.dot(tall * mks[...], kh[h], preferred_element_type=F32)
            row = tab_ref[4, h][0:1, :]
            fade = jnp.concatenate([row, row], axis=1)
            state = stv[l, :, h].reshape(be, head_dim)
            stv[l, :, h] = ((state + fresh) * fade).reshape(seqs, e_dim, head_dim)
            return carry

        with scope(f"update{l}"):
            lax.fori_loop(0, heads, update, 0, unroll=True)

        with scope(f"stwait{l}"):
            others = sb.at[l, pl.ds(0, n - 1)]
            remote(others, others, st_s.at[l], st_r.at[0], partner).wait_recv()

        with scope(f"gated{l}"):
            stats = jnp.sum(sb[l], axis=0)
            mean = stats[:, :rows] / head_dim
            var = stats[:, rows:] / head_dim - mean * mean
            rstd = lax.rsqrt(var + EPS_GROUP)

            def expand(small):
                return lax.dot_general(
                    small, heads_of, (((0,), (0,)), ((), ())),
                    preferred_element_type=F32, precision=highest,
                )

            gain = jnp.dot(gg_ref[l].astype(F32), place, preferred_element_type=F32, precision=highest)
            gain = jnp.sum(gain * heads_of, axis=0, keepdims=True)
            normal = (mixed - expand(mean)) * expand(rstd) * gain
            gated = (gates / (1.0 + jnp.exp(-gates)) * normal).astype(BF16)
            loads[("o", l)].wait()

        def chunk(j, l=l, gated=gated):
            at = pl.ds(pl.multiple_of(j * share, share), share)
            return jnp.dot(gated, wo[l, :, at], preferred_element_type=F32)

        order = far + [0]
        pb_s, ys_s, rz_s = rs_s.at[l, 0], rs_s.at[l, 1], rs_s.at[l, 2]

        def offer(o, side, l=l):
            k = side * nz + o
            y = 1 - yy if side else yy
            pbs[l, k] = chunk(at_z(o, y, 1 - core)).astype(BF16)
            remote(pbs.at[l, k], pbr.at[l, k], pb_s, pb_r.at[k], partner).start()

        def paired(o, side, l=l):
            k = side * nz + o
            own = chunk(at_z(o, 1 - yy if side else yy, core))
            remote(pbs.at[l, k], pbr.at[l, k], pb_s, pb_r.at[k], partner).wait_recv()
            return own + pbr[l, k].astype(F32)

        with scope(f"rsa{l}"):
            for o in order:
                offer(o, 1)
        with scope(f"rsb{l}"):
            for o in order:
                yss[l, o] = paired(o, 1).astype(BF16)
                remote(yss.at[l, o], ysr.at[l, o], ys_s, ys_r.at[o], facing).start()
        with scope(f"rsc{l}"):
            for o in order:
                offer(o, 0)
            drains.append((pbs.at[l], pb_s))
            drains.append((yss.at[l], ys_s))
        acc = None
        for o in order:
            with scope(f"rsd{l}{o}"):
                own = paired(o, 0)
                remote(yss.at[l, o], ysr.at[l, o], ys_s, ys_r.at[o], facing).wait_recv()
                own = own + ysr[l, o].astype(F32)
                if o:
                    rss[l, o] = own.astype(BF16)
                    remote(
                        rss.at[l, o], rsr.at[l, o], rz_s, rs_r.at[o], at_z(o, yy, core)
                    ).start()
                else:
                    acc = own
        drains.append((rss.at[l, pl.ds(1, nz - 1)], rz_s))
        for o in near:
            with scope(f"rse{l}{o}"):
                remote(rss.at[l, o], rsr.at[l, o], rz_s, rs_r.at[o], facing).wait_recv()
                acc = acc + rsr[l, o].astype(F32)
        fresh_x = (xs[l, me].astype(F32) + acc).astype(BF16)
        if l + 1 < layers:
            xs[l + 1, me] = fresh_x
            loads[("q", l + 1)].wait()
            loads[("k", l + 1)].wait()
            gather(
                f"x{l}", xs.at[l + 1], ax_r, ag_s.at[layers + l], clear,
                lambda c, l=l: absorb(l + 1, 2 * c, 2),
            )
        else:
            y_ref[...] = fresh_x

    with scope("drain"):
        for ref, sem in drains:
            remote(ref, ref, sem, st_r.at[0], partner).wait_send()


def store_kernel(y_ref, state_ref, y_out, state_out, yv, sem):
    layers, seqs = state_ref.shape[:2]
    copies = []
    parts = sem.shape[0] - 1
    per = layers * seqs // parts
    for i in range(parts):
        l, s = i * per // seqs, pl.ds(i * per % seqs, per)
        copies.append(pltpu.make_async_copy(state_ref.at[l, s], state_out.at[l, s], sem.at[i]))
    for copy in copies:
        copy.start()
    yv[...] = y_ref[...].astype(F32).reshape(yv.shape).astype(BF16)
    copy = pltpu.make_async_copy(yv, y_out, sem.at[parts])
    copy.start()
    for copy in copies + [copy]:
        copy.wait()


def local(
    stream_in, state_in, norm_gain, query_weight, key_weight,
    value_weight, gate_weight, group_gain, output_weight,
):
    n = lax.axis_size("tp")
    seqs, tok, width = stream_in.shape
    layers, _, heads, e_dim, head_dim = state_in.shape
    cols = query_weight.shape[2]
    rows = seqs * tok
    he = heads * e_dim
    share = width // n
    fits = (
        cols == 128 and head_dim == 256 and he == 128 and heads == 8 and e_dim == 16
        and share % 128 == 0 and n % 4 == 0 and n & (n - 1) == 0 and rows == 128 and 8 % tok == 0
        and n == 2 * heads and seqs % 4 == 0
    )
    if not fits:
        return plain_local(
            stream_in, state_in, norm_gain, query_weight, key_weight,
            value_weight, gate_weight, group_gain, output_weight,
        )
    nc = n // 2
    be = seqs * e_dim
    hbm = pl.BlockSpec(memory_space=pltpu.HBM)
    vmem = pl.BlockSpec(memory_space=pltpu.VMEM)
    dma = pltpu.SemaphoreType.DMA
    tables = jnp.asarray(rotary_tables(heads, tok, head_dim))
    flat = lambda w: jnp.transpose(w, (0, 2, 3, 1)).reshape(layers, he, width)
    y, new_state = pl.pallas_call(
        functools.partial(kernel, n, head_dim),
        name="retention",
        out_shape=(
            pltpu.VMEM((rows, share), BF16),
            pltpu.VMEM(state_in.shape, F32),
        ),
        in_specs=[hbm] * 10,
        out_specs=(vmem, vmem),
        scratch_shapes=[
            pltpu.VMEM(norm_gain.shape, BF16),
            pltpu.VMEM(group_gain.shape, BF16),
            pltpu.VMEM(tables.shape, F32),
            pltpu.VMEM((seqs, tok, width), BF16),
            pltpu.VMEM((layers, n, rows, share), BF16),
            pltpu.VMEM((rows, width), BF16),
            pltpu.VMEM((layers, width, 2 * cols), BF16),
            pltpu.VMEM((layers, 2 * he, width), BF16),
            pltpu.VMEM((layers, he, width), BF16),
            pltpu.VMEM((layers, n, rows, 2 * cols), BF16),
            pltpu.VMEM((heads, rows, head_dim), BF16),
            pltpu.VMEM((he, rows), BF16),
            pltpu.VMEM((layers, n, heads, 2 * rows), F32),
            pltpu.VMEM((layers, nc, rows, share), BF16),
            pltpu.VMEM((layers, nc, rows, share), BF16),
            pltpu.VMEM((layers, nc // 2, rows, share), BF16),
            pltpu.VMEM((layers, nc // 2, rows, share), BF16),
            pltpu.VMEM((layers, nc // 2, rows, share), BF16),
            pltpu.VMEM((layers, nc // 2, rows, share), BF16),
            pltpu.VMEM((rows, be), BF16),
            pltpu.VMEM((be, rows), BF16),
            pltpu.VMEM((be, he), BF16),
            pltpu.VMEM((rows, share), F32),
            pltpu.VMEM((rows, 2 * cols), F32),
            dma((XPARTS + 6 * layers + 3,)),
            dma((2 * layers - 1,)),
            dma((layers,)),
            dma((layers, 3)),
            dma((n,)),
            dma((n,)),
            dma((1,)),
            dma((nc,)),
            dma((nc // 2,)),
            dma((nc // 2,)),
        ],
        compiler_params=pltpu.CompilerParams(
            collective_id=0, has_side_effects=True, vmem_limit_bytes=58500000
        ),
    )(
        stream_in, state_in, norm_gain, query_weight, key_weight,
        flat(value_weight), flat(gate_weight), group_gain,
        output_weight.reshape(layers, he, width), tables,
    )
    return pl.pallas_call(
        store_kernel,
        name="store",
        out_shape=(
            jax.ShapeDtypeStruct((seqs, tok, share), BF16),
            jax.ShapeDtypeStruct(state_in.shape, F32),
        ),
        in_specs=[vmem, vmem],
        out_specs=(hbm, hbm),
        scratch_shapes=[pltpu.VMEM((seqs, tok, share), BF16), dma((4 * layers + 1,))],
        compiler_params=pltpu.CompilerParams(vmem_limit_bytes=2 * 2**20),
    )(y, new_state)


def solution(mesh):
    in_specs = (
        P("grp", None, None),
        P(None, "grp", None, "tp", None),
        P(),
        P(None, None, "tp"),
        P(None, None, "tp"),
        P(None, None, None, "tp"),
        P(None, None, None, "tp"),
        P(None, None, "tp"),
        P(None, None, "tp", None),
    )
    out_specs = (P("grp", None, "tp"), P(None, "grp", None, "tp", None))
    return jax.shard_map(local, mesh=mesh, in_specs=in_specs, out_specs=out_specs, check_vma=False)
```

```python
import functools

import jax
import jax.numpy as jnp
import numpy as np
from jax import lax
from jax.experimental import pallas as pl
from jax.experimental.pallas import tpu as pltpu
from jax.sharding import PartitionSpec as P

HEAD_DIM = 256
PAST = 1024


EPS_RMS = 1e-06
EPS_GROUP = 1e-05
ROTARY_BASE = 10000.0


def log_decays(count):
    return jnp.log(1.0 - jnp.power(2.0, -5.0 - jnp.arange(count, dtype=jnp.float32)))


def decay_tables(log_gamma, count):
    steps = jnp.arange(count, dtype=jnp.float32)
    gap = steps[:, None] - steps[None, :]
    intra = jnp.where(
        gap[None] >= 0, jnp.exp(log_gamma[:, None, None] * jnp.maximum(gap, 0.0)[None]), 0.0
    )
    q_decay = jnp.exp(log_gamma[None, :] * (steps[:, None] + 1.0))
    k_decay = jnp.exp(log_gamma[None, :] * (count - 1.0 - steps[:, None]))
    block_decay = jnp.exp(log_gamma * count)
    return (intra, q_decay, k_decay, block_decay)


def rotate(values, offset):
    half_dim = values.shape[-1] // 2
    freqs = jnp.power(
        ROTARY_BASE, -jnp.arange(half_dim, dtype=jnp.float32) * (2.0 / values.shape[-1])
    )
    places = (offset + jnp.arange(values.shape[1])).astype(jnp.float32)
    angles = places[:, None] * freqs[None, :]
    cosine = jnp.cos(angles)[None, :, None, :]
    sine = jnp.sin(angles)[None, :, None, :]
    first = values[..., :half_dim]
    second = values[..., half_dim:]
    return jnp.concatenate(
        [first * cosine - second * sine, second * cosine + first * sine], axis=-1
    )


def plain_local(
    stream_in,
    state_in,
    norm_gain,
    query_weight,
    key_weight,
    value_weight,
    gate_weight,
    group_gain,
    output_weight,
):
    seqs, new_tok, width = stream_in.shape
    heads, local_dim = (value_weight.shape[2], value_weight.shape[3])
    head_dim = HEAD_DIM
    log_gamma = log_decays(heads)
    intra, q_decay, k_decay, block_decay = decay_tables(log_gamma, new_tok)
    highest = lax.Precision.HIGHEST
    share_cols = width // lax.axis_size("tp")
    col_start = lax.axis_index("tp") * share_cols
    layers = state_in.shape[0]
    stream = stream_in
    stream_share = stream_in
    new_states = []
    for layer_no in range(layers):
        stream_f = stream.astype(jnp.float32)
        normed = stream_f * lax.rsqrt(
            jnp.mean(stream_f * stream_f, axis=-1, keepdims=True) + EPS_RMS
        )
        normed = (normed * norm_gain[layer_no].astype(jnp.float32)).astype(jnp.bfloat16)
        flat = normed.reshape(seqs * new_tok, width)
        query_part = jnp.dot(flat, query_weight[layer_no], preferred_element_type=jnp.float32)
        query_part = query_part.astype(jnp.bfloat16).reshape(seqs, new_tok, -1)
        key_part = jnp.dot(flat, key_weight[layer_no], preferred_element_type=jnp.float32)
        key_part = key_part.astype(jnp.bfloat16).reshape(seqs, new_tok, -1)

        def project_local(weight):
            result = jnp.dot(
                flat, weight.reshape(width, heads * local_dim), preferred_element_type=jnp.float32
            )
            result = lax.optimization_barrier(result.astype(jnp.bfloat16))
            return result.astype(jnp.float32).reshape(seqs, new_tok, heads, local_dim)

        values_f = project_local(value_weight[layer_no])
        gates_f = project_local(gate_weight[layer_no])
        queries, key_rows = (
            lax.all_gather(query_part, "tp", axis=2, tiled=True),
            lax.all_gather(key_part, "tp", axis=2, tiled=True),
        )
        queries = queries.astype(jnp.float32).reshape(seqs, new_tok, heads, head_dim)
        key_rows = key_rows.astype(jnp.float32).reshape(seqs, new_tok, heads, head_dim)
        rot_q = rotate(queries, PAST)
        rot_k = rotate(key_rows, PAST) * head_dim ** (-0.5)
        scores = jnp.einsum("bthd,bshd->bhts", rot_q, rot_k, precision=highest) * intra[None]
        inner = jnp.einsum("bhts,bshe->bthe", scores, values_f, precision=highest)
        state = state_in[layer_no]
        carried = (
            jnp.einsum("bthd,bhed->bthe", rot_q, state, precision=highest)
            * q_decay[None, :, :, None]
        )
        mixed = inner + carried
        new_state = state * block_decay[None, :, None, None] + jnp.einsum(
            "bthe,bthd->bhed", values_f, rot_k * k_decay[None, :, :, None], precision=highest
        )
        new_states.append(new_state)
        totals, squares = lax.psum((jnp.sum(mixed, axis=-1), jnp.sum(mixed * mixed, axis=-1)), "tp")
        mean_o = (totals / head_dim)[..., None]
        var_o = (squares / head_dim)[..., None] - mean_o * mean_o
        normal = (
            (mixed - mean_o)
            * lax.rsqrt(var_o + EPS_GROUP)
            * group_gain[layer_no].astype(jnp.float32)[None, None]
        )
        gated = (jax.nn.silu(gates_f) * normal).astype(jnp.bfloat16)
        partial_out = jnp.dot(
            gated.reshape(seqs * new_tok, heads * local_dim),
            output_weight[layer_no].reshape(heads * local_dim, width),
            preferred_element_type=jnp.float32,
        ).reshape(seqs, new_tok, width)
        share_out = lax.psum_scatter(partial_out, "tp", scatter_dimension=2, tiled=True)
        own_cols = lax.dynamic_slice_in_dim(stream, col_start, share_cols, 2)
        stream_share = (own_cols.astype(jnp.float32) + share_out).astype(jnp.bfloat16)
        if layer_no + 1 < layers:
            stream = lax.all_gather(stream_share, "tp", axis=2, tiled=True)
    result = stream_share
    return (result, jnp.stack(new_states))


F32 = jnp.float32
BF16 = jnp.bfloat16
XPARTS = 4
scope = jax.named_scope


def nt_dot(a, b, precision=None):
    return lax.dot_general(
        a, b, (((1,), (1,)), ((), ())), preferred_element_type=F32, precision=precision
    )


def log2(value):
    return int(value).bit_length() - 1


def rotary_tables(heads, new_tok, head_dim):
    half = head_dim // 2
    freqs = np.power(
        np.float32(ROTARY_BASE), -np.arange(half, dtype=np.float32) * np.float32(2.0 / head_dim)
    ).astype(np.float32)
    tok = np.arange(8) % new_tok
    places = (PAST + tok).astype(np.float32)
    angles = (places[:, None] * freqs[None, :]).astype(np.float32).astype(np.float64)
    gamma = 1.0 - np.power(2.0, -5.0 - np.arange(heads))
    grow = np.power(gamma[:, None], tok[None, :] + 1.0)[:, :, None]
    shrink = head_dim ** (-0.5) / grow
    cosine, sine = np.cos(angles)[None], np.sin(angles)[None]
    block = np.broadcast_to(np.power(gamma, new_tok)[:, None, None], (heads, 8, half))
    return np.stack(
        [cosine * grow, sine * grow, cosine * shrink, sine * shrink, block]
    ).astype(np.float32)


def kernel(
    n, head_dim,
    x_hbm, st_hbm, ng_hbm, qw_hbm, kw_hbm, vw_hbm, gw_hbm, gg_hbm, ow_hbm, tab_hbm,
    y_ref, stv,
    ng_ref, gg_ref, tab_ref, xr, xs, nv, wqk, wvg, wo, qg, kg, sc, vts, sb, pbs, pbr, yss, ysr, rss, rsr, mkc, mks, fold, sqa, qka,
    lsem, ag_s, st_s, rs_s, aq_r, ak_r, ax_r, sc_r, st_r, pb_r, ys_r, rs_r,
):
    layers, seqs, heads, e_dim, _ = st_hbm.shape
    tok = x_hbm.shape[1]
    width = x_hbm.shape[2]
    rows = seqs * tok
    share = width // n
    cols = qw_hbm.shape[2]
    he = heads * e_dim
    half = head_dim // 2
    nc = n // 2
    me = lax.axis_index("tp")
    core = lax.rem(me, 2)
    chip = lax.div(me, 2)
    partner = chip * 2 + 1 - core

    nz = nc // 2
    yy = lax.rem(chip, 2)
    zz = lax.div(chip, 2)

    def chip_at(o, y):
        z, bit = zz, 1
        while bit < nz:
            if o & bit:
                z = z + bit - 2 * bit * lax.rem(lax.div(z, bit), 2)
            bit = 2 * bit
        return z * 2 + y

    def at_z(o, y, c):
        return chip_at(o, y) * 2 + c

    facing = at_z(0, 1 - yy, core)
    far = list(range(2, nz)) + [1]
    near = [1] + list(range(nz - 1, 1, -1))

    def remote(src, dst, ssem, rsem, device):
        return pltpu.make_async_remote_copy(
            src_ref=src, dst_ref=dst, send_sem=ssem, recv_sem=rsem,
            device_id={"tp": device}, device_id_type=pl.DeviceIdType.MESH,
        )

    loads = {}
    count = 0

    def load(name, src, dst):
        nonlocal count
        loads[name] = pltpu.make_async_copy(src, dst, lsem.at[count])
        loads[name].start()
        count += 1

    wide = width // XPARTS
    for j in range(XPARTS):
        at = pl.ds(j * wide, wide)
        load(("x", j), x_hbm.at[:, :, at], xr.at[:, :, at])
    load("ng", ng_hbm, ng_ref)

    barrier = pltpu.get_barrier_semaphore()
    for o in range(1, n):
        pl.semaphore_signal(
            barrier, inc=1, device_id={"tp": lax.rem(me + o, n)},
            device_id_type=pl.DeviceIdType.MESH,
        )

    for l in range(layers):
        deep = wide if l == 0 else width
        for j in range(width // deep):
            at = pl.ds(j * deep, deep)
            load(("q", l, j), qw_hbm.at[l, at], wqk.at[l, at, pl.ds(0, cols)])
            load(("k", l, j), kw_hbm.at[l, at], wqk.at[l, at, pl.ds(cols, cols)])
        load(("v", l), vw_hbm.at[l], wvg.at[l, pl.ds(0, he)])
        load(("g", l), gw_hbm.at[l], wvg.at[l, pl.ds(he, he)])
        load(("s", l), st_hbm.at[l], stv.at[l])
        load(("o", l), ow_hbm.at[l], wo.at[l])
        if l == 0:
            load("tab", tab_hbm, tab_ref)
            load("gg", gg_hbm, gg_ref)

    be = seqs * e_dim

    def iota(shape, dim, shift=0):
        return jnp.right_shift(lax.broadcasted_iota(jnp.int32, shape, dim), shift)

    te, tt = log2(e_dim), log2(tok)
    low = e_dim - 1
    causal = (
        (iota((rows, rows), 0, tt) == iota((rows, rows), 1, tt))
        & (iota((rows, rows), 0) >= iota((rows, rows), 1))
    ).astype(F32)
    heads_of = (iota((heads, he), 0) == iota((heads, he), 1, te)).astype(F32)
    place = (
        iota((e_dim, he), 0) == jnp.bitwise_and(iota((e_dim, he), 1), low)
    ).astype(F32)
    same = (iota((rows, rows), 0, tt) == iota((rows, rows), 1, tt)).astype(F32)
    pick = (
        jnp.bitwise_and(iota((8, rows), 1), tok - 1) == iota((8, rows), 0)
    ).astype(F32).astype(BF16)
    highest = lax.Precision.HIGHEST

    def make_masks():
        mkc[...] = (iota((rows, be), 0, tt) == iota((rows, be), 1, te)).astype(F32).astype(BF16)
        mks[...] = (iota((be, rows), 0, te) == iota((be, rows), 1, tt)).astype(F32).astype(BF16)
        fold[...] = (
            jnp.bitwise_and(iota((be, he), 0), low) == jnp.bitwise_and(iota((be, he), 1), low)
        ).astype(F32).astype(BF16)

    drains = []

    def ring(name, buf, recv, send):
        def push(slot, k, device):
            remote(slot, slot, send, recv.at[k], device).start()

        def arrive(slot, k):
            remote(slot, slot, send, recv.at[k], partner).wait_recv()

        def start(others=True, other_core=True):
            own = buf.at[me]
            if other_core:
                push(own, nc, partner)
            if others:
                push(own, nz, facing)
                for o in near:
                    push(own, o, at_z(o, yy, core))
                drains.append((buf.at[pl.ds(0, n - 1)], send))

        def last(k):
            return k if recv.shape[0] == n else nc if k == nc else nc + 1

        def from_z(o):
            with scope(f"{name}z{o}"):
                slot = buf.at[at_z(o, yy, core)]
                arrive(slot, o)
                push(slot, nz + o, facing)
                push(slot, last(nc + o), partner)

        def from_y(o):
            with scope(f"{name}y{o}"):
                slot = buf.at[at_z(o, 1 - yy, core)]
                arrive(slot, nz + o)
                push(slot, last(nc + nz + o), partner)

        def done(o, side):
            with scope(f"{name}d{side}{o}"):
                arrive(buf.at[at_z(o, 1 - yy if side else yy, 1 - core)], nc + nz * side + o)

        def done_rest():
            with scope(name + "rest"):
                arrive(buf.at[pl.ds(0, nc - 1)], nc + 1)

        return start, from_z, from_y, done, done_rest

    def in_order(name, from_z, from_y, done, on_chip):
        def use(o, side):
            done(o, side)
            with scope(f"{name}c{side}{o}"):
                on_chip(o, side)

        use(0, 0)
        from_z(near[0])
        from_y(0)
        for o in near[1:]:
            from_z(o)
        use(near[0], 0)
        use(0, 1)
        from_y(near[0])
        for a, b in zip(near[1:], near[:-1]):
            use(a, 0)
            from_y(a)
            use(b, 1)
        use(near[-1], 1)

    def spread(table):
        return jnp.broadcast_to(table[None], (rows // 8, 8, half)).reshape(rows, half)

    def rotated(buf, l, h, table):
        a, b = buf[l, 2 * h].astype(F32), buf[l, 2 * h + 1].astype(F32)
        cosine, sine = spread(tab_ref[table, h]), spread(tab_ref[table + 1, h])
        return jnp.concatenate([a * cosine - b * sine, b * cosine + a * sine], axis=1).astype(BF16)

    def absorb(l, j, count, block_of):
        at = pl.ds(pl.multiple_of(j * share, share), share * count)
        parts = []
        for i in range(count):
            block = block_of(j + i)
            sqa[...] += block * block
            one = pl.ds(pl.multiple_of((j + i) * share, share), share)
            gain = ng_ref[l : l + 1, one].astype(F32)
            scaled = (block * gain).astype(BF16)
            nv[:, one] = scaled
            parts.append(scaled)
        both = jnp.concatenate(parts, axis=1) if count > 1 else parts[0]
        qka[...] += jnp.dot(both, wqk[l, at, :], preferred_element_type=F32)

    def unpack(j):
        block = xr[:, :, pl.ds(j * share, share)].astype(F32).reshape(rows, share)
        xs[0, j] = block.astype(BF16)
        return block

    def clear():
        sqa[...] = jnp.zeros_like(sqa)
        qka[...] = jnp.zeros_like(qka)

    for l in range(layers):
        if l == 0:
            with scope("absorb"):
                clear()
                per = n // XPARTS
                loads["ng"].wait()
                for p in range(XPARTS):
                    for name in (("x", p), ("q", 0, p), ("k", 0, p)):
                        loads[name].wait()
                    absorb(0, p * per, per, unpack)

        with scope(f"qk{l}"):
            scale = lax.rsqrt(jnp.sum(sqa[...], axis=1, keepdims=True) / width + EPS_RMS)
            both = (qka[...] * scale).astype(BF16)
            qg[l, me] = both[:, :cols]
            kg[l, me] = both[:, cols:]
        if l == 0:
            with scope("bar"):
                pl.semaphore_wait(barrier, n - 1)

        q_start, q_z, q_y, q_done, _ = ring(f"q{l}", qg.at[l], aq_r, ag_s.at[l, 0])
        k_start, k_z, k_y, k_done, k_rest = ring(f"k{l}", kg.at[l], ak_r, ag_s.at[l, 1])
        q_start()
        k_start(others=False)
        if l == 0:
            with scope("masks"):
                make_masks()
                loads["tab"].wait()
                loads["gg"].wait()
        q_done(0, 0)
        k_done(0, 0)
        with scope(f"scores{l}"):
            rk = rotated(kg, l, chip, 2)
            scores = (nt_dot(rotated(qg, l, chip, 0), rk) * causal).astype(BF16)
            sc[l, chip] = nt_dot(pick, scores)
            for o, side in [(o, 0) for o in near] + [(0, 1)] + [(o, 1) for o in near]:
                slot = sc.at[l, chip]
                remote(
                    slot, slot, ag_s.at[l, 2], sc_r.at[side * nz + o],
                    at_z(o, 1 - yy if side else yy, core),
                ).start()
            drains.append((sc.at[l, pl.ds(0, nc - 1)], ag_s.at[l, 2]))
        k_start(other_core=False)

        with scope(f"vg{l}"):
            loads[("v", l)].wait()
            loads[("g", l)].wait()
            vg = nt_dot(nv[...], wvg[l]) * scale
            values = vg[:, :he].astype(BF16)
            gates = vg[:, he:].astype(BF16).astype(F32)
            vts[...] = jnp.transpose(values.astype(F32)).astype(BF16)
            loads[("s", l)].wait()
        box = {"mixed": jnp.zeros((rows, he), F32)}

        def mix(o, side, l=l, box=box, values=values):
            h = chip_at(o, 1 - yy if side else yy)
            rq = rotated(qg, l, h, 0)
            state = stv[l, :, h].reshape(be, head_dim).astype(BF16)
            carried = nt_dot(rq, state).astype(BF16) * mkc[...]
            part = jnp.dot(carried, fold[...], preferred_element_type=F32)
            if o or side:
                slot = sc.at[l, h]
                remote(slot, slot, ag_s.at[l, 2], sc_r.at[side * nz + o], partner).wait_recv()
            full = lax.dot_general(
                sc[l, h].astype(BF16), pick, (((0,), (0,)), ((), ())), preferred_element_type=F32
            )
            part = part + jnp.dot((full * same).astype(BF16), values, preferred_element_type=F32)
            own = (iota((1, he), 1, te) == h).astype(F32)
            box["mixed"] = box["mixed"] + part * own

        in_order(f"q{l}", q_z, q_y, lambda o, s: None if o == s == 0 else q_done(o, s), mix)
        mixed = box["mixed"]

        with scope(f"sums{l}"):
            sums = nt_dot(heads_of, mixed, highest)
            squares = nt_dot(heads_of, mixed * mixed, highest)
            sb[l, me] = jnp.concatenate([sums, squares], axis=1)
            for o in range(1, n):
                remote(sb.at[l, me], sb.at[l, me], st_s.at[l], st_r.at[0], lax.rem(me + o, n)).start()
            drains.append((sb.at[l, pl.ds(0, n - 1)], st_s.at[l]))

        for o in near:
            k_z(o)
        k_y(0)

        def update(h, carry, l=l):
            at = pl.ds(pl.multiple_of(h * e_dim, e_dim), e_dim)
            tall = jnp.broadcast_to(vts[at, :][None], (seqs, e_dim, rows)).reshape(be, rows)
            fresh = jnp.dot(tall * mks[...], rotated(kg, l, h, 2), preferred_element_type=F32)
            row = tab_ref[4, h][0:1, :]
            fade = jnp.concatenate([row, row], axis=1)
            state = stv[l, :, h].reshape(be, head_dim)
            stv[l, :, h] = ((state + fresh) * fade).reshape(seqs, e_dim, head_dim)
            return carry

        with scope(f"stwait{l}"):
            others = sb.at[l, pl.ds(0, n - 1)]
            remote(others, others, st_s.at[l], st_r.at[0], partner).wait_recv()

        with scope(f"gated{l}"):
            stats = jnp.sum(sb[l], axis=0)
            mean = stats[:, :rows] / head_dim
            var = stats[:, rows:] / head_dim - mean * mean
            rstd = lax.rsqrt(var + EPS_GROUP)

            def expand(small):
                return lax.dot_general(
                    small, heads_of, (((0,), (0,)), ((), ())),
                    preferred_element_type=F32, precision=highest,
                )

            gain = jnp.dot(gg_ref[l].astype(F32), place, preferred_element_type=F32, precision=highest)
            gain = jnp.sum(gain * heads_of, axis=0, keepdims=True)
            normal = (mixed - expand(mean)) * expand(rstd) * gain
            gated = (gates / (1.0 + jnp.exp(-gates)) * normal).astype(BF16)
            loads[("o", l)].wait()

        def chunk(j, l=l, gated=gated):
            at = pl.ds(pl.multiple_of(j * share, share), share)
            return jnp.dot(gated, wo[l, :, at], preferred_element_type=F32)

        order = far + [0]
        pb_s, ys_s, rz_s = rs_s.at[l, 0], rs_s.at[l, 1], rs_s.at[l, 2]

        def offer(o, side, l=l):
            k = side * nz + o
            y = 1 - yy if side else yy
            pbs[l, k] = chunk(at_z(o, y, 1 - core)).astype(BF16)
            remote(pbs.at[l, k], pbr.at[l, k], pb_s, pb_r.at[k], partner).start()

        def paired(o, side, l=l):
            k = side * nz + o
            own = chunk(at_z(o, 1 - yy if side else yy, core))
            remote(pbs.at[l, k], pbr.at[l, k], pb_s, pb_r.at[k], partner).wait_recv()
            return own + pbr[l, k].astype(F32)

        with scope(f"rsa{l}"):
            for o in order:
                offer(o, 1)
        with scope(f"rsb{l}"):
            for o in order:
                yss[l, o] = paired(o, 1).astype(BF16)
                remote(yss.at[l, o], ysr.at[l, o], ys_s, ys_r.at[o], facing).start()
        with scope(f"rsc{l}"):
            for o in order:
                offer(o, 0)
            drains.append((pbs.at[l], pb_s))
            drains.append((yss.at[l], ys_s))
        for o in near:
            k_y(o)
        k_rest()
        with scope(f"update{l}"):
            lax.fori_loop(0, heads, update, 0, unroll=True)
        acc = None
        for o in order:
            with scope(f"rsd{l}{o}"):
                own = paired(o, 0)
                remote(yss.at[l, o], ysr.at[l, o], ys_s, ys_r.at[o], facing).wait_recv()
                own = own + ysr[l, o].astype(F32)
                if o:
                    rss[l, o] = own.astype(BF16)
                    remote(
                        rss.at[l, o], rsr.at[l, o], rz_s, rs_r.at[o], at_z(o, yy, core)
                    ).start()
                else:
                    acc = own
        drains.append((rss.at[l, pl.ds(1, nz - 1)], rz_s))
        for o in near:
            with scope(f"rse{l}{o}"):
                remote(rss.at[l, o], rsr.at[l, o], rz_s, rs_r.at[o], facing).wait_recv()
                acc = acc + rsr[l, o].astype(F32)
        fresh_x = (xs[l, me].astype(F32) + acc).astype(BF16)
        if l + 1 < layers:
            xs[l + 1, me] = fresh_x
            loads[("q", l + 1, 0)].wait()
            loads[("k", l + 1, 0)].wait()
            x_start, x_z, x_y, x_done, _ = ring(f"x{l}", xs.at[l + 1], ax_r, ag_s.at[l, 3])
            x_start()
            clear()

            def take(o, side, l=l):
                c = chip_at(o, 1 - yy if side else yy)
                absorb(l + 1, 2 * c, 2, lambda j: xs[l + 1, j].astype(F32))

            in_order(f"x{l}", x_z, x_y, x_done, take)
        else:
            y_ref[...] = fresh_x

    with scope("drain"):
        for ref, sem in drains:
            remote(ref, ref, sem, st_r.at[0], partner).wait_send()


def store_kernel(y_ref, state_ref, y_out, state_out, yv, sem):
    layers, seqs = state_ref.shape[:2]
    copies = []
    parts = sem.shape[0] - 1
    per = layers * seqs // parts
    for i in range(parts):
        l, s = i * per // seqs, pl.ds(i * per % seqs, per)
        copies.append(pltpu.make_async_copy(state_ref.at[l, s], state_out.at[l, s], sem.at[i]))
    for copy in copies:
        copy.start()
    yv[...] = y_ref[...].astype(F32).reshape(yv.shape).astype(BF16)
    copy = pltpu.make_async_copy(yv, y_out, sem.at[parts])
    copy.start()
    for copy in copies + [copy]:
        copy.wait()


def local(
    stream_in, state_in, norm_gain, query_weight, key_weight,
    value_weight, gate_weight, group_gain, output_weight,
):
    n = lax.axis_size("tp")
    seqs, tok, width = stream_in.shape
    layers, _, heads, e_dim, head_dim = state_in.shape
    cols = query_weight.shape[2]
    rows = seqs * tok
    he = heads * e_dim
    share = width // n
    fits = (
        cols == 128 and head_dim == 256 and he == 128 and heads == 8 and e_dim == 16
        and share % 128 == 0 and n % 4 == 0 and n & (n - 1) == 0 and rows == 128 and 8 % tok == 0
        and n == 2 * heads and seqs % 4 == 0
    )
    if not fits:
        return plain_local(
            stream_in, state_in, norm_gain, query_weight, key_weight,
            value_weight, gate_weight, group_gain, output_weight,
        )
    nc = n // 2
    be = seqs * e_dim
    hbm = pl.BlockSpec(memory_space=pltpu.HBM)
    vmem = pl.BlockSpec(memory_space=pltpu.VMEM)
    dma = pltpu.SemaphoreType.DMA
    tables = jnp.asarray(rotary_tables(heads, tok, head_dim))
    flat = lambda w: jnp.transpose(w, (0, 2, 3, 1)).reshape(layers, he, width)
    y, new_state = pl.pallas_call(
        functools.partial(kernel, n, head_dim),
        name="retention",
        out_shape=(
            pltpu.VMEM((rows, share), BF16),
            pltpu.VMEM(state_in.shape, F32),
        ),
        in_specs=[hbm] * 10,
        out_specs=(vmem, vmem),
        scratch_shapes=[
            pltpu.VMEM(norm_gain.shape, BF16),
            pltpu.VMEM(group_gain.shape, BF16),
            pltpu.VMEM(tables.shape, F32),
            pltpu.VMEM((seqs, tok, width), BF16),
            pltpu.VMEM((layers, n, rows, share), BF16),
            pltpu.VMEM((rows, width), BF16),
            pltpu.VMEM((layers, width, 2 * cols), BF16),
            pltpu.VMEM((layers, 2 * he, width), BF16),
            pltpu.VMEM((layers, he, width), BF16),
            pltpu.VMEM((layers, n, rows, cols), BF16),
            pltpu.VMEM((layers, n, rows, cols), BF16),
            pltpu.VMEM((layers, heads, 8, rows), F32),
            pltpu.VMEM((he, rows), BF16),
            pltpu.VMEM((layers, n, heads, 2 * rows), F32),
            pltpu.VMEM((layers, nc, rows, share), BF16),
            pltpu.VMEM((layers, nc, rows, share), BF16),
            pltpu.VMEM((layers, nc // 2, rows, share), BF16),
            pltpu.VMEM((layers, nc // 2, rows, share), BF16),
            pltpu.VMEM((layers, nc // 2, rows, share), BF16),
            pltpu.VMEM((layers, nc // 2, rows, share), BF16),
            pltpu.VMEM((rows, be), BF16),
            pltpu.VMEM((be, rows), BF16),
            pltpu.VMEM((be, he), BF16),
            pltpu.VMEM((rows, share), F32),
            pltpu.VMEM((rows, 2 * cols), F32),
            dma((3 * XPARTS + 6 * layers + 1,)),
            dma((layers, 4)),
            dma((layers,)),
            dma((layers, 3)),
            dma((n,)),
            dma((nc + 2,)),
            dma((n,)),
            dma((nc,)),
            dma((1,)),
            dma((nc,)),
            dma((nc // 2,)),
            dma((nc // 2,)),
        ],
        compiler_params=pltpu.CompilerParams(
            collective_id=0, has_side_effects=True, vmem_limit_bytes=58500000
        ),
    )(
        stream_in, state_in, norm_gain, query_weight, key_weight,
        flat(value_weight), flat(gate_weight), group_gain,
        output_weight.reshape(layers, he, width), tables,
    )
    return pl.pallas_call(
        store_kernel,
        name="store",
        out_shape=(
            jax.ShapeDtypeStruct((seqs, tok, share), BF16),
            jax.ShapeDtypeStruct(state_in.shape, F32),
        ),
        in_specs=[vmem, vmem],
        out_specs=(hbm, hbm),
        scratch_shapes=[pltpu.VMEM((seqs, tok, share), BF16), dma((4 * layers + 1,))],
        compiler_params=pltpu.CompilerParams(vmem_limit_bytes=2 * 2**20),
    )(y, new_state)


def solution(mesh):
    in_specs = (
        P("grp", None, None),
        P(None, "grp", None, "tp", None),
        P(),
        P(None, None, "tp"),
        P(None, None, "tp"),
        P(None, None, None, "tp"),
        P(None, None, None, "tp"),
        P(None, None, "tp"),
        P(None, None, "tp", None),
    )
    out_specs = (P("grp", None, "tp"), P(None, "grp", None, "tp", None))
    return jax.shard_map(local, mesh=mesh, in_specs=in_specs, out_specs=out_specs, check_vma=False)
```

```python
import functools

import jax
import jax.numpy as jnp
import numpy as np
from jax import lax
from jax.experimental import pallas as pl
from jax.experimental.pallas import tpu as pltpu
from jax.sharding import PartitionSpec as P

HEAD_DIM = 256
PAST = 1024


EPS_RMS = 1e-06
EPS_GROUP = 1e-05
ROTARY_BASE = 10000.0


def log_decays(count):
    return jnp.log(1.0 - jnp.power(2.0, -5.0 - jnp.arange(count, dtype=jnp.float32)))


def decay_tables(log_gamma, count):
    steps = jnp.arange(count, dtype=jnp.float32)
    gap = steps[:, None] - steps[None, :]
    intra = jnp.where(
        gap[None] >= 0, jnp.exp(log_gamma[:, None, None] * jnp.maximum(gap, 0.0)[None]), 0.0
    )
    q_decay = jnp.exp(log_gamma[None, :] * (steps[:, None] + 1.0))
    k_decay = jnp.exp(log_gamma[None, :] * (count - 1.0 - steps[:, None]))
    block_decay = jnp.exp(log_gamma * count)
    return (intra, q_decay, k_decay, block_decay)


def rotate(values, offset):
    half_dim = values.shape[-1] // 2
    freqs = jnp.power(
        ROTARY_BASE, -jnp.arange(half_dim, dtype=jnp.float32) * (2.0 / values.shape[-1])
    )
    places = (offset + jnp.arange(values.shape[1])).astype(jnp.float32)
    angles = places[:, None] * freqs[None, :]
    cosine = jnp.cos(angles)[None, :, None, :]
    sine = jnp.sin(angles)[None, :, None, :]
    first = values[..., :half_dim]
    second = values[..., half_dim:]
    return jnp.concatenate(
        [first * cosine - second * sine, second * cosine + first * sine], axis=-1
    )


def plain_local(
    stream_in,
    state_in,
    norm_gain,
    query_weight,
    key_weight,
    value_weight,
    gate_weight,
    group_gain,
    output_weight,
):
    seqs, new_tok, width = stream_in.shape
    heads, local_dim = (value_weight.shape[2], value_weight.shape[3])
    head_dim = HEAD_DIM
    log_gamma = log_decays(heads)
    intra, q_decay, k_decay, block_decay = decay_tables(log_gamma, new_tok)
    highest = lax.Precision.HIGHEST
    share_cols = width // lax.axis_size("tp")
    col_start = lax.axis_index("tp") * share_cols
    layers = state_in.shape[0]
    stream = stream_in
    stream_share = stream_in
    new_states = []
    for layer_no in range(layers):
        stream_f = stream.astype(jnp.float32)
        normed = stream_f * lax.rsqrt(
            jnp.mean(stream_f * stream_f, axis=-1, keepdims=True) + EPS_RMS
        )
        normed = (normed * norm_gain[layer_no].astype(jnp.float32)).astype(jnp.bfloat16)
        flat = normed.reshape(seqs * new_tok, width)
        query_part = jnp.dot(flat, query_weight[layer_no], preferred_element_type=jnp.float32)
        query_part = query_part.astype(jnp.bfloat16).reshape(seqs, new_tok, -1)
        key_part = jnp.dot(flat, key_weight[layer_no], preferred_element_type=jnp.float32)
        key_part = key_part.astype(jnp.bfloat16).reshape(seqs, new_tok, -1)

        def project_local(weight):
            result = jnp.dot(
                flat, weight.reshape(width, heads * local_dim), preferred_element_type=jnp.float32
            )
            result = lax.optimization_barrier(result.astype(jnp.bfloat16))
            return result.astype(jnp.float32).reshape(seqs, new_tok, heads, local_dim)

        values_f = project_local(value_weight[layer_no])
        gates_f = project_local(gate_weight[layer_no])
        queries, key_rows = (
            lax.all_gather(query_part, "tp", axis=2, tiled=True),
            lax.all_gather(key_part, "tp", axis=2, tiled=True),
        )
        queries = queries.astype(jnp.float32).reshape(seqs, new_tok, heads, head_dim)
        key_rows = key_rows.astype(jnp.float32).reshape(seqs, new_tok, heads, head_dim)
        rot_q = rotate(queries, PAST)
        rot_k = rotate(key_rows, PAST) * head_dim ** (-0.5)
        scores = jnp.einsum("bthd,bshd->bhts", rot_q, rot_k, precision=highest) * intra[None]
        inner = jnp.einsum("bhts,bshe->bthe", scores, values_f, precision=highest)
        state = state_in[layer_no]
        carried = (
            jnp.einsum("bthd,bhed->bthe", rot_q, state, precision=highest)
            * q_decay[None, :, :, None]
        )
        mixed = inner + carried
        new_state = state * block_decay[None, :, None, None] + jnp.einsum(
            "bthe,bthd->bhed", values_f, rot_k * k_decay[None, :, :, None], precision=highest
        )
        new_states.append(new_state)
        totals, squares = lax.psum((jnp.sum(mixed, axis=-1), jnp.sum(mixed * mixed, axis=-1)), "tp")
        mean_o = (totals / head_dim)[..., None]
        var_o = (squares / head_dim)[..., None] - mean_o * mean_o
        normal = (
            (mixed - mean_o)
            * lax.rsqrt(var_o + EPS_GROUP)
            * group_gain[layer_no].astype(jnp.float32)[None, None]
        )
        gated = (jax.nn.silu(gates_f) * normal).astype(jnp.bfloat16)
        partial_out = jnp.dot(
            gated.reshape(seqs * new_tok, heads * local_dim),
            output_weight[layer_no].reshape(heads * local_dim, width),
            preferred_element_type=jnp.float32,
        ).reshape(seqs, new_tok, width)
        share_out = lax.psum_scatter(partial_out, "tp", scatter_dimension=2, tiled=True)
        own_cols = lax.dynamic_slice_in_dim(stream, col_start, share_cols, 2)
        stream_share = (own_cols.astype(jnp.float32) + share_out).astype(jnp.bfloat16)
        if layer_no + 1 < layers:
            stream = lax.all_gather(stream_share, "tp", axis=2, tiled=True)
    result = stream_share
    return (result, jnp.stack(new_states))


F32 = jnp.float32
BF16 = jnp.bfloat16
XPARTS = 4
scope = jax.named_scope


def nt_dot(a, b, precision=None):
    return lax.dot_general(
        a, b, (((1,), (1,)), ((), ())), preferred_element_type=F32, precision=precision
    )


def log2(value):
    return int(value).bit_length() - 1


def rotary_tables(heads, new_tok, head_dim):
    half = head_dim // 2
    freqs = np.power(
        np.float32(ROTARY_BASE), -np.arange(half, dtype=np.float32) * np.float32(2.0 / head_dim)
    ).astype(np.float32)
    tok = np.arange(8) % new_tok
    places = (PAST + tok).astype(np.float32)
    angles = (places[:, None] * freqs[None, :]).astype(np.float32).astype(np.float64)
    gamma = 1.0 - np.power(2.0, -5.0 - np.arange(heads))
    grow = np.power(gamma[:, None], tok[None, :] + 1.0)[:, :, None]
    shrink = head_dim ** (-0.5) / grow
    cosine, sine = np.cos(angles)[None], np.sin(angles)[None]
    block = np.broadcast_to(np.power(gamma, new_tok)[:, None, None], (heads, 8, half))
    return np.stack(
        [cosine * grow, sine * grow, cosine * shrink, sine * shrink, block]
    ).astype(np.float32)


def kernel(
    n, head_dim,
    x_hbm, st_hbm, ng_hbm, qw_hbm, kw_hbm, vw_hbm, gw_hbm, gg_hbm, ow_hbm, tab_hbm,
    y_ref, stv,
    ng_ref, gg_ref, tab_ref, xr, xs, nv, wqk, wvg, wo, qg, kg, sc, vts, vb, sb, pbs, pbr, yss, ysr, rss, rsr, mkc, mks, fold, sqa, qka, osum,
    lsem, ag_s, st_s, rs_s, aq_r, ak_r, ax_r, sc_r, st_r, pb_r, ys_r, rs_r,
):
    layers, seqs, heads, e_dim, _ = st_hbm.shape
    tok = x_hbm.shape[1]
    width = x_hbm.shape[2]
    rows = seqs * tok
    share = width // n
    cols = qw_hbm.shape[2]
    he = heads * e_dim
    half = head_dim // 2
    nc = n // 2
    me = lax.axis_index("tp")
    core = lax.rem(me, 2)
    chip = lax.div(me, 2)
    partner = chip * 2 + 1 - core

    nz = nc // 2
    yy = lax.rem(chip, 2)
    zz = lax.div(chip, 2)

    def chip_at(o, y):
        z, bit = zz, 1
        while bit < nz:
            if o & bit:
                z = z + bit - 2 * bit * lax.rem(lax.div(z, bit), 2)
            bit = 2 * bit
        return z * 2 + y

    def at_z(o, y, c):
        return chip_at(o, y) * 2 + c

    facing = at_z(0, 1 - yy, core)
    far = list(range(2, nz)) + [1]
    near = [1] + list(range(nz - 1, 1, -1))

    def remote(src, dst, ssem, rsem, device):
        return pltpu.make_async_remote_copy(
            src_ref=src, dst_ref=dst, send_sem=ssem, recv_sem=rsem,
            device_id={"tp": device}, device_id_type=pl.DeviceIdType.MESH,
        )

    loads = {}
    count = 0

    def load(name, src, dst):
        nonlocal count
        loads[name] = pltpu.make_async_copy(src, dst, lsem.at[count])
        loads[name].start()
        count += 1

    wide = width // XPARTS
    for j in range(XPARTS):
        at = pl.ds(j * wide, wide)
        load(("x", j), x_hbm.at[:, :, at], xr.at[:, :, at])
    load("ng", ng_hbm, ng_ref)

    barrier = pltpu.get_barrier_semaphore()
    for o in range(1, n):
        pl.semaphore_signal(
            barrier, inc=1, device_id={"tp": lax.rem(me + o, n)},
            device_id_type=pl.DeviceIdType.MESH,
        )

    for l in range(layers):
        deep = wide if l == 0 else width
        for j in range(width // deep):
            at = pl.ds(j * deep, deep)
            load(("q", l, j), qw_hbm.at[l, at], wqk.at[l, at, pl.ds(0, cols)])
            load(("k", l, j), kw_hbm.at[l, at], wqk.at[l, at, pl.ds(cols, cols)])
        load(("v", l), vw_hbm.at[l], wvg.at[l, pl.ds(0, he)])
        load(("g", l), gw_hbm.at[l], wvg.at[l, pl.ds(he, he)])
        load(("s", l), st_hbm.at[l], stv.at[l])
        load(("o", l), ow_hbm.at[l], wo.at[l])
        if l == 0:
            load("tab", tab_hbm, tab_ref)
            load("gg", gg_hbm, gg_ref)

    be = seqs * e_dim

    def iota(shape, dim, shift=0):
        return jnp.right_shift(lax.broadcasted_iota(jnp.int32, shape, dim), shift)

    te, tt = log2(e_dim), log2(tok)
    low = e_dim - 1
    causal = (
        (iota((rows, rows), 0, tt) == iota((rows, rows), 1, tt))
        & (iota((rows, rows), 0) >= iota((rows, rows), 1))
    ).astype(F32)
    heads_of = (iota((heads, he), 0) == iota((heads, he), 1, te)).astype(F32)
    place = (
        iota((e_dim, he), 0) == jnp.bitwise_and(iota((e_dim, he), 1), low)
    ).astype(F32)
    nth = jnp.concatenate(
        [
            (
                jnp.left_shift(iota((rows, rows), 0, tt), tt) + t == iota((rows, rows), 1)
            ).astype(F32).astype(BF16)
            for t in range(tok)
        ],
        axis=0,
    )
    pick = (
        jnp.bitwise_and(iota((8, rows), 1), tok - 1) == iota((8, rows), 0)
    ).astype(F32).astype(BF16)
    highest = lax.Precision.HIGHEST

    def make_masks():
        mkc[...] = (iota((rows, be), 0, tt) == iota((rows, be), 1, te)).astype(F32).astype(BF16)
        mks[...] = (iota((be, rows), 0, te) == iota((be, rows), 1, tt)).astype(F32).astype(BF16)
        fold[...] = (
            jnp.bitwise_and(iota((be, he), 0), low) == jnp.bitwise_and(iota((be, he), 1), low)
        ).astype(F32).astype(BF16)

    drains = []
    halves = [pl.ds(i * (rows // 2), rows // 2) for i in range(2)]

    def ring(name, buf, recv, send, at=None):
        def slot_of(j):
            return buf.at[j] if at is None else buf.at[j, at]

        def push(slot, k, device):
            remote(slot, slot, send, recv.at[k], device).start()

        def arrive(slot, k):
            remote(slot, slot, send, recv.at[k], partner).wait_recv()

        def start(others=True, other_core=True):
            own = slot_of(me)
            if other_core:
                push(own, nc, partner)
            if others:
                push(own, nz, facing)
                for o in near:
                    push(own, o, at_z(o, yy, core))
                drains.append((slot_of(pl.ds(0, n - 1)), send))

        def last(k):
            return k if recv.shape[0] == n else nc if k == nc else nc + 1

        def from_z(o):
            with scope(f"{name}z{o}"):
                slot = slot_of(at_z(o, yy, core))
                arrive(slot, o)
                push(slot, nz + o, facing)
                push(slot, last(nc + o), partner)

        def from_y(o):
            with scope(f"{name}y{o}"):
                slot = slot_of(at_z(o, 1 - yy, core))
                arrive(slot, nz + o)
                push(slot, last(nc + nz + o), partner)

        def done(o, side):
            with scope(f"{name}d{side}{o}"):
                arrive(slot_of(at_z(o, 1 - yy if side else yy, 1 - core)), nc + nz * side + o)

        def done_rest():
            with scope(name + "rest"):
                arrive(slot_of(pl.ds(0, nc - 1)), nc + 1)

        return start, from_z, from_y, done, done_rest

    def in_order(name, from_z, from_y, done, on_chip, between=lambda: None):
        def use(*which):
            for o, side in which:
                done(o, side)
            with scope(f"{name}c{which[0][1]}{which[0][0]}"):
                on_chip(which)

        use((0, 0))
        from_z(near[0])
        from_y(0)
        for o in near[1:]:
            from_z(o)
        use((near[0], 0), (0, 1))
        from_y(near[0])
        use(*[(o, 0) for o in near[1:]])
        for o in near[1:-1]:
            from_y(o)
        between()
        from_y(near[-1])
        use(*[(o, 1) for o in near[:-1]])
        use((near[-1], 1))

    def spread(table):
        return jnp.broadcast_to(table[None], (rows // 8, 8, half)).reshape(rows, half)

    def rotated(buf, l, h, table):
        a, b = buf[l, 2 * h].astype(F32), buf[l, 2 * h + 1].astype(F32)
        cosine, sine = spread(tab_ref[table, h]), spread(tab_ref[table + 1, h])
        return jnp.concatenate([a * cosine - b * sine, b * cosine + a * sine], axis=1).astype(BF16)

    def absorb(l, j, count, block_of):
        at = pl.ds(pl.multiple_of(j * share, share), share * count)
        parts = []
        for i in range(count):
            block = block_of(j + i)
            sqa[...] += block * block
            one = pl.ds(pl.multiple_of((j + i) * share, share), share)
            gain = ng_ref[l : l + 1, one].astype(F32)
            scaled = (block * gain).astype(BF16)
            nv[:, one] = scaled
            parts.append(scaled)
        both = jnp.concatenate(parts, axis=1) if count > 1 else parts[0]
        qka[...] += jnp.dot(both, wqk[l, at, :], preferred_element_type=F32)

    def unpack(j):
        block = xr[:, :, pl.ds(j * share, share)].astype(F32).reshape(rows, share)
        xs[0, j] = block.astype(BF16)
        return block

    def clear():
        sqa[...] = jnp.zeros_like(sqa)
        qka[...] = jnp.zeros_like(qka)

    for l in range(layers):
        if l == 0:
            with scope("absorb"):
                clear()
                per = n // XPARTS
                loads["ng"].wait()
                for p in range(XPARTS):
                    for name in (("x", p), ("q", 0, p), ("k", 0, p)):
                        loads[name].wait()
                    absorb(0, p * per, per, unpack)

        with scope(f"qk{l}"):
            scale = lax.rsqrt(jnp.sum(sqa[...], axis=1, keepdims=True) / width + EPS_RMS)
            both = (qka[...] * scale).astype(BF16)
            qg[l, me] = both[:, :cols]
            kg[l, me] = both[:, cols:]
        if l == 0:
            with scope("bar"):
                pl.semaphore_wait(barrier, n - 1)

        q_start, q_z, q_y, q_done, _ = ring(f"q{l}", qg.at[l], aq_r, ag_s.at[l, 0])
        k_start, k_z, k_y, k_done, k_rest = ring(f"k{l}", kg.at[l], ak_r, ag_s.at[l, 1])
        q_start()
        k_start(others=False)
        if l == 0:
            with scope("masks"):
                make_masks()
                loads["tab"].wait()
                loads["gg"].wait()
        q_done(0, 0)
        k_done(0, 0)
        with scope(f"scores{l}"):
            rk = rotated(kg, l, chip, 2)
            scores = (nt_dot(rotated(qg, l, chip, 0), rk) * causal).astype(BF16)
            sc[l, chip] = nt_dot(pick, scores)
            for o, side in [(o, side) for o in far for side in (1, 0)] + [(0, 1)]:
                slot = sc.at[l, chip]
                remote(
                    slot, slot, ag_s.at[l, 2], sc_r.at[0],
                    at_z(o, 1 - yy if side else yy, core),
                ).start()
            drains.append((sc.at[l, pl.ds(0, nc - 1)], ag_s.at[l, 2]))
        k_start(other_core=False)

        with scope(f"vg{l}"):
            loads[("v", l)].wait()
            loads[("g", l)].wait()
            vg = nt_dot(nv[...], wvg[l]) * scale
            values = vg[:, :he].astype(BF16)
            gates = vg[:, he:].astype(BF16).astype(F32)
            vts[...] = jnp.transpose(values.astype(F32)).astype(BF16)
            vb[...] = jnp.dot(nth, values, preferred_element_type=F32).reshape(tok, rows, he)
            loads[("s", l)].wait()
        box = {"mixed": jnp.zeros((rows, he), F32)}

        def carry_one(o, side, l=l):
            h = chip_at(o, 1 - yy if side else yy)
            rq = rotated(qg, l, h, 0)
            state = stv[l, :, h].reshape(be, head_dim).astype(BF16)
            carried = nt_dot(rq, state).astype(BF16) * mkc[...]
            part = jnp.dot(carried, fold[...], preferred_element_type=F32)
            return part * (iota((1, he), 1, te) == h).astype(F32)

        def intra(l=l, box=box):
            with scope(f"intra{l}"):
                others = sc.at[l, pl.ds(0, nc - 1)]
                remote(others, others, ag_s.at[l, 2], sc_r.at[0], partner).wait_recv()
                flat = jnp.concatenate([sc[l, :, t, :] for t in range(tok)], axis=1).astype(BF16)
                wide = lax.dot_general(
                    flat, heads_of.astype(BF16), (((0,), (0,)), ((), ())), preferred_element_type=F32
                )
                box["mixed"] = box["mixed"] + jnp.sum(wide.reshape(tok, rows, he) * vb[...], axis=0)

        def mix(which, box=box):
            for o, side in which:
                box["mixed"] = box["mixed"] + carry_one(o, side)

        in_order(f"q{l}", q_z, q_y, lambda o, s: None if o == s == 0 else q_done(o, s), mix, intra)
        mixed = box["mixed"]

        with scope(f"sums{l}"):
            sums = nt_dot(heads_of, mixed, highest)
            squares = nt_dot(heads_of, mixed * mixed, highest)
            sb[l, me] = jnp.concatenate([sums, squares], axis=1)
            peers = [at_z(o, y, c) for o in far for y in (1 - yy, yy) for c in (core, 1 - core)]
            for device in peers + [at_z(0, 1 - yy, 1 - core), facing, partner]:
                remote(sb.at[l, me], sb.at[l, me], st_s.at[l], st_r.at[0], device).start()
            drains.append((sb.at[l, pl.ds(0, n - 1)], st_s.at[l]))

        for o in near:
            k_z(o)
        k_y(0)

        def update(h, carry, l=l):
            at = pl.ds(pl.multiple_of(h * e_dim, e_dim), e_dim)
            tall = jnp.broadcast_to(vts[at, :][None], (seqs, e_dim, rows)).reshape(be, rows)
            fresh = jnp.dot(tall * mks[...], rotated(kg, l, h, 2), preferred_element_type=F32)
            row = tab_ref[4, h][0:1, :]
            fade = jnp.concatenate([row, row], axis=1)
            state = stv[l, :, h].reshape(be, head_dim)
            stv[l, :, h] = ((state + fresh) * fade).reshape(seqs, e_dim, head_dim)
            return carry

        with scope(f"silu{l}"):
            gain = jnp.dot(gg_ref[l].astype(F32), place, preferred_element_type=F32, precision=highest)
            gain = jnp.sum(gain * heads_of, axis=0, keepdims=True)
            gains = gates / (1.0 + jnp.exp(-gates)) * gain

        with scope(f"stwait{l}"):
            others = sb.at[l, pl.ds(0, n - 1)]
            remote(others, others, st_s.at[l], st_r.at[0], partner).wait_recv()

        with scope(f"gated{l}"):
            stats = jnp.sum(sb[l], axis=0)
            mean = stats[:, :rows] / head_dim
            var = stats[:, rows:] / head_dim - mean * mean
            rstd = lax.rsqrt(var + EPS_GROUP)

            def expand(small):
                return lax.dot_general(
                    small, heads_of, (((0,), (0,)), ((), ())),
                    preferred_element_type=F32, precision=highest,
                )

            gated = ((mixed - expand(mean)) * expand(rstd) * gains).astype(BF16)
            loads[("o", l)].wait()

        def chunk(j, l=l, gated=gated):
            at = pl.ds(pl.multiple_of(j * share, share), share)
            return jnp.dot(gated, wo[l, :, at], preferred_element_type=F32)

        order = far + [0]
        pb_s, ys_s, rz_s = rs_s.at[l, 0], rs_s.at[l, 1], rs_s.at[l, 2]

        def offer(o, side, l=l):
            k = side * nz + o
            y = 1 - yy if side else yy
            pbs[l, k] = chunk(at_z(o, y, 1 - core)).astype(BF16)
            remote(pbs.at[l, k], pbr.at[l, k], pb_s, pb_r.at[k], partner).start()

        def paired(o, side, l=l):
            k = side * nz + o
            own = chunk(at_z(o, 1 - yy if side else yy, core))
            remote(pbs.at[l, k], pbr.at[l, k], pb_s, pb_r.at[k], partner).wait_recv()
            return own + pbr[l, k].astype(F32)

        early = order[0]
        later = order[1:]
        tail = halves[1]

        def hop(o, at, l=l):
            src, dst = yss.at[l, o, at], ysr.at[l, o, at]
            return remote(src, dst, ys_s, ys_r.at[halves.index(at), o], facing)

        def turn(o, at, l=l):
            src, dst = rss.at[l, o, at], rsr.at[l, o, at]
            return remote(src, dst, rz_s, rs_r.at[halves.index(at), o], at_z(o, yy, core))

        def cross(l=l):
            return remote(rss.at[l, 0, tail], rsr.at[l, 0, tail], rz_s, rs_r.at[1, 0], at_z(early, yy, core))

        with scope(f"rsa{l}"):
            offer(early, 1)
            offer(early, 0)
            for o in later:
                offer(o, 1)
        with scope(f"rsb{l}"):
            both = paired(early, 1).astype(BF16)
            yss[l, early] = both
            hop(early, halves[0]).start()
            rss[l, 0, tail] = both[rows // 2 :]
            cross().start()
            osum[early] = paired(early, 0)
            rss[l, early, tail] = osum[early, tail].astype(BF16)
            turn(early, tail).start()
            for o in later[:-1]:
                yss[l, o] = paired(o, 1).astype(BF16)
                hop(o, halves[0]).start()
            osum[nz] = paired(0, 1)
            yss[l, 0, halves[0]] = osum[nz, halves[0]].astype(BF16)
            hop(0, halves[0]).start()
            for o in later[:-1]:
                hop(o, tail).start()
        with scope(f"rsc{l}"):
            for o in later:
                offer(o, 0)
            for o in near:
                k_y(o)
            drains.append((pbs.at[l], pb_s))
            drains.append((pbs.at[l, pl.ds(0, 2 * nz - 1), tail], ys_s))
            drains.append((pbs.at[l, pl.ds(0, 2 * nz - 1), tail], rz_s))
        with scope(f"own{l}"):
            for o in later:
                osum[o] = paired(o, 0)

        def join(o, at, l=l):
            with scope(f"rsd{l}{o}"):
                hop(o, at).wait_recv()
                own = osum[o, at] + ysr[l, o, at].astype(F32)
                if o:
                    rss[l, o, at] = own.astype(BF16)
                    turn(o, at).start()
                else:
                    osum[o, at] = own

        def finish(at, l=l):
            acc = osum[0, at] + xs[l, me, at].astype(F32)
            with scope(f"rse{l}"):
                for o in near:
                    turn(o, at).wait_recv()
                    acc = acc + rsr[l, o, at].astype(F32)
            return acc.astype(BF16)

        for o in order:
            join(o, halves[0])
        for o in later[:-1]:
            join(o, tail)
        with scope(f"cross{l}"):
            cross().wait_recv()
            yss[l, 0, tail] = (osum[nz, tail] + rsr[l, 0, tail].astype(F32)).astype(BF16)
            hop(0, tail).start()
        k_rest()
        with scope(f"update{l}"):
            lax.fori_loop(0, heads, update, 0, unroll=True)
        if l + 1 == layers:
            y_ref[halves[0], :] = finish(halves[0])
            join(0, tail)
            y_ref[tail, :] = finish(tail)
            continue

        rings = []
        clear()
        for i, at in enumerate(halves):
            rings.append(ring(f"x{l}{i}", xs.at[l + 1], ax_r.at[i], ag_s.at[l, 3 + i], at))
            if i:
                join(0, tail)
            xs[l + 1, me, at] = finish(at)
            rings[i][0]()
        loads[("q", l + 1, 0)].wait()
        loads[("k", l + 1, 0)].wait()
        (_, az, ay, ad, _), (_, bz, by, bd, _) = rings

        def use(*which, l=l):
            for o, side in which:
                ad(o, side)
                bd(o, side)
            with scope(f"x{l}c{which[0][1]}{which[0][0]}"):
                for o, side in which:
                    c = chip_at(o, 1 - yy if side else yy)
                    absorb(l + 1, 2 * c, 2, lambda j: xs[l + 1, j].astype(F32))

        first, rest, end = near[0], near[1:], near[-1]
        az(first)
        ay(0)
        for o in rest:
            az(o)
        bz(first)
        ay(first)
        by(0)
        use((0, 0))
        for o in rest[:-1]:
            ay(o)
            bz(o)
        ay(end)
        bz(end)
        use((first, 0), (0, 1))
        by(first)
        use(*[(o, 0) for o in rest])
        for o in rest[:-1]:
            by(o)
        by(end)
        use(*[(o, 1) for o in near[:-1]])
        use((end, 1))

    with scope("drain"):
        for ref, sem in drains:
            remote(ref, ref, sem, st_r.at[0], partner).wait_send()


def store_kernel(y_ref, state_ref, y_out, state_out, yv, sem):
    layers, seqs = state_ref.shape[:2]
    copies = []
    parts = sem.shape[0] - 1
    per = layers * seqs // parts
    for i in range(parts):
        l, s = i * per // seqs, pl.ds(i * per % seqs, per)
        copies.append(pltpu.make_async_copy(state_ref.at[l, s], state_out.at[l, s], sem.at[i]))
    for copy in copies:
        copy.start()
    yv[...] = y_ref[...].astype(F32).reshape(yv.shape).astype(BF16)
    copy = pltpu.make_async_copy(yv, y_out, sem.at[parts])
    copy.start()
    for copy in copies + [copy]:
        copy.wait()


def local(
    stream_in, state_in, norm_gain, query_weight, key_weight,
    value_weight, gate_weight, group_gain, output_weight,
):
    n = lax.axis_size("tp")
    seqs, tok, width = stream_in.shape
    layers, _, heads, e_dim, head_dim = state_in.shape
    cols = query_weight.shape[2]
    rows = seqs * tok
    he = heads * e_dim
    share = width // n
    fits = (
        cols == 128 and head_dim == 256 and he == 128 and heads == 8 and e_dim == 16
        and share % 128 == 0 and n % 4 == 0 and n & (n - 1) == 0 and rows == 128 and 8 % tok == 0
        and n == 2 * heads and seqs % 4 == 0
    )
    if not fits:
        return plain_local(
            stream_in, state_in, norm_gain, query_weight, key_weight,
            value_weight, gate_weight, group_gain, output_weight,
        )
    nc = n // 2
    be = seqs * e_dim
    hbm = pl.BlockSpec(memory_space=pltpu.HBM)
    vmem = pl.BlockSpec(memory_space=pltpu.VMEM)
    dma = pltpu.SemaphoreType.DMA
    tables = jnp.asarray(rotary_tables(heads, tok, head_dim))
    flat = lambda w: jnp.transpose(w, (0, 2, 3, 1)).reshape(layers, he, width)
    y, new_state = pl.pallas_call(
        functools.partial(kernel, n, head_dim),
        name="retention",
        out_shape=(
            pltpu.VMEM((rows, share), BF16),
            pltpu.VMEM(state_in.shape, F32),
        ),
        in_specs=[hbm] * 10,
        out_specs=(vmem, vmem),
        scratch_shapes=[
            pltpu.VMEM(norm_gain.shape, BF16),
            pltpu.VMEM(group_gain.shape, BF16),
            pltpu.VMEM(tables.shape, F32),
            pltpu.VMEM((seqs, tok, width), BF16),
            pltpu.VMEM((layers, n, rows, share), BF16),
            pltpu.VMEM((rows, width), BF16),
            pltpu.VMEM((layers, width, 2 * cols), BF16),
            pltpu.VMEM((layers, 2 * he, width), BF16),
            pltpu.VMEM((layers, he, width), BF16),
            pltpu.VMEM((layers, n, rows, cols), BF16),
            pltpu.VMEM((layers, n, rows, cols), BF16),
            pltpu.VMEM((layers, heads, 8, rows), F32),
            pltpu.VMEM((he, rows), BF16),
            pltpu.VMEM((tok, rows, he), F32),
            pltpu.VMEM((layers, n, heads, 2 * rows), F32),
            pltpu.VMEM((layers, nc, rows, share), BF16),
            pltpu.VMEM((layers, nc, rows, share), BF16),
            pltpu.VMEM((layers, nc // 2, rows, share), BF16),
            pltpu.VMEM((layers, nc // 2, rows, share), BF16),
            pltpu.VMEM((layers, nc // 2, rows, share), BF16),
            pltpu.VMEM((layers, nc // 2, rows, share), BF16),
            pltpu.VMEM((rows, be), BF16),
            pltpu.VMEM((be, rows), BF16),
            pltpu.VMEM((be, he), BF16),
            pltpu.VMEM((rows, share), F32),
            pltpu.VMEM((rows, 2 * cols), F32),
            pltpu.VMEM((nc // 2 + 1, rows, share), F32),
            dma((3 * XPARTS + 6 * layers + 1,)),
            dma((layers, 5)),
            dma((layers,)),
            dma((layers, 3)),
            dma((n,)),
            dma((nc + 2,)),
            dma((2, n)),
            dma((1,)),
            dma((1,)),
            dma((nc,)),
            dma((2, nc // 2)),
            dma((2, nc // 2)),
        ],
        compiler_params=pltpu.CompilerParams(
            collective_id=0, has_side_effects=True, vmem_limit_bytes=58500000
        ),
    )(
        stream_in, state_in, norm_gain, query_weight, key_weight,
        flat(value_weight), flat(gate_weight), group_gain,
        output_weight.reshape(layers, he, width), tables,
    )
    return pl.pallas_call(
        store_kernel,
        name="store",
        out_shape=(
            jax.ShapeDtypeStruct((seqs, tok, share), BF16),
            jax.ShapeDtypeStruct(state_in.shape, F32),
        ),
        in_specs=[vmem, vmem],
        out_specs=(hbm, hbm),
        scratch_shapes=[pltpu.VMEM((seqs, tok, share), BF16), dma((4 * layers + 1,))],
        compiler_params=pltpu.CompilerParams(vmem_limit_bytes=2 * 2**20),
    )(y, new_state)


def solution(mesh):
    in_specs = (
        P("grp", None, None),
        P(None, "grp", None, "tp", None),
        P(),
        P(None, None, "tp"),
        P(None, None, "tp"),
        P(None, None, None, "tp"),
        P(None, None, None, "tp"),
        P(None, None, "tp"),
        P(None, None, "tp", None),
    )
    out_specs = (P("grp", None, "tp"), P(None, "grp", None, "tp", None))
    return jax.shard_map(local, mesh=mesh, in_specs=in_specs, out_specs=out_specs, check_vma=False)
```

```python
import functools

import jax
import jax.numpy as jnp
import numpy as np
from jax import lax
from jax.experimental import pallas as pl
from jax.experimental.pallas import tpu as pltpu
from jax.sharding import PartitionSpec as P

HEAD_DIM = 256
PAST = 1024


EPS_RMS = 1e-06
EPS_GROUP = 1e-05
ROTARY_BASE = 10000.0


def log_decays(count):
    return jnp.log(1.0 - jnp.power(2.0, -5.0 - jnp.arange(count, dtype=jnp.float32)))


def decay_tables(log_gamma, count):
    steps = jnp.arange(count, dtype=jnp.float32)
    gap = steps[:, None] - steps[None, :]
    intra = jnp.where(
        gap[None] >= 0, jnp.exp(log_gamma[:, None, None] * jnp.maximum(gap, 0.0)[None]), 0.0
    )
    q_decay = jnp.exp(log_gamma[None, :] * (steps[:, None] + 1.0))
    k_decay = jnp.exp(log_gamma[None, :] * (count - 1.0 - steps[:, None]))
    block_decay = jnp.exp(log_gamma * count)
    return (intra, q_decay, k_decay, block_decay)


def rotate(values, offset):
    half_dim = values.shape[-1] // 2
    freqs = jnp.power(
        ROTARY_BASE, -jnp.arange(half_dim, dtype=jnp.float32) * (2.0 / values.shape[-1])
    )
    places = (offset + jnp.arange(values.shape[1])).astype(jnp.float32)
    angles = places[:, None] * freqs[None, :]
    cosine = jnp.cos(angles)[None, :, None, :]
    sine = jnp.sin(angles)[None, :, None, :]
    first = values[..., :half_dim]
    second = values[..., half_dim:]
    return jnp.concatenate(
        [first * cosine - second * sine, second * cosine + first * sine], axis=-1
    )


def plain_local(
    stream_in,
    state_in,
    norm_gain,
    query_weight,
    key_weight,
    value_weight,
    gate_weight,
    group_gain,
    output_weight,
):
    seqs, new_tok, width = stream_in.shape
    heads, local_dim = (value_weight.shape[2], value_weight.shape[3])
    head_dim = HEAD_DIM
    log_gamma = log_decays(heads)
    intra, q_decay, k_decay, block_decay = decay_tables(log_gamma, new_tok)
    highest = lax.Precision.HIGHEST
    share_cols = width // lax.axis_size("tp")
    col_start = lax.axis_index("tp") * share_cols
    layers = state_in.shape[0]
    stream = stream_in
    stream_share = stream_in
    new_states = []
    for layer_no in range(layers):
        stream_f = stream.astype(jnp.float32)
        normed = stream_f * lax.rsqrt(
            jnp.mean(stream_f * stream_f, axis=-1, keepdims=True) + EPS_RMS
        )
        normed = (normed * norm_gain[layer_no].astype(jnp.float32)).astype(jnp.bfloat16)
        flat = normed.reshape(seqs * new_tok, width)
        query_part = jnp.dot(flat, query_weight[layer_no], preferred_element_type=jnp.float32)
        query_part = query_part.astype(jnp.bfloat16).reshape(seqs, new_tok, -1)
        key_part = jnp.dot(flat, key_weight[layer_no], preferred_element_type=jnp.float32)
        key_part = key_part.astype(jnp.bfloat16).reshape(seqs, new_tok, -1)

        def project_local(weight):
            result = jnp.dot(
                flat, weight.reshape(width, heads * local_dim), preferred_element_type=jnp.float32
            )
            result = lax.optimization_barrier(result.astype(jnp.bfloat16))
            return result.astype(jnp.float32).reshape(seqs, new_tok, heads, local_dim)

        values_f = project_local(value_weight[layer_no])
        gates_f = project_local(gate_weight[layer_no])
        queries, key_rows = (
            lax.all_gather(query_part, "tp", axis=2, tiled=True),
            lax.all_gather(key_part, "tp", axis=2, tiled=True),
        )
        queries = queries.astype(jnp.float32).reshape(seqs, new_tok, heads, head_dim)
        key_rows = key_rows.astype(jnp.float32).reshape(seqs, new_tok, heads, head_dim)
        rot_q = rotate(queries, PAST)
        rot_k = rotate(key_rows, PAST) * head_dim ** (-0.5)
        scores = jnp.einsum("bthd,bshd->bhts", rot_q, rot_k, precision=highest) * intra[None]
        inner = jnp.einsum("bhts,bshe->bthe", scores, values_f, precision=highest)
        state = state_in[layer_no]
        carried = (
            jnp.einsum("bthd,bhed->bthe", rot_q, state, precision=highest)
            * q_decay[None, :, :, None]
        )
        mixed = inner + carried
        new_state = state * block_decay[None, :, None, None] + jnp.einsum(
            "bthe,bthd->bhed", values_f, rot_k * k_decay[None, :, :, None], precision=highest
        )
        new_states.append(new_state)
        totals, squares = lax.psum((jnp.sum(mixed, axis=-1), jnp.sum(mixed * mixed, axis=-1)), "tp")
        mean_o = (totals / head_dim)[..., None]
        var_o = (squares / head_dim)[..., None] - mean_o * mean_o
        normal = (
            (mixed - mean_o)
            * lax.rsqrt(var_o + EPS_GROUP)
            * group_gain[layer_no].astype(jnp.float32)[None, None]
        )
        gated = (jax.nn.silu(gates_f) * normal).astype(jnp.bfloat16)
        partial_out = jnp.dot(
            gated.reshape(seqs * new_tok, heads * local_dim),
            output_weight[layer_no].reshape(heads * local_dim, width),
            preferred_element_type=jnp.float32,
        ).reshape(seqs, new_tok, width)
        share_out = lax.psum_scatter(partial_out, "tp", scatter_dimension=2, tiled=True)
        own_cols = lax.dynamic_slice_in_dim(stream, col_start, share_cols, 2)
        stream_share = (own_cols.astype(jnp.float32) + share_out).astype(jnp.bfloat16)
        if layer_no + 1 < layers:
            stream = lax.all_gather(stream_share, "tp", axis=2, tiled=True)
    result = stream_share
    return (result, jnp.stack(new_states))


F32 = jnp.float32
BF16 = jnp.bfloat16
XPARTS = 4
scope = jax.named_scope


def nt_dot(a, b, precision=None):
    return lax.dot_general(
        a, b, (((1,), (1,)), ((), ())), preferred_element_type=F32, precision=precision
    )


def thirds(value, axis):
    high = value.astype(BF16)
    rest = value - high.astype(F32)
    middle = rest.astype(BF16)
    low = (rest - middle.astype(F32)).astype(BF16)
    return jnp.concatenate([high, middle, low], axis=axis)


def log2(value):
    return int(value).bit_length() - 1


def rotary_tables(heads, new_tok, head_dim):
    half = head_dim // 2
    freqs = np.power(
        np.float32(ROTARY_BASE), -np.arange(half, dtype=np.float32) * np.float32(2.0 / head_dim)
    ).astype(np.float32)
    tok = np.arange(8) % new_tok
    places = (PAST + tok).astype(np.float32)
    angles = (places[:, None] * freqs[None, :]).astype(np.float32).astype(np.float64)
    gamma = 1.0 - np.power(2.0, -5.0 - np.arange(heads))
    grow = np.power(gamma[:, None], tok[None, :] + 1.0)[:, :, None]
    shrink = head_dim ** (-0.5) / grow
    cosine, sine = np.cos(angles)[None], np.sin(angles)[None]
    block = np.broadcast_to(np.power(gamma, new_tok)[:, None, None], (heads, 8, half))
    return np.stack(
        [cosine * grow, sine * grow, cosine * shrink, sine * shrink, block]
    ).astype(np.float32)


def kernel(
    n, head_dim,
    x_hbm, st_hbm, ng_hbm, qw_hbm, kw_hbm, vw_hbm, gw_hbm, gg_hbm, ow_hbm, tab_hbm,
    y_ref, stv,
    ng_ref, gg_ref, tab_ref, xr, xs, nv, wqk, wvg, wo, qg, kg, sc, vts, vb, sb, pbs, pbr, yss, ysr, rss, rsr, mkc, mks, fold, sqa, qka, vga, osum,
    lsem, ag_s, st_s, rs_s, aq_r, ak_r, ax_r, sc_r, st_r, pb_r, ys_r, rs_r,
):
    layers, seqs, heads, e_dim, _ = st_hbm.shape
    tok = x_hbm.shape[1]
    width = x_hbm.shape[2]
    rows = seqs * tok
    share = width // n
    cols = qw_hbm.shape[2]
    he = heads * e_dim
    half = head_dim // 2
    nc = n // 2
    me = lax.axis_index("tp")
    core = lax.rem(me, 2)
    chip = lax.div(me, 2)
    partner = chip * 2 + 1 - core

    nz = nc // 2
    yy = lax.rem(chip, 2)
    zz = lax.div(chip, 2)

    def chip_at(o, y):
        z, bit = zz, 1
        while bit < nz:
            if o & bit:
                z = z + bit - 2 * bit * lax.rem(lax.div(z, bit), 2)
            bit = 2 * bit
        return z * 2 + y

    def at_z(o, y, c):
        return chip_at(o, y) * 2 + c

    facing = at_z(0, 1 - yy, core)
    far = list(range(2, nz)) + [1]
    near = [1] + list(range(nz - 1, 1, -1))

    def remote(src, dst, ssem, rsem, device):
        return pltpu.make_async_remote_copy(
            src_ref=src, dst_ref=dst, send_sem=ssem, recv_sem=rsem,
            device_id={"tp": device}, device_id_type=pl.DeviceIdType.MESH,
        )

    loads = {}
    count = 0

    def load(name, src, dst):
        nonlocal count
        loads[name] = pltpu.make_async_copy(src, dst, lsem.at[count])
        loads[name].start()
        count += 1

    wide = width // XPARTS
    for j in range(XPARTS):
        at = pl.ds(j * wide, wide)
        load(("x", j), x_hbm.at[:, :, at], xr.at[:, :, at])
    load("ng", ng_hbm, ng_ref)

    barrier = pltpu.get_barrier_semaphore()
    for o in range(1, n):
        pl.semaphore_signal(
            barrier, inc=1, device_id={"tp": lax.rem(me + o, n)},
            device_id_type=pl.DeviceIdType.MESH,
        )

    for l in range(layers):
        deep = wide if l == 0 else width
        for j in range(width // deep):
            at = pl.ds(j * deep, deep)
            load(("q", l, j), qw_hbm.at[l, at], wqk.at[l, at, pl.ds(0, cols)])
            load(("k", l, j), kw_hbm.at[l, at], wqk.at[l, at, pl.ds(cols, cols)])
        load(("v", l), vw_hbm.at[l], wvg.at[l, pl.ds(0, he)])
        load(("g", l), gw_hbm.at[l], wvg.at[l, pl.ds(he, he)])
        load(("s", l), st_hbm.at[l], stv.at[l])
        load(("o", l), ow_hbm.at[l], wo.at[l])
        if l == 0:
            load("tab", tab_hbm, tab_ref)
            load("gg", gg_hbm, gg_ref)

    be = seqs * e_dim

    def iota(shape, dim, shift=0):
        return jnp.right_shift(lax.broadcasted_iota(jnp.int32, shape, dim), shift)

    te, tt = log2(e_dim), log2(tok)
    low = e_dim - 1
    causal = (
        (iota((rows, rows), 0, tt) == iota((rows, rows), 1, tt))
        & (iota((rows, rows), 0) >= iota((rows, rows), 1))
    ).astype(F32)
    heads_of = (iota((heads, he), 0) == iota((heads, he), 1, te)).astype(F32)
    place = (
        iota((e_dim, he), 0) == jnp.bitwise_and(iota((e_dim, he), 1), low)
    ).astype(F32)
    nth = jnp.concatenate(
        [
            (
                jnp.left_shift(iota((rows, rows), 0, tt), tt) + t == iota((rows, rows), 1)
            ).astype(F32).astype(BF16)
            for t in range(tok)
        ],
        axis=0,
    )
    pick = (
        jnp.bitwise_and(iota((8, rows), 1), tok - 1) == iota((8, rows), 0)
    ).astype(F32).astype(BF16)
    highest = lax.Precision.HIGHEST

    def make_masks():
        mkc[...] = (iota((rows, be), 0, tt) == iota((rows, be), 1, te)).astype(F32).astype(BF16)
        mks[...] = (iota((be, rows), 0, te) == iota((be, rows), 1, tt)).astype(F32).astype(BF16)
        fold[...] = (
            jnp.bitwise_and(iota((be, he), 0), low) == jnp.bitwise_and(iota((be, he), 1), low)
        ).astype(F32).astype(BF16)

    drains = []
    halves = [pl.ds(i * (rows // 2), rows // 2) for i in range(2)]

    def ring(name, buf, recv, send, at=None, direct=()):
        def slot_of(j):
            return buf.at[j] if at is None else buf.at[j, at]

        def push(slot, k, device):
            remote(slot, slot, send, recv.at[k], device).start()

        def arrive(slot, k):
            remote(slot, slot, send, recv.at[k], partner).wait_recv()

        def start(others=True, other_core=True):
            own = slot_of(me)
            if other_core:
                push(own, nc, partner)
            if others:
                push(own, nz, facing)
                for o in near:
                    push(own, o, at_z(o, yy, core))
                drains.append((slot_of(pl.ds(0, n - 1)), send))

        def last(k):
            return k if recv.shape[0] == n else nc if k == nc else nc + 1

        def from_z(o):
            with scope(f"{name}z{o}"):
                slot = slot_of(at_z(o, yy, core))
                arrive(slot, o)
                if o not in direct:
                    push(slot, nz + o, facing)
                push(slot, last(nc + o), partner)

        def from_y(o):
            with scope(f"{name}y{o}"):
                slot = slot_of(at_z(o, 1 - yy, core))
                arrive(slot, nz + o)
                for far_o in direct if o == 0 else ():
                    push(slot, nz + far_o, at_z(far_o, yy, core))
                push(slot, last(nc + nz + o), partner)

        def done(o, side):
            with scope(f"{name}d{side}{o}"):
                arrive(slot_of(at_z(o, 1 - yy if side else yy, 1 - core)), nc + nz * side + o)

        def done_rest():
            with scope(name + "rest"):
                arrive(slot_of(pl.ds(0, nc - 1)), nc + 1)

        return start, from_z, from_y, done, done_rest

    def in_order(name, from_z, from_y, done, on_chip, early, between, later):
        def use(*which):
            for o, side in which:
                done(o, side)
            with scope(f"{name}c{which[0][1]}{which[0][0]}"):
                on_chip(which)

        use((0, 0))
        from_z(near[0])
        from_y(0)
        early()
        for o in near[1:]:
            from_z(o)
        use((near[0], 0), (0, 1))
        from_y(near[0])
        use(*[(o, 0) for o in near[1:]])
        for o in near[1:-1]:
            from_y(o)
        between()
        from_y(near[-1])
        later()
        use(*[(o, 1) for o in near[:-1]])
        use((near[-1], 1))

    def spread(table):
        return jnp.broadcast_to(table[None], (rows // 8, 8, half)).reshape(rows, half)

    def rotated(buf, l, h, table):
        a, b = buf[l, 2 * h].astype(F32), buf[l, 2 * h + 1].astype(F32)
        cosine, sine = spread(tab_ref[table, h]), spread(tab_ref[table + 1, h])
        return jnp.concatenate([a * cosine - b * sine, b * cosine + a * sine], axis=1).astype(BF16)

    def absorb(l, j, count, block_of):
        at = pl.ds(pl.multiple_of(j * share, share), share * count)
        parts = []
        for i in range(count):
            block = block_of(j + i)
            sqa[...] += block * block
            one = pl.ds(pl.multiple_of((j + i) * share, share), share)
            gain = ng_ref[l : l + 1, one].astype(F32)
            scaled = (block * gain).astype(BF16)
            nv[:, one] = scaled
            parts.append(scaled)
        both = jnp.concatenate(parts, axis=1) if count > 1 else parts[0]
        qka[...] += jnp.dot(both, wqk[l, at, :], preferred_element_type=F32)
        if l:
            vga[...] += nt_dot(both, wvg[l, :, at])

    def unpack(j):
        block = xr[:, :, pl.ds(j * share, share)].astype(F32).reshape(rows, share)
        xs[0, j] = block.astype(BF16)
        return block

    def clear():
        sqa[...] = jnp.zeros_like(sqa)
        qka[...] = jnp.zeros_like(qka)
        vga[...] = jnp.zeros_like(vga)

    for l in range(layers):
        if l == 0:
            with scope("absorb"):
                clear()
                per = n // XPARTS
                loads["ng"].wait()
                for p in range(XPARTS):
                    for name in (("x", p), ("q", 0, p), ("k", 0, p)):
                        loads[name].wait()
                    absorb(0, p * per, per, unpack)

        with scope(f"qk{l}"):
            scale = lax.rsqrt(jnp.sum(sqa[...], axis=1, keepdims=True) / width + EPS_RMS)
            both = (qka[...] * scale).astype(BF16)
            qg[l, me] = both[:, :cols]
            kg[l, me] = both[:, cols:]
        if l == 0:
            with scope("bar"):
                pl.semaphore_wait(barrier, n - 1)

        q_start, q_z, q_y, q_done, _ = ring(f"q{l}", qg.at[l], aq_r, ag_s.at[l, 0])
        k_start, k_z, k_y, k_done, k_rest = ring(f"k{l}", kg.at[l], ak_r, ag_s.at[l, 1])
        q_start()
        k_start(others=False)
        if l == 0:
            with scope("masks"):
                make_masks()
                loads["tab"].wait()
                loads["gg"].wait()
        q_done(0, 0)
        k_done(0, 0)
        with scope(f"scores{l}"):
            rk = rotated(kg, l, chip, 2)
            scores = (nt_dot(rotated(qg, l, chip, 0), rk) * causal).astype(BF16)
            sc[l, chip] = nt_dot(pick, scores)
            for o, side in [(o, side) for o in far for side in (1, 0)] + [(0, 1)]:
                slot = sc.at[l, chip]
                remote(
                    slot, slot, ag_s.at[l, 2], sc_r.at[0],
                    at_z(o, 1 - yy if side else yy, core),
                ).start()
            drains.append((sc.at[l, pl.ds(0, nc - 1)], ag_s.at[l, 2]))
        k_start(other_core=False)

        with scope(f"vg{l}"):
            if l == 0:
                loads[("v", l)].wait()
                vga[:, :he] = nt_dot(nv[...], wvg[l, :he])
            values = (vga[:, :he] * scale).astype(BF16)
            vts[...] = jnp.transpose(values.astype(F32)).astype(BF16)
            vb[...] = jnp.dot(nth, values, preferred_element_type=F32).reshape(tok, rows, he)
            loads[("s", l)].wait()
        box = {"mixed": jnp.zeros((rows, he), F32)}

        def gate_on(l=l):
            if l == 0:
                with scope(f"gates{l}"):
                    loads[("g", l)].wait()
                    vga[:, he:] = nt_dot(nv[...], wvg[l, he:])

        def carry_one(o, side, l=l):
            h = chip_at(o, 1 - yy if side else yy)
            rq = rotated(qg, l, h, 0)
            state = stv[l, :, h].reshape(be, head_dim).astype(BF16)
            carried = nt_dot(rq, state).astype(BF16) * mkc[...]
            part = jnp.dot(carried, fold[...], preferred_element_type=F32)
            return part * (iota((1, he), 1, te) == h).astype(F32)

        def intra(l=l, box=box):
            with scope(f"intra{l}"):
                others = sc.at[l, pl.ds(0, nc - 1)]
                remote(others, others, ag_s.at[l, 2], sc_r.at[0], partner).wait_recv()
                flat = jnp.concatenate([sc[l, :, t, :] for t in range(tok)], axis=1).astype(BF16)
                wide = lax.dot_general(
                    flat, heads_of.astype(BF16), (((0,), (0,)), ((), ())), preferred_element_type=F32
                )
                box["mixed"] = box["mixed"] + jnp.sum(wide.reshape(tok, rows, he) * vb[...], axis=0)

        def k_on(k_z=k_z, k_y=k_y):
            for o in near:
                k_z(o)
            k_y(0)

        def mix(which, box=box):
            for o, side in which:
                box["mixed"] = box["mixed"] + carry_one(o, side)

        in_order(f"q{l}", q_z, q_y, lambda o, s: None if o == s == 0 else q_done(o, s), mix, gate_on, intra, k_on)
        mixed = box["mixed"]

        with scope(f"sums{l}"):
            both = nt_dot(
                jnp.concatenate([heads_of.astype(BF16)] * 3, axis=1),
                thirds(jnp.concatenate([mixed, mixed * mixed], axis=0), 1),
            )
            sums = both[:, :rows]
            squares = jnp.maximum(both[:, rows:] - sums * sums / e_dim, 0.0)
            sb[l, me] = jnp.concatenate([sums, squares], axis=1).astype(BF16)
            peers = [at_z(o, y, c) for o in far for y in (1 - yy, yy) for c in (core, 1 - core)]
            for device in peers + [at_z(0, 1 - yy, 1 - core), facing, partner]:
                remote(sb.at[l, me], sb.at[l, me], st_s.at[l], st_r.at[0], device).start()
            drains.append((sb.at[l, pl.ds(0, n - 1)], st_s.at[l]))

        def update(h, carry, l=l):
            at = pl.ds(pl.multiple_of(h * e_dim, e_dim), e_dim)
            tall = jnp.broadcast_to(vts[at, :][None], (seqs, e_dim, rows)).reshape(be, rows)
            fresh = jnp.dot(tall * mks[...], rotated(kg, l, h, 2), preferred_element_type=F32)
            row = tab_ref[4, h][0:1, :]
            fade = jnp.concatenate([row, row], axis=1)
            state = stv[l, :, h].reshape(be, head_dim)
            stv[l, :, h] = ((state + fresh) * fade).reshape(seqs, e_dim, head_dim)
            return carry

        with scope(f"silu{l}"):
            gates = (vga[:, he:] * scale).astype(BF16).astype(F32)
            gain = jnp.dot(gg_ref[l].astype(F32), place, preferred_element_type=F32, precision=highest)
            gain = jnp.sum(gain * heads_of, axis=0, keepdims=True)
            gains = gates / (1.0 + jnp.exp(-gates)) * gain

        with scope(f"stwait{l}"):
            others = sb.at[l, pl.ds(0, n - 1)]
            remote(others, others, st_s.at[l], st_r.at[0], partner).wait_recv()

        with scope(f"gated{l}"):
            stats = sb[l].astype(F32)
            sums = stats[:, :, :rows]
            total = jnp.sum(sums, axis=0)
            off = sums - (total / n)[None]
            var = jnp.sum(stats[:, :, rows:] + off * off / e_dim, axis=0) / head_dim
            both = jnp.concatenate([total / head_dim, lax.rsqrt(var + EPS_GROUP)], axis=1)
            both = lax.dot_general(
                thirds(both, 0), jnp.concatenate([heads_of.astype(BF16)] * 3, axis=0),
                (((0,), (0,)), ((), ())), preferred_element_type=F32,
            )
            gated = ((mixed - both[:rows]) * both[rows:] * gains).astype(BF16)
            loads[("o", l)].wait()

        def chunk(j, l=l, gated=gated):
            at = pl.ds(pl.multiple_of(j * share, share), share)
            return jnp.dot(gated, wo[l, :, at], preferred_element_type=F32)

        order = far + [0]
        pb_s, ys_s, rz_s = rs_s.at[l, 0], rs_s.at[l, 1], rs_s.at[l, 2]

        def offer(o, side, l=l):
            k = side * nz + o
            y = 1 - yy if side else yy
            pbs[l, k] = chunk(at_z(o, y, 1 - core)).astype(BF16)
            remote(pbs.at[l, k], pbr.at[l, k], pb_s, pb_r.at[k], partner).start()

        def paired(o, side, l=l):
            k = side * nz + o
            own = chunk(at_z(o, 1 - yy if side else yy, core))
            remote(pbs.at[l, k], pbr.at[l, k], pb_s, pb_r.at[k], partner).wait_recv()
            return own + pbr[l, k].astype(F32)

        early = order[0]
        later = order[1:]
        tail = halves[1]

        def hop(o, at, l=l):
            src, dst = yss.at[l, o, at], ysr.at[l, o, at]
            return remote(src, dst, ys_s, ys_r.at[halves.index(at), o], facing)

        def turn(o, at, l=l):
            src, dst = rss.at[l, o, at], rsr.at[l, o, at]
            return remote(src, dst, rz_s, rs_r.at[halves.index(at), o], at_z(o, yy, core))

        def cross(l=l):
            return remote(rss.at[l, 0, tail], rsr.at[l, 0, tail], rz_s, rs_r.at[1, 0], at_z(early, yy, core))

        with scope(f"rsa{l}"):
            offer(early, 1)
            offer(early, 0)
            for o in later:
                offer(o, 1)
        with scope(f"rsb{l}"):
            both = paired(early, 1).astype(BF16)
            yss[l, early] = both
            hop(early, halves[0]).start()
            rss[l, 0, tail] = both[rows // 2 :]
            cross().start()
            osum[early] = paired(early, 0)
            rss[l, early, tail] = osum[early, tail].astype(BF16)
            turn(early, tail).start()
            for o in later[:-1]:
                yss[l, o] = paired(o, 1).astype(BF16)
                hop(o, halves[0]).start()
            osum[nz] = paired(0, 1)
            yss[l, 0, halves[0]] = osum[nz, halves[0]].astype(BF16)
            hop(0, halves[0]).start()
            for o in later[:-1]:
                hop(o, tail).start()
        with scope(f"rsc{l}"):
            for o in later:
                offer(o, 0)
            for o in near:
                k_y(o)
            drains.append((pbs.at[l], pb_s))
            drains.append((pbs.at[l, pl.ds(0, 2 * nz - 1), tail], ys_s))
            drains.append((pbs.at[l, pl.ds(0, 2 * nz - 1), tail], rz_s))
        with scope(f"own{l}"):
            for o in later:
                osum[o] = paired(o, 0)

        def join(o, at, l=l):
            with scope(f"rsd{l}{o}"):
                hop(o, at).wait_recv()
                own = osum[o, at] + ysr[l, o, at].astype(F32)
                if o:
                    rss[l, o, at] = own.astype(BF16)
                    turn(o, at).start()
                else:
                    osum[o, at] = own

        def finish(at, l=l):
            acc = osum[0, at] + xs[l, me, at].astype(F32)
            with scope(f"rse{l}"):
                for o in near:
                    turn(o, at).wait_recv()
                    acc = acc + rsr[l, o, at].astype(F32)
            return acc.astype(BF16)

        for o in order:
            join(o, halves[0])
        for o in later[:-1]:
            join(o, tail)
        with scope(f"cross{l}"):
            cross().wait_recv()
            yss[l, 0, tail] = (osum[nz, tail] + rsr[l, 0, tail].astype(F32)).astype(BF16)
            hop(0, tail).start()
        k_rest()
        with scope(f"update{l}"):
            lax.fori_loop(0, heads, update, 0, unroll=True)
        if l + 1 == layers:
            y_ref[halves[0], :] = finish(halves[0])
            join(0, tail)
            y_ref[tail, :] = finish(tail)
            continue

        rings = []
        clear()
        for i, at in enumerate(halves):
            rings.append(ring(f"x{l}{i}", xs.at[l + 1], ax_r.at[i], ag_s.at[l, 3 + i], at, (near[-1],) if i else ()))
            if i:
                join(0, tail)
            xs[l + 1, me, at] = finish(at)
            rings[i][0]()
        loads[("q", l + 1, 0)].wait()
        loads[("k", l + 1, 0)].wait()
        loads[("v", l + 1)].wait()
        loads[("g", l + 1)].wait()
        (_, az, ay, ad, _), (_, bz, by, bd, _) = rings

        def use(*which, l=l):
            for o, side in which:
                ad(o, side)
                bd(o, side)
            with scope(f"x{l}c{which[0][1]}{which[0][0]}"):
                for o, side in which:
                    c = chip_at(o, 1 - yy if side else yy)
                    absorb(l + 1, 2 * c, 2, lambda j: xs[l + 1, j].astype(F32))

        first, rest, end = near[0], near[1:], near[-1]
        az(first)
        ay(0)
        for o in rest:
            az(o)
        bz(first)
        ay(first)
        by(0)
        use((0, 0))
        for o in rest[:-1]:
            ay(o)
            bz(o)
        ay(end)
        bz(end)
        use((first, 0), (0, 1))
        by(first)
        use(*[(o, 0) for o in rest])
        for o in rest[:-1]:
            by(o)
        by(end)
        use(*[(o, 1) for o in near[:-1]])
        use((end, 1))

    with scope("drain"):
        for ref, sem in drains:
            remote(ref, ref, sem, st_r.at[0], partner).wait_send()


def store_kernel(y_ref, state_ref, y_out, state_out, yv, sem):
    layers, seqs = state_ref.shape[:2]
    copies = []
    parts = sem.shape[0] - 1
    per = layers * seqs // parts
    for i in range(parts):
        l, s = i * per // seqs, pl.ds(i * per % seqs, per)
        copies.append(pltpu.make_async_copy(state_ref.at[l, s], state_out.at[l, s], sem.at[i]))
    for copy in copies:
        copy.start()
    yv[...] = y_ref[...].astype(F32).reshape(yv.shape).astype(BF16)
    copy = pltpu.make_async_copy(yv, y_out, sem.at[parts])
    copy.start()
    for copy in copies + [copy]:
        copy.wait()


def local(
    stream_in, state_in, norm_gain, query_weight, key_weight,
    value_weight, gate_weight, group_gain, output_weight,
):
    n = lax.axis_size("tp")
    seqs, tok, width = stream_in.shape
    layers, _, heads, e_dim, head_dim = state_in.shape
    cols = query_weight.shape[2]
    rows = seqs * tok
    he = heads * e_dim
    share = width // n
    fits = (
        cols == 128 and head_dim == 256 and he == 128 and heads == 8 and e_dim == 16
        and share % 128 == 0 and n % 4 == 0 and n & (n - 1) == 0 and rows == 128 and 8 % tok == 0
        and n == 2 * heads and seqs % 4 == 0
    )
    if not fits:
        return plain_local(
            stream_in, state_in, norm_gain, query_weight, key_weight,
            value_weight, gate_weight, group_gain, output_weight,
        )
    nc = n // 2
    be = seqs * e_dim
    hbm = pl.BlockSpec(memory_space=pltpu.HBM)
    vmem = pl.BlockSpec(memory_space=pltpu.VMEM)
    dma = pltpu.SemaphoreType.DMA
    tables = jnp.asarray(rotary_tables(heads, tok, head_dim))
    flat = lambda w: jnp.transpose(w, (0, 2, 3, 1)).reshape(layers, he, width)
    y, new_state = pl.pallas_call(
        functools.partial(kernel, n, head_dim),
        name="retention",
        out_shape=(
            pltpu.VMEM((rows, share), BF16),
            pltpu.VMEM(state_in.shape, F32),
        ),
        in_specs=[hbm] * 10,
        out_specs=(vmem, vmem),
        scratch_shapes=[
            pltpu.VMEM(norm_gain.shape, BF16),
            pltpu.VMEM(group_gain.shape, BF16),
            pltpu.VMEM(tables.shape, F32),
            pltpu.VMEM((seqs, tok, width), BF16),
            pltpu.VMEM((layers, n, rows, share), BF16),
            pltpu.VMEM((rows, width), BF16),
            pltpu.VMEM((layers, width, 2 * cols), BF16),
            pltpu.VMEM((layers, 2 * he, width), BF16),
            pltpu.VMEM((layers, he, width), BF16),
            pltpu.VMEM((layers, n, rows, cols), BF16),
            pltpu.VMEM((layers, n, rows, cols), BF16),
            pltpu.VMEM((layers, heads, 8, rows), F32),
            pltpu.VMEM((he, rows), BF16),
            pltpu.VMEM((tok, rows, he), F32),
            pltpu.VMEM((layers, n, heads, 2 * rows), BF16),
            pltpu.VMEM((layers, nc, rows, share), BF16),
            pltpu.VMEM((layers, nc, rows, share), BF16),
            pltpu.VMEM((layers, nc // 2, rows, share), BF16),
            pltpu.VMEM((layers, nc // 2, rows, share), BF16),
            pltpu.VMEM((layers, nc // 2, rows, share), BF16),
            pltpu.VMEM((layers, nc // 2, rows, share), BF16),
            pltpu.VMEM((rows, be), BF16),
            pltpu.VMEM((be, rows), BF16),
            pltpu.VMEM((be, he), BF16),
            pltpu.VMEM((rows, share), F32),
            pltpu.VMEM((rows, 2 * cols), F32),
            pltpu.VMEM((rows, 2 * he), F32),
            pltpu.VMEM((nc // 2 + 1, rows, share), F32),
            dma((3 * XPARTS + 6 * layers + 1,)),
            dma((layers, 5)),
            dma((layers,)),
            dma((layers, 3)),
            dma((n,)),
            dma((nc + 2,)),
            dma((2, n)),
            dma((1,)),
            dma((1,)),
            dma((nc,)),
            dma((2, nc // 2)),
            dma((2, nc // 2)),
        ],
        compiler_params=pltpu.CompilerParams(
            collective_id=0, has_side_effects=True, vmem_limit_bytes=58500000
        ),
    )(
        stream_in, state_in, norm_gain, query_weight, key_weight,
        flat(value_weight), flat(gate_weight), group_gain,
        output_weight.reshape(layers, he, width), tables,
    )
    return pl.pallas_call(
        store_kernel,
        name="store",
        out_shape=(
            jax.ShapeDtypeStruct((seqs, tok, share), BF16),
            jax.ShapeDtypeStruct(state_in.shape, F32),
        ),
        in_specs=[vmem, vmem],
        out_specs=(hbm, hbm),
        scratch_shapes=[pltpu.VMEM((seqs, tok, share), BF16), dma((4 * layers + 1,))],
        compiler_params=pltpu.CompilerParams(vmem_limit_bytes=2 * 2**20),
    )(y, new_state)


def solution(mesh):
    in_specs = (
        P("grp", None, None),
        P(None, "grp", None, "tp", None),
        P(),
        P(None, None, "tp"),
        P(None, None, "tp"),
        P(None, None, None, "tp"),
        P(None, None, None, "tp"),
        P(None, None, "tp"),
        P(None, None, "tp", None),
    )
    out_specs = (P("grp", None, "tp"), P(None, "grp", None, "tp", None))
    return jax.shard_map(local, mesh=mesh, in_specs=in_specs, out_specs=out_specs, check_vma=False)
```

```python
import functools

import jax
import jax.numpy as jnp
import numpy as np
from jax import lax
from jax.experimental import pallas as pl
from jax.experimental.pallas import tpu as pltpu
from jax.sharding import PartitionSpec as P

HEAD_DIM = 256
PAST = 1024


EPS_RMS = 1e-06
EPS_GROUP = 1e-05
ROTARY_BASE = 10000.0


def log_decays(count):
    return jnp.log(1.0 - jnp.power(2.0, -5.0 - jnp.arange(count, dtype=jnp.float32)))


def decay_tables(log_gamma, count):
    steps = jnp.arange(count, dtype=jnp.float32)
    gap = steps[:, None] - steps[None, :]
    intra = jnp.where(
        gap[None] >= 0, jnp.exp(log_gamma[:, None, None] * jnp.maximum(gap, 0.0)[None]), 0.0
    )
    q_decay = jnp.exp(log_gamma[None, :] * (steps[:, None] + 1.0))
    k_decay = jnp.exp(log_gamma[None, :] * (count - 1.0 - steps[:, None]))
    block_decay = jnp.exp(log_gamma * count)
    return (intra, q_decay, k_decay, block_decay)


def rotate(values, offset):
    half_dim = values.shape[-1] // 2
    freqs = jnp.power(
        ROTARY_BASE, -jnp.arange(half_dim, dtype=jnp.float32) * (2.0 / values.shape[-1])
    )
    places = (offset + jnp.arange(values.shape[1])).astype(jnp.float32)
    angles = places[:, None] * freqs[None, :]
    cosine = jnp.cos(angles)[None, :, None, :]
    sine = jnp.sin(angles)[None, :, None, :]
    first = values[..., :half_dim]
    second = values[..., half_dim:]
    return jnp.concatenate(
        [first * cosine - second * sine, second * cosine + first * sine], axis=-1
    )


def plain_local(
    stream_in,
    state_in,
    norm_gain,
    query_weight,
    key_weight,
    value_weight,
    gate_weight,
    group_gain,
    output_weight,
):
    seqs, new_tok, width = stream_in.shape
    heads, local_dim = (value_weight.shape[2], value_weight.shape[3])
    head_dim = HEAD_DIM
    log_gamma = log_decays(heads)
    intra, q_decay, k_decay, block_decay = decay_tables(log_gamma, new_tok)
    highest = lax.Precision.HIGHEST
    share_cols = width // lax.axis_size("tp")
    col_start = lax.axis_index("tp") * share_cols
    layers = state_in.shape[0]
    stream = stream_in
    stream_share = stream_in
    new_states = []
    for layer_no in range(layers):
        stream_f = stream.astype(jnp.float32)
        normed = stream_f * lax.rsqrt(
            jnp.mean(stream_f * stream_f, axis=-1, keepdims=True) + EPS_RMS
        )
        normed = (normed * norm_gain[layer_no].astype(jnp.float32)).astype(jnp.bfloat16)
        flat = normed.reshape(seqs * new_tok, width)
        query_part = jnp.dot(flat, query_weight[layer_no], preferred_element_type=jnp.float32)
        query_part = query_part.astype(jnp.bfloat16).reshape(seqs, new_tok, -1)
        key_part = jnp.dot(flat, key_weight[layer_no], preferred_element_type=jnp.float32)
        key_part = key_part.astype(jnp.bfloat16).reshape(seqs, new_tok, -1)

        def project_local(weight):
            result = jnp.dot(
                flat, weight.reshape(width, heads * local_dim), preferred_element_type=jnp.float32
            )
            result = lax.optimization_barrier(result.astype(jnp.bfloat16))
            return result.astype(jnp.float32).reshape(seqs, new_tok, heads, local_dim)

        values_f = project_local(value_weight[layer_no])
        gates_f = project_local(gate_weight[layer_no])
        queries, key_rows = (
            lax.all_gather(query_part, "tp", axis=2, tiled=True),
            lax.all_gather(key_part, "tp", axis=2, tiled=True),
        )
        queries = queries.astype(jnp.float32).reshape(seqs, new_tok, heads, head_dim)
        key_rows = key_rows.astype(jnp.float32).reshape(seqs, new_tok, heads, head_dim)
        rot_q = rotate(queries, PAST)
        rot_k = rotate(key_rows, PAST) * head_dim ** (-0.5)
        scores = jnp.einsum("bthd,bshd->bhts", rot_q, rot_k, precision=highest) * intra[None]
        inner = jnp.einsum("bhts,bshe->bthe", scores, values_f, precision=highest)
        state = state_in[layer_no]
        carried = (
            jnp.einsum("bthd,bhed->bthe", rot_q, state, precision=highest)
            * q_decay[None, :, :, None]
        )
        mixed = inner + carried
        new_state = state * block_decay[None, :, None, None] + jnp.einsum(
            "bthe,bthd->bhed", values_f, rot_k * k_decay[None, :, :, None], precision=highest
        )
        new_states.append(new_state)
        totals, squares = lax.psum((jnp.sum(mixed, axis=-1), jnp.sum(mixed * mixed, axis=-1)), "tp")
        mean_o = (totals / head_dim)[..., None]
        var_o = (squares / head_dim)[..., None] - mean_o * mean_o
        normal = (
            (mixed - mean_o)
            * lax.rsqrt(var_o + EPS_GROUP)
            * group_gain[layer_no].astype(jnp.float32)[None, None]
        )
        gated = (jax.nn.silu(gates_f) * normal).astype(jnp.bfloat16)
        partial_out = jnp.dot(
            gated.reshape(seqs * new_tok, heads * local_dim),
            output_weight[layer_no].reshape(heads * local_dim, width),
            preferred_element_type=jnp.float32,
        ).reshape(seqs, new_tok, width)
        share_out = lax.psum_scatter(partial_out, "tp", scatter_dimension=2, tiled=True)
        own_cols = lax.dynamic_slice_in_dim(stream, col_start, share_cols, 2)
        stream_share = (own_cols.astype(jnp.float32) + share_out).astype(jnp.bfloat16)
        if layer_no + 1 < layers:
            stream = lax.all_gather(stream_share, "tp", axis=2, tiled=True)
    result = stream_share
    return (result, jnp.stack(new_states))


F32 = jnp.float32
BF16 = jnp.bfloat16
XPARTS = 4
scope = jax.named_scope


def nt_dot(a, b, precision=None):
    return lax.dot_general(
        a, b, (((1,), (1,)), ((), ())), preferred_element_type=F32, precision=precision
    )


def thirds(value, axis):
    high = value.astype(BF16)
    rest = value - high.astype(F32)
    middle = rest.astype(BF16)
    low = (rest - middle.astype(F32)).astype(BF16)
    return jnp.concatenate([high, middle, low], axis=axis)


def log2(value):
    return int(value).bit_length() - 1


def rotary_tables(heads, new_tok, head_dim):
    half = head_dim // 2
    freqs = np.power(
        np.float32(ROTARY_BASE), -np.arange(half, dtype=np.float32) * np.float32(2.0 / head_dim)
    ).astype(np.float32)
    tok = np.arange(8) % new_tok
    places = (PAST + tok).astype(np.float32)
    angles = (places[:, None] * freqs[None, :]).astype(np.float32).astype(np.float64)
    gamma = 1.0 - np.power(2.0, -5.0 - np.arange(heads))
    grow = np.power(gamma[:, None], tok[None, :] + 1.0)[:, :, None]
    shrink = head_dim ** (-0.5) / grow
    cosine, sine = np.cos(angles)[None], np.sin(angles)[None]
    block = np.broadcast_to(np.power(gamma, new_tok)[:, None, None], (heads, 8, half))
    return np.stack(
        [cosine * grow, sine * grow, cosine * shrink, sine * shrink, block]
    ).astype(np.float32)


def kernel(
    n, head_dim,
    x_hbm, st_hbm, ng_hbm, qw_hbm, kw_hbm, vw_hbm, gw_hbm, gg_hbm, ow_hbm, tab_hbm,
    y_ref, stv,
    ng_ref, gg_ref, tab_ref, xr, xs, nv, wqk, wvg, wo, qg, kg, sc, vts, vb, sb, pbs, pbr, yss, ysr, rss, rsr, mkc, mks, fold, sqa, qka, vga, osum,
    lsem, ag_s, st_s, rs_s, aq_r, ak_r, ax_r, sc_r, st_r, pb_r, ys_r, rs_r,
):
    layers, seqs, heads, e_dim, _ = st_hbm.shape
    tok = x_hbm.shape[1]
    width = x_hbm.shape[2]
    rows = seqs * tok
    share = width // n
    cols = qw_hbm.shape[2]
    he = heads * e_dim
    half = head_dim // 2
    nc = n // 2
    me = lax.axis_index("tp")
    core = lax.rem(me, 2)
    chip = lax.div(me, 2)
    partner = chip * 2 + 1 - core

    nz = nc // 2
    yy = lax.rem(chip, 2)
    zz = lax.div(chip, 2)

    def chip_at(o, y):
        z, bit = zz, 1
        while bit < nz:
            if o & bit:
                z = z + bit - 2 * bit * lax.rem(lax.div(z, bit), 2)
            bit = 2 * bit
        return z * 2 + y

    def at_z(o, y, c):
        return chip_at(o, y) * 2 + c

    facing = at_z(0, 1 - yy, core)
    far = list(range(2, nz)) + [1]
    near = [1] + list(range(nz - 1, 1, -1))

    def remote(src, dst, ssem, rsem, device):
        return pltpu.make_async_remote_copy(
            src_ref=src, dst_ref=dst, send_sem=ssem, recv_sem=rsem,
            device_id={"tp": device}, device_id_type=pl.DeviceIdType.MESH,
        )

    loads = {}
    count = 0

    def load(name, src, dst):
        nonlocal count
        loads[name] = pltpu.make_async_copy(src, dst, lsem.at[count])
        loads[name].start()
        count += 1

    wide = width // XPARTS

    def load_queries(l, deep, j):
        at = pl.ds(j * deep, deep)
        load(("q", l, j), qw_hbm.at[l, at], wqk.at[l, at, pl.ds(0, cols)])
        load(("k", l, j), kw_hbm.at[l, at], wqk.at[l, at, pl.ds(cols, cols)])

    load("ng", ng_hbm, ng_ref)
    for j in range(XPARTS):
        at = pl.ds(j * wide, wide)
        load(("x", j), x_hbm.at[:, :, at], xr.at[:, :, at])
        load_queries(0, wide, j)

    barrier = pltpu.get_barrier_semaphore()
    for o in range(1, n):
        pl.semaphore_signal(
            barrier, inc=1, device_id={"tp": lax.rem(me + o, n)},
            device_id_type=pl.DeviceIdType.MESH,
        )

    def load_rest():
        for l in range(layers):
            if l:
                load_queries(l, width, 0)
            load(("v", l), vw_hbm.at[l], wvg.at[l, pl.ds(0, he)])
            load(("g", l), gw_hbm.at[l], wvg.at[l, pl.ds(he, he)])
            load(("s", l), st_hbm.at[l], stv.at[l])
            if l == 0:
                load("tab", tab_hbm, tab_ref)
                load("gg", gg_hbm, gg_ref)
            load(("o", l), ow_hbm.at[l], wo.at[l])

    be = seqs * e_dim

    def iota(shape, dim, shift=0):
        return jnp.right_shift(lax.broadcasted_iota(jnp.int32, shape, dim), shift)

    te, tt = log2(e_dim), log2(tok)
    low = e_dim - 1
    causal = (
        (iota((rows, rows), 0, tt) == iota((rows, rows), 1, tt))
        & (iota((rows, rows), 0) >= iota((rows, rows), 1))
    ).astype(F32)
    heads_of = (iota((heads, he), 0) == iota((heads, he), 1, te)).astype(F32)
    place = (
        iota((e_dim, he), 0) == jnp.bitwise_and(iota((e_dim, he), 1), low)
    ).astype(F32)
    nth = jnp.concatenate(
        [
            (
                jnp.left_shift(iota((rows, rows), 0, tt), tt) + t == iota((rows, rows), 1)
            ).astype(F32).astype(BF16)
            for t in range(tok)
        ],
        axis=0,
    )
    pick = (
        jnp.bitwise_and(iota((8, rows), 1), tok - 1) == iota((8, rows), 0)
    ).astype(F32).astype(BF16)
    highest = lax.Precision.HIGHEST

    def make_masks():
        mkc[...] = (iota((rows, be), 0, tt) == iota((rows, be), 1, te)).astype(F32).astype(BF16)
        mks[...] = (iota((be, rows), 0, te) == iota((be, rows), 1, tt)).astype(F32).astype(BF16)
        fold[...] = (
            jnp.bitwise_and(iota((be, he), 0), low) == jnp.bitwise_and(iota((be, he), 1), low)
        ).astype(F32).astype(BF16)

    drains = []
    halves = [pl.ds(i * (rows // 2), rows // 2) for i in range(2)]

    def ring(name, buf, recv, send, at=None, direct=(), twice=()):
        def slot_of(j):
            return buf.at[j] if at is None else buf.at[j, at]

        def push(slot, k, device):
            remote(slot, slot, send, recv.at[k], device).start()

        def arrive(slot, k):
            remote(slot, slot, send, recv.at[k], partner).wait_recv()

        def start(others=True, other_core=True):
            own = slot_of(me)
            if other_core:
                push(own, nc, partner)
            if others:
                push(own, nz, facing)
                for o in near:
                    push(own, o, at_z(o, yy, core))
                drains.append((slot_of(pl.ds(0, n - 1)), send))

        def last(k):
            return k if recv.shape[0] == n else nc if k == nc else nc + 1

        def from_z(o):
            with scope(f"{name}z{o}"):
                slot = slot_of(at_z(o, yy, core))
                arrive(slot, o)
                if o not in direct:
                    push(slot, nz + o, facing)
                if o in twice:
                    push(slot, nc + nz + o, at_z(0, 1 - yy, 1 - core))
                push(slot, last(nc + o), partner)

        def from_y(o):
            with scope(f"{name}y{o}"):
                slot = slot_of(at_z(o, 1 - yy, core))
                arrive(slot, nz + o)
                for far_o in direct if o == 0 else ():
                    push(slot, nz + far_o, at_z(far_o, yy, core))
                if o not in twice:
                    push(slot, last(nc + nz + o), partner)

        def done(o, side):
            with scope(f"{name}d{side}{o}"):
                arrive(slot_of(at_z(o, 1 - yy if side else yy, 1 - core)), nc + nz * side + o)

        def done_rest():
            with scope(name + "rest"):
                arrive(slot_of(pl.ds(0, nc - 1)), nc + 1)

        return start, from_z, from_y, done, done_rest

    def in_order(name, from_z, from_y, done, on_chip, early, between, later):
        def use(*which):
            for o, side in which:
                done(o, side)
            with scope(f"{name}c{which[0][1]}{which[0][0]}"):
                on_chip(which)

        use((0, 0))
        from_z(near[0])
        from_y(0)
        early()
        for o in near[1:]:
            from_z(o)
        use((near[0], 0), (0, 1))
        from_y(near[0])
        use(*[(o, 0) for o in near[1:]])
        for o in near[1:-1]:
            from_y(o)
        between()
        from_y(near[-1])
        later()
        use(*[(o, 1) for o in near[:-1]])
        use((near[-1], 1))

    def spread(table):
        return jnp.broadcast_to(table[None], (rows // 8, 8, half)).reshape(rows, half)

    def rotated(buf, l, h, table):
        a, b = buf[l, 2 * h].astype(F32), buf[l, 2 * h + 1].astype(F32)
        cosine, sine = spread(tab_ref[table, h]), spread(tab_ref[table + 1, h])
        return jnp.concatenate([a * cosine - b * sine, b * cosine + a * sine], axis=1).astype(BF16)

    def absorb(l, j, count, block_of):
        at = pl.ds(pl.multiple_of(j * share, share), share * count)
        parts = []
        square = sqa[...]
        for i in range(count):
            block = block_of(j + i)
            for k in range(0, share, 128):
                square = square + block[:, k : k + 128] * block[:, k : k + 128]
            one = pl.ds(pl.multiple_of((j + i) * share, share), share)
            gain = ng_ref[l : l + 1, one].astype(F32)
            scaled = (block * gain).astype(BF16)
            nv[:, one] = scaled
            parts.append(scaled)
        sqa[...] = square
        both = jnp.concatenate(parts, axis=1) if count > 1 else parts[0]
        qka[...] += jnp.dot(both, wqk[l, at, :], preferred_element_type=F32)
        if l:
            vga[...] += nt_dot(both, wvg[l, :, at])

    def unpack(j):
        at = pl.ds(j * share if isinstance(j, int) else pl.multiple_of(j * share, share), share)
        return xr[:, :, at].astype(F32).reshape(rows, share)

    def clear():
        sqa[...] = jnp.zeros_like(sqa)
        qka[...] = jnp.zeros_like(qka)
        vga[...] = jnp.zeros_like(vga)

    for l in range(layers):
        if l == 0:
            with scope("absorb"):
                clear()
                per = n // XPARTS
                loads["ng"].wait()
                for p in range(XPARTS):
                    with scope(f"await{p}"):
                        for name in (("x", p), ("q", 0, p), ("k", 0, p)):
                            loads[name].wait()
                    if p == XPARTS - 1:
                        load_rest()
                    absorb(0, p * per, per, unpack)

        with scope(f"qk{l}"):
            scale = lax.rsqrt(jnp.sum(sqa[...], axis=1, keepdims=True) / width + EPS_RMS)
            both = (qka[...] * scale).astype(BF16)
            qg[l, me] = both[:, :cols]
            kg[l, me] = both[:, cols:]
        if l == 0:
            with scope("bar"):
                pl.semaphore_wait(barrier, n - 1)

        q_start, q_z, q_y, q_done, _ = ring(f"q{l}", qg.at[l], aq_r, ag_s.at[l, 0], None, (), (near[-1],))
        k_start, k_z, k_y, k_done, k_rest = ring(f"k{l}", kg.at[l], ak_r, ag_s.at[l, 1])
        q_start()
        k_start(others=False)
        if l == 0:
            with scope("masks"):
                make_masks()
                xs[0, me] = unpack(me).astype(BF16)
                loads["tab"].wait()
                loads["gg"].wait()
        q_done(0, 0)
        k_done(0, 0)
        with scope(f"scores{l}"):
            rk = rotated(kg, l, chip, 2)
            scores = (nt_dot(rotated(qg, l, chip, 0), rk) * causal).astype(BF16)
            sc[l, chip] = nt_dot(pick, scores)
            for o, side in [(o, side) for o in far for side in (1, 0)] + [(0, 1)]:
                slot = sc.at[l, chip]
                remote(
                    slot, slot, ag_s.at[l, 2], sc_r.at[0],
                    at_z(o, 1 - yy if side else yy, core),
                ).start()
            drains.append((sc.at[l, pl.ds(0, nc - 1)], ag_s.at[l, 2]))
        k_start(other_core=False)

        with scope(f"vg{l}"):
            if l == 0:
                loads[("v", l)].wait()
                vga[:, :he] = nt_dot(nv[...], wvg[l, :he])
            values = (vga[:, :he] * scale).astype(BF16)
            vts[...] = jnp.transpose(values.astype(F32)).astype(BF16)
            vb[...] = jnp.dot(nth, values, preferred_element_type=F32).reshape(tok, rows, he)
            loads[("s", l)].wait()
        box = {"mixed": jnp.zeros((rows, he), F32)}

        def gate_on(l=l):
            if l == 0:
                with scope(f"gates{l}"):
                    loads[("g", l)].wait()
                    vga[:, he:] = nt_dot(nv[...], wvg[l, he:])

        def carry_one(o, side, l=l):
            h = chip_at(o, 1 - yy if side else yy)
            rq = rotated(qg, l, h, 0)
            state = stv[l, :, h].reshape(be, head_dim).astype(BF16)
            carried = nt_dot(rq, state).astype(BF16) * mkc[...]
            part = jnp.dot(carried, fold[...], preferred_element_type=F32)
            return part * (iota((1, he), 1, te) == h).astype(F32)

        def intra(l=l, box=box):
            with scope(f"intra{l}"):
                others = sc.at[l, pl.ds(0, nc - 1)]
                remote(others, others, ag_s.at[l, 2], sc_r.at[0], partner).wait_recv()
                flat = jnp.concatenate([sc[l, :, t, :] for t in range(tok)], axis=1).astype(BF16)
                wide = lax.dot_general(
                    flat, heads_of.astype(BF16), (((0,), (0,)), ((), ())), preferred_element_type=F32
                )
                box["mixed"] = box["mixed"] + jnp.sum(wide.reshape(tok, rows, he) * vb[...], axis=0)

        def k_on(k_z=k_z, k_y=k_y):
            for o in near:
                k_z(o)
            k_y(0)

        def mix(which, box=box):
            for o, side in which:
                box["mixed"] = box["mixed"] + carry_one(o, side)

        in_order(f"q{l}", q_z, q_y, lambda o, s: None if o == s == 0 else q_done(o, s), mix, gate_on, intra, k_on)
        mixed = box["mixed"]

        with scope(f"sums{l}"):
            both = nt_dot(
                jnp.concatenate([heads_of.astype(BF16)] * 3, axis=1),
                thirds(jnp.concatenate([mixed, mixed * mixed], axis=0), 1),
            )
            sums = both[:, :rows]
            squares = jnp.maximum(both[:, rows:] - sums * sums / e_dim, 0.0)
            sb[l, me] = jnp.concatenate([sums, squares], axis=1).astype(BF16)
            peers = [at_z(o, y, c) for o in far for y in (1 - yy, yy) for c in (core, 1 - core)]
            for device in peers + [at_z(0, 1 - yy, 1 - core), facing, partner]:
                remote(sb.at[l, me], sb.at[l, me], st_s.at[l], st_r.at[0], device).start()
            drains.append((sb.at[l, pl.ds(0, n - 1)], st_s.at[l]))

        def update(h, carry, l=l):
            at = pl.ds(pl.multiple_of(h * e_dim, e_dim), e_dim)
            tall = jnp.broadcast_to(vts[at, :][None], (seqs, e_dim, rows)).reshape(be, rows)
            fresh = jnp.dot(tall * mks[...], rotated(kg, l, h, 2), preferred_element_type=F32)
            row = tab_ref[4, h][0:1, :]
            fade = jnp.concatenate([row, row], axis=1)
            state = stv[l, :, h].reshape(be, head_dim)
            stv[l, :, h] = ((state + fresh) * fade).reshape(seqs, e_dim, head_dim)
            return carry

        with scope(f"silu{l}"):
            gates = (vga[:, he:] * scale).astype(BF16).astype(F32)
            gain = jnp.dot(gg_ref[l].astype(F32), place, preferred_element_type=F32, precision=highest)
            gain = jnp.sum(gain * heads_of, axis=0, keepdims=True)
            gains = gates / (1.0 + jnp.exp(-gates)) * gain

        with scope(f"stwait{l}"):
            others = sb.at[l, pl.ds(0, n - 1)]
            remote(others, others, st_s.at[l], st_r.at[0], partner).wait_recv()

        with scope(f"gated{l}"):
            stats = sb[l].astype(F32)
            sums = stats[:, :, :rows]
            total = jnp.sum(sums, axis=0)
            off = sums - (total / n)[None]
            var = jnp.sum(stats[:, :, rows:] + off * off / e_dim, axis=0) / head_dim
            both = jnp.concatenate([total / head_dim, lax.rsqrt(var + EPS_GROUP)], axis=1)
            both = lax.dot_general(
                thirds(both, 0), jnp.concatenate([heads_of.astype(BF16)] * 3, axis=0),
                (((0,), (0,)), ((), ())), preferred_element_type=F32,
            )
            gated = ((mixed - both[:rows]) * both[rows:] * gains).astype(BF16)
            loads[("o", l)].wait()

        def chunk(j, l=l, gated=gated):
            at = pl.ds(pl.multiple_of(j * share, share), share)
            return jnp.dot(gated, wo[l, :, at], preferred_element_type=F32)

        order = list(range(nz - 1, -1, -1))
        pb_s, ys_s, rz_s = rs_s.at[l, 0], rs_s.at[l, 1], rs_s.at[l, 2]

        def offer(o, side, l=l):
            k = side * nz + o
            y = 1 - yy if side else yy
            pbs[l, k] = chunk(at_z(o, y, 1 - core)).astype(BF16)
            remote(pbs.at[l, k], pbr.at[l, k], pb_s, pb_r.at[k], partner).start()

        def paired(o, side, l=l):
            k = side * nz + o
            own = chunk(at_z(o, 1 - yy if side else yy, core))
            remote(pbs.at[l, k], pbr.at[l, k], pb_s, pb_r.at[k], partner).wait_recv()
            return own + pbr[l, k].astype(F32)

        early = order[0]
        later = order[1:]
        tail = halves[1]

        def hop(o, at, l=l):
            src, dst = yss.at[l, o, at], ysr.at[l, o, at]
            return remote(src, dst, ys_s, ys_r.at[halves.index(at), o], facing)

        def turn(o, at, l=l):
            src, dst = rss.at[l, o, at], rsr.at[l, o, at]
            return remote(src, dst, rz_s, rs_r.at[halves.index(at), o], at_z(o, yy, core))

        def cross(l=l):
            return remote(rss.at[l, 0, tail], rsr.at[l, 0, tail], rz_s, rs_r.at[1, 0], at_z(early, yy, core))

        with scope(f"rsa{l}"):
            offer(early, 1)
            offer(early, 0)
            for o in later:
                offer(o, 1)
        with scope(f"rsb{l}"):
            both = paired(early, 1).astype(BF16)
            yss[l, early] = both
            hop(early, halves[0]).start()
            rss[l, 0, tail] = both[rows // 2 :]
            cross().start()
            osum[early] = paired(early, 0)
            rss[l, early, tail] = osum[early, tail].astype(BF16)
            turn(early, tail).start()
            for o in later[:-1]:
                yss[l, o] = paired(o, 1).astype(BF16)
                hop(o, halves[0]).start()
            osum[nz] = paired(0, 1)
            yss[l, 0, halves[0]] = osum[nz, halves[0]].astype(BF16)
            hop(0, halves[0]).start()
            for o in later[:-1]:
                hop(o, tail).start()
        with scope(f"rsc{l}"):
            for o in later:
                offer(o, 0)
            for o in near:
                k_y(o)
            drains.append((pbs.at[l], pb_s))
            drains.append((pbs.at[l, pl.ds(0, 2 * nz - 1), tail], ys_s))
            drains.append((pbs.at[l, pl.ds(0, 2 * nz - 1), tail], rz_s))
        with scope(f"own{l}"):
            for o in later:
                osum[o] = paired(o, 0)

        def join(o, at, l=l):
            with scope(f"rsd{l}{o}"):
                hop(o, at).wait_recv()
                own = osum[o, at] + ysr[l, o, at].astype(F32)
                if o:
                    rss[l, o, at] = own.astype(BF16)
                    turn(o, at).start()
                else:
                    osum[o, at] = own

        def finish(at, l=l):
            acc = osum[0, at] + xs[l, me, at].astype(F32)
            with scope(f"rse{l}"):
                for o in near:
                    turn(o, at).wait_recv()
                    acc = acc + rsr[l, o, at].astype(F32)
            return acc.astype(BF16)

        for o in order:
            join(o, halves[0])
        with scope(f"cross{l}"):
            cross().wait_recv()
            yss[l, 0, tail] = (osum[nz, tail] + rsr[l, 0, tail].astype(F32)).astype(BF16)
            hop(0, tail).start()
        for o in later[:-1]:
            join(o, tail)
        k_rest()
        with scope(f"update{l}"):
            lax.fori_loop(0, heads, update, 0, unroll=True)
        if l + 1 == layers:
            y_ref[halves[0], :] = finish(halves[0])
            join(0, tail)
            y_ref[tail, :] = finish(tail)
            continue

        rings = []
        clear()
        for i, at in enumerate(halves):
            rings.append(ring(f"x{l}{i}", xs.at[l + 1], ax_r.at[i], ag_s.at[l, 3 + i], at, (near[-1],) if i else ()))
            if i:
                join(0, tail)
            xs[l + 1, me, at] = finish(at)
            rings[i][0]()
        loads[("q", l + 1, 0)].wait()
        loads[("k", l + 1, 0)].wait()
        loads[("v", l + 1)].wait()
        loads[("g", l + 1)].wait()
        (_, az, ay, ad, _), (_, bz, by, bd, _) = rings

        def use(*which, l=l):
            for o, side in which:
                ad(o, side)
                bd(o, side)
            with scope(f"x{l}c{which[0][1]}{which[0][0]}"):
                for o, side in which:
                    c = chip_at(o, 1 - yy if side else yy)
                    absorb(l + 1, 2 * c, 2, lambda j: xs[l + 1, j].astype(F32))

        first, rest, end = near[0], near[1:], near[-1]
        az(first)
        ay(0)
        for o in rest:
            az(o)
        bz(first)
        ay(first)
        by(0)
        use((0, 0))
        for o in rest[:-1]:
            ay(o)
            bz(o)
        ay(end)
        bz(end)
        use((first, 0), (0, 1))
        by(first)
        use(*[(o, 0) for o in rest])
        by(end)
        for o in rest[:-1]:
            by(o)
        use((first, 1), (end, 1))
        use(*[(o, 1) for o in rest[:-1]])

    with scope("drain"):
        for ref, sem in drains:
            remote(ref, ref, sem, st_r.at[0], partner).wait_send()


def store_kernel(y_ref, state_ref, y_out, state_out, yv, sem):
    layers, seqs = state_ref.shape[:2]
    copies = []
    parts = sem.shape[0] - 1
    per = layers * seqs // parts
    for i in range(parts):
        l, s = i * per // seqs, pl.ds(i * per % seqs, per)
        copies.append(pltpu.make_async_copy(state_ref.at[l, s], state_out.at[l, s], sem.at[i]))
    for copy in copies:
        copy.start()
    yv[...] = y_ref[...].astype(F32).reshape(yv.shape).astype(BF16)
    copy = pltpu.make_async_copy(yv, y_out, sem.at[parts])
    copy.start()
    for copy in copies + [copy]:
        copy.wait()


def local(
    stream_in, state_in, norm_gain, query_weight, key_weight,
    value_weight, gate_weight, group_gain, output_weight,
):
    n = lax.axis_size("tp")
    seqs, tok, width = stream_in.shape
    layers, _, heads, e_dim, head_dim = state_in.shape
    cols = query_weight.shape[2]
    rows = seqs * tok
    he = heads * e_dim
    share = width // n
    fits = (
        cols == 128 and head_dim == 256 and he == 128 and heads == 8 and e_dim == 16
        and share % 128 == 0 and n % 4 == 0 and n & (n - 1) == 0 and rows == 128 and 8 % tok == 0
        and n == 2 * heads and seqs % 4 == 0
    )
    if not fits:
        return plain_local(
            stream_in, state_in, norm_gain, query_weight, key_weight,
            value_weight, gate_weight, group_gain, output_weight,
        )
    nc = n // 2
    be = seqs * e_dim
    hbm = pl.BlockSpec(memory_space=pltpu.HBM)
    vmem = pl.BlockSpec(memory_space=pltpu.VMEM)
    dma = pltpu.SemaphoreType.DMA
    tables = jnp.asarray(rotary_tables(heads, tok, head_dim))
    flat = lambda w: jnp.transpose(w, (0, 2, 3, 1)).reshape(layers, he, width)
    y, new_state = pl.pallas_call(
        functools.partial(kernel, n, head_dim),
        name="retention",
        out_shape=(
            pltpu.VMEM((rows, share), BF16),
            pltpu.VMEM(state_in.shape, F32),
        ),
        in_specs=[hbm] * 10,
        out_specs=(vmem, vmem),
        scratch_shapes=[
            pltpu.VMEM(norm_gain.shape, BF16),
            pltpu.VMEM(group_gain.shape, BF16),
            pltpu.VMEM(tables.shape, F32),
            pltpu.VMEM((seqs, tok, width), BF16),
            pltpu.VMEM((layers, n, rows, share), BF16),
            pltpu.VMEM((rows, width), BF16),
            pltpu.VMEM((layers, width, 2 * cols), BF16),
            pltpu.VMEM((layers, 2 * he, width), BF16),
            pltpu.VMEM((layers, he, width), BF16),
            pltpu.VMEM((layers, n, rows, cols), BF16),
            pltpu.VMEM((layers, n, rows, cols), BF16),
            pltpu.VMEM((layers, heads, 8, rows), F32),
            pltpu.VMEM((he, rows), BF16),
            pltpu.VMEM((tok, rows, he), F32),
            pltpu.VMEM((layers, n, heads, 2 * rows), BF16),
            pltpu.VMEM((layers, nc, rows, share), BF16),
            pltpu.VMEM((layers, nc, rows, share), BF16),
            pltpu.VMEM((layers, nc // 2, rows, share), BF16),
            pltpu.VMEM((layers, nc // 2, rows, share), BF16),
            pltpu.VMEM((layers, nc // 2, rows, share), BF16),
            pltpu.VMEM((layers, nc // 2, rows, share), BF16),
            pltpu.VMEM((rows, be), BF16),
            pltpu.VMEM((be, rows), BF16),
            pltpu.VMEM((be, he), BF16),
            pltpu.VMEM((rows, 128), F32),
            pltpu.VMEM((rows, 2 * cols), F32),
            pltpu.VMEM((rows, 2 * he), F32),
            pltpu.VMEM((nc // 2 + 1, rows, share), F32),
            dma((3 * XPARTS + 6 * layers + 1,)),
            dma((layers, 5)),
            dma((layers,)),
            dma((layers, 3)),
            dma((n,)),
            dma((nc + 2,)),
            dma((2, n)),
            dma((1,)),
            dma((1,)),
            dma((nc,)),
            dma((2, nc // 2)),
            dma((2, nc // 2)),
        ],
        compiler_params=pltpu.CompilerParams(
            collective_id=0, has_side_effects=True, vmem_limit_bytes=58500000
        ),
    )(
        stream_in, state_in, norm_gain, query_weight, key_weight,
        flat(value_weight), flat(gate_weight), group_gain,
        output_weight.reshape(layers, he, width), tables,
    )
    return pl.pallas_call(
        store_kernel,
        name="store",
        out_shape=(
            jax.ShapeDtypeStruct((seqs, tok, share), BF16),
            jax.ShapeDtypeStruct(state_in.shape, F32),
        ),
        in_specs=[vmem, vmem],
        out_specs=(hbm, hbm),
        scratch_shapes=[pltpu.VMEM((seqs, tok, share), BF16), dma((4 * layers + 1,))],
        compiler_params=pltpu.CompilerParams(vmem_limit_bytes=2 * 2**20),
    )(y, new_state)


def solution(mesh):
    in_specs = (
        P("grp", None, None),
        P(None, "grp", None, "tp", None),
        P(),
        P(None, None, "tp"),
        P(None, None, "tp"),
        P(None, None, None, "tp"),
        P(None, None, None, "tp"),
        P(None, None, "tp"),
        P(None, None, "tp", None),
    )
    out_specs = (P("grp", None, "tp"), P(None, "grp", None, "tp", None))
    return jax.shard_map(local, mesh=mesh, in_specs=in_specs, out_specs=out_specs, check_vma=False)
```

```python
import functools

import jax
import jax.numpy as jnp
import numpy as np
from jax import lax
from jax.experimental import pallas as pl
from jax.experimental.pallas import tpu as pltpu
from jax.sharding import PartitionSpec as P

HEAD_DIM = 256
PAST = 1024


EPS_RMS = 1e-06
EPS_GROUP = 1e-05
ROTARY_BASE = 10000.0


def log_decays(count):
    return jnp.log(1.0 - jnp.power(2.0, -5.0 - jnp.arange(count, dtype=jnp.float32)))


def decay_tables(log_gamma, count):
    steps = jnp.arange(count, dtype=jnp.float32)
    gap = steps[:, None] - steps[None, :]
    intra = jnp.where(
        gap[None] >= 0, jnp.exp(log_gamma[:, None, None] * jnp.maximum(gap, 0.0)[None]), 0.0
    )
    q_decay = jnp.exp(log_gamma[None, :] * (steps[:, None] + 1.0))
    k_decay = jnp.exp(log_gamma[None, :] * (count - 1.0 - steps[:, None]))
    block_decay = jnp.exp(log_gamma * count)
    return (intra, q_decay, k_decay, block_decay)


def rotate(values, offset):
    half_dim = values.shape[-1] // 2
    freqs = jnp.power(
        ROTARY_BASE, -jnp.arange(half_dim, dtype=jnp.float32) * (2.0 / values.shape[-1])
    )
    places = (offset + jnp.arange(values.shape[1])).astype(jnp.float32)
    angles = places[:, None] * freqs[None, :]
    cosine = jnp.cos(angles)[None, :, None, :]
    sine = jnp.sin(angles)[None, :, None, :]
    first = values[..., :half_dim]
    second = values[..., half_dim:]
    return jnp.concatenate(
        [first * cosine - second * sine, second * cosine + first * sine], axis=-1
    )


def plain_local(
    stream_in,
    state_in,
    norm_gain,
    query_weight,
    key_weight,
    value_weight,
    gate_weight,
    group_gain,
    output_weight,
):
    seqs, new_tok, width = stream_in.shape
    heads, local_dim = (value_weight.shape[2], value_weight.shape[3])
    head_dim = HEAD_DIM
    log_gamma = log_decays(heads)
    intra, q_decay, k_decay, block_decay = decay_tables(log_gamma, new_tok)
    highest = lax.Precision.HIGHEST
    share_cols = width // lax.axis_size("tp")
    col_start = lax.axis_index("tp") * share_cols
    layers = state_in.shape[0]
    stream = stream_in
    stream_share = stream_in
    new_states = []
    for layer_no in range(layers):
        stream_f = stream.astype(jnp.float32)
        normed = stream_f * lax.rsqrt(
            jnp.mean(stream_f * stream_f, axis=-1, keepdims=True) + EPS_RMS
        )
        normed = (normed * norm_gain[layer_no].astype(jnp.float32)).astype(jnp.bfloat16)
        flat = normed.reshape(seqs * new_tok, width)
        query_part = jnp.dot(flat, query_weight[layer_no], preferred_element_type=jnp.float32)
        query_part = query_part.astype(jnp.bfloat16).reshape(seqs, new_tok, -1)
        key_part = jnp.dot(flat, key_weight[layer_no], preferred_element_type=jnp.float32)
        key_part = key_part.astype(jnp.bfloat16).reshape(seqs, new_tok, -1)

        def project_local(weight):
            result = jnp.dot(
                flat, weight.reshape(width, heads * local_dim), preferred_element_type=jnp.float32
            )
            result = lax.optimization_barrier(result.astype(jnp.bfloat16))
            return result.astype(jnp.float32).reshape(seqs, new_tok, heads, local_dim)

        values_f = project_local(value_weight[layer_no])
        gates_f = project_local(gate_weight[layer_no])
        queries, key_rows = (
            lax.all_gather(query_part, "tp", axis=2, tiled=True),
            lax.all_gather(key_part, "tp", axis=2, tiled=True),
        )
        queries = queries.astype(jnp.float32).reshape(seqs, new_tok, heads, head_dim)
        key_rows = key_rows.astype(jnp.float32).reshape(seqs, new_tok, heads, head_dim)
        rot_q = rotate(queries, PAST)
        rot_k = rotate(key_rows, PAST) * head_dim ** (-0.5)
        scores = jnp.einsum("bthd,bshd->bhts", rot_q, rot_k, precision=highest) * intra[None]
        inner = jnp.einsum("bhts,bshe->bthe", scores, values_f, precision=highest)
        state = state_in[layer_no]
        carried = (
            jnp.einsum("bthd,bhed->bthe", rot_q, state, precision=highest)
            * q_decay[None, :, :, None]
        )
        mixed = inner + carried
        new_state = state * block_decay[None, :, None, None] + jnp.einsum(
            "bthe,bthd->bhed", values_f, rot_k * k_decay[None, :, :, None], precision=highest
        )
        new_states.append(new_state)
        totals, squares = lax.psum((jnp.sum(mixed, axis=-1), jnp.sum(mixed * mixed, axis=-1)), "tp")
        mean_o = (totals / head_dim)[..., None]
        var_o = (squares / head_dim)[..., None] - mean_o * mean_o
        normal = (
            (mixed - mean_o)
            * lax.rsqrt(var_o + EPS_GROUP)
            * group_gain[layer_no].astype(jnp.float32)[None, None]
        )
        gated = (jax.nn.silu(gates_f) * normal).astype(jnp.bfloat16)
        partial_out = jnp.dot(
            gated.reshape(seqs * new_tok, heads * local_dim),
            output_weight[layer_no].reshape(heads * local_dim, width),
            preferred_element_type=jnp.float32,
        ).reshape(seqs, new_tok, width)
        share_out = lax.psum_scatter(partial_out, "tp", scatter_dimension=2, tiled=True)
        own_cols = lax.dynamic_slice_in_dim(stream, col_start, share_cols, 2)
        stream_share = (own_cols.astype(jnp.float32) + share_out).astype(jnp.bfloat16)
        if layer_no + 1 < layers:
            stream = lax.all_gather(stream_share, "tp", axis=2, tiled=True)
    result = stream_share
    return (result, jnp.stack(new_states))


F32 = jnp.float32
BF16 = jnp.bfloat16
XPARTS = 4
scope = jax.named_scope


def nt_dot(a, b, precision=None):
    return lax.dot_general(
        a, b, (((1,), (1,)), ((), ())), preferred_element_type=F32, precision=precision
    )


def thirds(value, axis):
    high = value.astype(BF16)
    rest = value - high.astype(F32)
    middle = rest.astype(BF16)
    low = (rest - middle.astype(F32)).astype(BF16)
    return jnp.concatenate([high, middle, low], axis=axis)


def log2(value):
    return int(value).bit_length() - 1


def rotary_tables(heads, new_tok, head_dim):
    half = head_dim // 2
    freqs = np.power(
        np.float32(ROTARY_BASE), -np.arange(half, dtype=np.float32) * np.float32(2.0 / head_dim)
    ).astype(np.float32)
    tok = np.arange(8) % new_tok
    places = (PAST + tok).astype(np.float32)
    angles = (places[:, None] * freqs[None, :]).astype(np.float32).astype(np.float64)
    gamma = 1.0 - np.power(2.0, -5.0 - np.arange(heads))
    grow = np.power(gamma[:, None], tok[None, :] + 1.0)[:, :, None]
    shrink = head_dim ** (-0.5) / grow
    cosine, sine = np.cos(angles)[None], np.sin(angles)[None]
    block = np.broadcast_to(np.power(gamma, new_tok)[:, None, None], (heads, 8, half))
    return np.stack(
        [cosine * grow, sine * grow, cosine * shrink, sine * shrink, block]
    ).astype(np.float32)


def kernel(
    n, head_dim,
    x_hbm, st_hbm, ng_hbm, qw_hbm, kw_hbm, vw_hbm, gw_hbm, gg_hbm, ow_hbm, tab_hbm,
    y_ref, stv,
    ng_ref, gg_ref, tab_ref, xr, xs, nv, wqk, wvg, wo, qg, kg, sc, vts, vb, sb, pbs, pbr, yss, ysr, rss, rsr, mkc, mks, fold, sqa, qka, vga, osum,
    lsem, ag_s, st_s, rs_s, aq_r, ak_r, ax_r, am_r, sc_r, st_r, pb_r, ys_r, rs_r,
):
    layers, seqs, heads, e_dim, _ = st_hbm.shape
    tok = x_hbm.shape[1]
    width = x_hbm.shape[2]
    rows = seqs * tok
    share = width // n
    cols = qw_hbm.shape[2]
    he = heads * e_dim
    half = head_dim // 2
    nc = n // 2
    me = lax.axis_index("tp")
    core = lax.rem(me, 2)
    chip = lax.div(me, 2)
    partner = chip * 2 + 1 - core

    nz = nc // 2
    yy = lax.rem(chip, 2)
    zz = lax.div(chip, 2)

    def chip_at(o, y):
        z, bit = zz, 1
        while bit < nz:
            if o & bit:
                z = z + bit - 2 * bit * lax.rem(lax.div(z, bit), 2)
            bit = 2 * bit
        return z * 2 + y

    def at_z(o, y, c):
        return chip_at(o, y) * 2 + c

    facing = at_z(0, 1 - yy, core)
    far = list(range(2, nz)) + [1]
    xnear = list(range(1, nz))
    near = [1] + list(range(nz - 1, 1, -1))

    def remote(src, dst, ssem, rsem, device):
        return pltpu.make_async_remote_copy(
            src_ref=src, dst_ref=dst, send_sem=ssem, recv_sem=rsem,
            device_id={"tp": device}, device_id_type=pl.DeviceIdType.MESH,
        )

    loads = {}
    count = 0

    def load(name, src, dst):
        nonlocal count
        loads[name] = pltpu.make_async_copy(src, dst, lsem.at[count])
        loads[name].start()
        count += 1

    wide = width // XPARTS

    def load_queries(l, deep, j):
        at = pl.ds(j * deep, deep)
        load(("q", l, j), qw_hbm.at[l, at], wqk.at[l, at, pl.ds(0, cols)])
        load(("k", l, j), kw_hbm.at[l, at], wqk.at[l, at, pl.ds(cols, cols)])

    load("ng", ng_hbm, ng_ref)
    for j in range(XPARTS):
        at = pl.ds(j * wide, wide)
        load(("x", j), x_hbm.at[:, :, at], xr.at[:, :, at])
        load_queries(0, wide, j)

    barrier = pltpu.get_barrier_semaphore()
    for o in range(1, n):
        pl.semaphore_signal(
            barrier, inc=1, device_id={"tp": lax.rem(me + o, n)},
            device_id_type=pl.DeviceIdType.MESH,
        )

    def load_rest():
        for l in range(layers):
            if l:
                load_queries(l, width, 0)
            load(("v", l), vw_hbm.at[l], wvg.at[l, pl.ds(0, he)])
            load(("g", l), gw_hbm.at[l], wvg.at[l, pl.ds(he, he)])
            load(("s", l), st_hbm.at[l], stv.at[l])
            if l == 0:
                load("tab", tab_hbm, tab_ref)
                load("gg", gg_hbm, gg_ref)
            load(("o", l), ow_hbm.at[l], wo.at[l])

    be = seqs * e_dim

    def iota(shape, dim, shift=0):
        return jnp.right_shift(lax.broadcasted_iota(jnp.int32, shape, dim), shift)

    te, tt = log2(e_dim), log2(tok)
    low = e_dim - 1
    causal = (
        (iota((rows, rows), 0, tt) == iota((rows, rows), 1, tt))
        & (iota((rows, rows), 0) >= iota((rows, rows), 1))
    ).astype(F32)
    heads_of = (iota((heads, he), 0) == iota((heads, he), 1, te)).astype(F32)
    place = (
        iota((e_dim, he), 0) == jnp.bitwise_and(iota((e_dim, he), 1), low)
    ).astype(F32)
    nth = jnp.concatenate(
        [
            (
                jnp.left_shift(iota((rows, rows), 0, tt), tt) + t == iota((rows, rows), 1)
            ).astype(F32).astype(BF16)
            for t in range(tok)
        ],
        axis=0,
    )
    pick = (
        jnp.bitwise_and(iota((8, rows), 1), tok - 1) == iota((8, rows), 0)
    ).astype(F32).astype(BF16)
    highest = lax.Precision.HIGHEST

    def make_masks():
        mkc[...] = (iota((rows, be), 0, tt) == iota((rows, be), 1, te)).astype(F32).astype(BF16)
        mks[...] = (iota((be, rows), 0, te) == iota((be, rows), 1, tt)).astype(F32).astype(BF16)
        fold[...] = (
            jnp.bitwise_and(iota((be, he), 0), low) == jnp.bitwise_and(iota((be, he), 1), low)
        ).astype(F32).astype(BF16)

    drains = []
    most = xs.at[0, pl.ds(0, n - 1)]
    halves = [pl.ds(i * (rows // 2), rows // 2) for i in range(2)]

    def ring(name, buf, recv, send, at=None, direct=(), twice=(), near=near, meet=None):
        def slot_of(j):
            return buf.at[j] if at is None else buf.at[j, at]

        def sem(k):
            return recv.at[k] if meet is None or k < nc else am_r.at[meet[k - nc]]

        def push(slot, k, device):
            remote(slot, slot, send, sem(k), device).start()

        def arrive(slot, k):
            remote(slot, slot, send, recv.at[k], partner).wait_recv()

        def start(others=True, other_core=True):
            own = slot_of(me)
            if other_core:
                push(own, nc, partner)
            if others:
                push(own, nz, facing)
                for o in near:
                    push(own, o, at_z(o, yy, core))

        def last(k):
            return nc + 1 if recv.shape[0] == nc + 2 and k > nc else k

        def from_z(o):
            with scope(f"{name}z{o}"):
                slot = slot_of(at_z(o, yy, core))
                arrive(slot, o)
                if o not in direct:
                    push(slot, nz + o, facing)
                if o in twice:
                    push(slot, nc + nz + o, at_z(0, 1 - yy, 1 - core))
                push(slot, last(nc + o), partner)

        def from_y(o):
            with scope(f"{name}y{o}"):
                slot = slot_of(at_z(o, 1 - yy, core))
                arrive(slot, nz + o)
                for far_o in direct if o == 0 else ():
                    push(slot, nz + far_o, at_z(far_o, yy, core))
                if o not in twice:
                    push(slot, last(nc + nz + o), partner)

        def done(o, side):
            with scope(f"{name}d{side}{o}"):
                arrive(slot_of(at_z(o, 1 - yy if side else yy, 1 - core)), nc + nz * side + o)

        def done_rest():
            with scope(name + "rest"):
                arrive(slot_of(pl.ds(0, nc - 1)), nc + 1)

        return start, from_z, from_y, done, done_rest

    def in_order(name, from_z, from_y, done, on_chip, early, between, later):
        def use(*which):
            for o, side in which:
                done(o, side)
            with scope(f"{name}c{which[0][1]}{which[0][0]}"):
                on_chip(which)

        use((0, 0))
        from_z(near[0])
        from_y(0)
        early()
        for o in near[1:]:
            from_z(o)
        use((near[0], 0), (0, 1))
        from_y(near[0])
        use(*[(o, 0) for o in near[1:]])
        for o in near[1:-1]:
            from_y(o)
        between()
        from_y(near[-1])
        later()
        use(*[(o, 1) for o in near[:-1]])
        use((near[-1], 1))

    def spread(table):
        return jnp.broadcast_to(table[None], (rows // 8, 8, half)).reshape(rows, half)

    def rotated(buf, l, h, table):
        a, b = buf[l, 2 * h].astype(F32), buf[l, 2 * h + 1].astype(F32)
        cosine, sine = spread(tab_ref[table, h]), spread(tab_ref[table + 1, h])
        return jnp.concatenate([a * cosine - b * sine, b * cosine + a * sine], axis=1).astype(BF16)

    def absorb(l, j, count, block_of):
        at = pl.ds(pl.multiple_of(j * share, share), share * count)
        parts = []
        square = sqa[...]
        for i in range(count):
            block = block_of(j + i)
            for k in range(0, share, 128):
                square = square + block[:, k : k + 128] * block[:, k : k + 128]
            one = pl.ds(pl.multiple_of((j + i) * share, share), share)
            gain = ng_ref[l : l + 1, one].astype(F32)
            scaled = (block * gain).astype(BF16)
            nv[:, one] = scaled
            parts.append(scaled)
        sqa[...] = square
        both = jnp.concatenate(parts, axis=1) if count > 1 else parts[0]
        qka[...] += jnp.dot(both, wqk[l, at, :], preferred_element_type=F32)
        if l:
            vga[...] += nt_dot(both, wvg[l, :, at])

    def unpack(j):
        at = pl.ds(j * share if isinstance(j, int) else pl.multiple_of(j * share, share), share)
        return xr[:, :, at].astype(F32).reshape(rows, share)

    def clear():
        sqa[...] = jnp.zeros_like(sqa)
        qka[...] = jnp.zeros_like(qka)
        vga[...] = jnp.zeros_like(vga)

    for l in range(layers):
        if l == 0:
            with scope("absorb"):
                clear()
                per = n // XPARTS
                loads["ng"].wait()
                for p in range(XPARTS):
                    with scope(f"await{p}"):
                        for name in (("x", p), ("q", 0, p), ("k", 0, p)):
                            loads[name].wait()
                    if p == XPARTS - 1:
                        load_rest()
                    absorb(0, p * per, per, unpack)

        with scope(f"qk{l}"):
            scale = lax.rsqrt(jnp.sum(sqa[...], axis=1, keepdims=True) / width + EPS_RMS)
            both = (qka[...] * scale).astype(BF16)
            qg[l, me] = both[:, :cols]
            kg[l, me] = both[:, cols:]
        if l == 0:
            with scope("bar"):
                pl.semaphore_wait(barrier, n - 1)

        q_start, q_z, q_y, q_done, _ = ring(f"q{l}", qg.at[l], aq_r, ag_s.at[l], None, (), (near[-1],))
        k_start, k_z, k_y, k_done, k_rest = ring(f"k{l}", kg.at[l], ak_r, ag_s.at[l])
        drains.append((most, ag_s.at[l]))
        q_start()
        k_start(others=False)
        if l == 0:
            with scope("masks"):
                make_masks()
                xs[0, me] = unpack(me).astype(BF16)
                loads["tab"].wait()
                loads["gg"].wait()
        q_done(0, 0)
        k_done(0, 0)
        with scope(f"scores{l}"):
            rk = rotated(kg, l, chip, 2)
            scores = (nt_dot(rotated(qg, l, chip, 0), rk) * causal).astype(BF16)
            sc[l, chip] = nt_dot(pick, scores)
            for o, side in [(o, side) for o in far for side in (1, 0)] + [(0, 1)]:
                slot = sc.at[l, chip]
                remote(
                    slot, slot, ag_s.at[layers + l], sc_r.at[0],
                    at_z(o, 1 - yy if side else yy, core),
                ).start()
            drains.append((sc.at[l, pl.ds(0, nc - 1)], ag_s.at[layers + l]))
        k_start(other_core=False)

        with scope(f"vg{l}"):
            if l == 0:
                loads[("v", l)].wait()
                vga[:, :he] = nt_dot(nv[...], wvg[l, :he])
            values = (vga[:, :he] * scale).astype(BF16)
            vts[...] = jnp.transpose(values.astype(F32)).astype(BF16)
            vb[...] = jnp.dot(nth, values, preferred_element_type=F32).reshape(tok, rows, he)
            loads[("s", l)].wait()
        box = {"mixed": jnp.zeros((rows, he), F32)}

        def gate_on(l=l):
            if l == 0:
                with scope(f"gates{l}"):
                    loads[("g", l)].wait()
                    vga[:, he:] = nt_dot(nv[...], wvg[l, he:])

        def carry_one(o, side, l=l):
            h = chip_at(o, 1 - yy if side else yy)
            rq = rotated(qg, l, h, 0)
            state = stv[l, :, h].reshape(be, head_dim).astype(BF16)
            carried = nt_dot(rq, state).astype(BF16) * mkc[...]
            part = jnp.dot(carried, fold[...], preferred_element_type=F32)
            return part * (iota((1, he), 1, te) == h).astype(F32)

        def intra(l=l, box=box):
            with scope(f"intra{l}"):
                others = sc.at[l, pl.ds(0, nc - 1)]
                remote(others, others, ag_s.at[layers + l], sc_r.at[0], partner).wait_recv()
                flat = jnp.concatenate([sc[l, :, t, :] for t in range(tok)], axis=1).astype(BF16)
                wide = lax.dot_general(
                    flat, heads_of.astype(BF16), (((0,), (0,)), ((), ())), preferred_element_type=F32
                )
                box["mixed"] = box["mixed"] + jnp.sum(wide.reshape(tok, rows, he) * vb[...], axis=0)

        def k_on(k_z=k_z, k_y=k_y):
            for o in near:
                k_z(o)
            k_y(0)

        def mix(which, box=box):
            for o, side in which:
                box["mixed"] = box["mixed"] + carry_one(o, side)

        in_order(f"q{l}", q_z, q_y, lambda o, s: None if o == s == 0 else q_done(o, s), mix, gate_on, intra, k_on)
        mixed = box["mixed"]

        with scope(f"sums{l}"):
            both = nt_dot(
                jnp.concatenate([heads_of.astype(BF16)] * 3, axis=1),
                thirds(jnp.concatenate([mixed, mixed * mixed], axis=0), 1),
            )
            sums = both[:, :rows]
            squares = jnp.maximum(both[:, rows:] - sums * sums / e_dim, 0.0)
            sb[l, me] = jnp.concatenate([sums, squares], axis=1).astype(BF16)
            peers = [at_z(o, y, c) for o in far for y in (1 - yy, yy) for c in (core, 1 - core)]
            for device in peers + [at_z(0, 1 - yy, 1 - core), facing, partner]:
                remote(sb.at[l, me], sb.at[l, me], st_s.at[l], st_r.at[0], device).start()
            drains.append((sb.at[l, pl.ds(0, n - 1)], st_s.at[l]))

        def update(h, carry, l=l):
            at = pl.ds(pl.multiple_of(h * e_dim, e_dim), e_dim)
            tall = jnp.broadcast_to(vts[at, :][None], (seqs, e_dim, rows)).reshape(be, rows)
            fresh = jnp.dot(tall * mks[...], rotated(kg, l, h, 2), preferred_element_type=F32)
            row = tab_ref[4, h][0:1, :]
            fade = jnp.concatenate([row, row], axis=1)
            state = stv[l, :, h].reshape(be, head_dim)
            stv[l, :, h] = ((state + fresh) * fade).reshape(seqs, e_dim, head_dim)
            return carry

        with scope(f"silu{l}"):
            gates = (vga[:, he:] * scale).astype(BF16).astype(F32)
            gain = jnp.dot(gg_ref[l].astype(F32), place, preferred_element_type=F32, precision=highest)
            gain = jnp.sum(gain * heads_of, axis=0, keepdims=True)
            gains = gates / (1.0 + jnp.exp(-gates)) * gain

        with scope(f"stwait{l}"):
            others = sb.at[l, pl.ds(0, n - 1)]
            remote(others, others, st_s.at[l], st_r.at[0], partner).wait_recv()

        with scope(f"gated{l}"):
            stats = sb[l].astype(F32)
            sums = stats[:, :, :rows]
            total = jnp.sum(sums, axis=0)
            off = sums - (total / n)[None]
            var = jnp.sum(stats[:, :, rows:] + off * off / e_dim, axis=0) / head_dim
            both = jnp.concatenate([total / head_dim, lax.rsqrt(var + EPS_GROUP)], axis=1)
            both = lax.dot_general(
                thirds(both, 0), jnp.concatenate([heads_of.astype(BF16)] * 3, axis=0),
                (((0,), (0,)), ((), ())), preferred_element_type=F32,
            )
            gated = ((mixed - both[:rows]) * both[rows:] * gains).astype(BF16)
            loads[("o", l)].wait()

        def chunk(j, l=l, gated=gated):
            at = pl.ds(pl.multiple_of(j * share, share), share)
            return jnp.dot(gated, wo[l, :, at], preferred_element_type=F32)

        order = list(range(nz - 1, -1, -1))
        pb_s = ys_s = rz_s = rs_s.at[l]

        def offer(o, side, l=l):
            k = side * nz + o
            y = 1 - yy if side else yy
            pbs[l, k] = chunk(at_z(o, y, 1 - core)).astype(BF16)
            remote(pbs.at[l, k], pbr.at[l, k], pb_s, pb_r.at[k], partner).start()

        def paired(o, side, l=l):
            k = side * nz + o
            own = chunk(at_z(o, 1 - yy if side else yy, core))
            remote(pbs.at[l, k], pbr.at[l, k], pb_s, pb_r.at[k], partner).wait_recv()
            return own + pbr[l, k].astype(F32)

        early = order[0]
        later = order[1:]
        tail = halves[1]

        def hop(o, at, l=l):
            src, dst = yss.at[l, o, at], ysr.at[l, o, at]
            return remote(src, dst, ys_s, ys_r.at[halves.index(at), o], facing)

        def turn(o, at, l=l):
            src, dst = rss.at[l, o, at], rsr.at[l, o, at]
            return remote(src, dst, rz_s, rs_r.at[halves.index(at)], at_z(o, yy, core))

        def cross(l=l):
            return remote(rss.at[l, 0, tail], rsr.at[l, 0, tail], rz_s, rs_r.at[2], at_z(early, yy, core))

        with scope(f"rsa{l}"):
            offer(early, 1)
            offer(early, 0)
            for o in later:
                offer(o, 1)
        with scope(f"rsb{l}"):
            both = paired(early, 1).astype(BF16)
            yss[l, early] = both
            hop(early, halves[0]).start()
            rss[l, 0, tail] = both[rows // 2 :]
            cross().start()
            osum[early] = paired(early, 0)
            rss[l, early, tail] = osum[early, tail].astype(BF16)
            turn(early, tail).start()
            for o in later[:-1]:
                yss[l, o] = paired(o, 1).astype(BF16)
                hop(o, halves[0]).start()
            osum[nz] = paired(0, 1)
            yss[l, 0, halves[0]] = osum[nz, halves[0]].astype(BF16)
            hop(0, halves[0]).start()
            for o in later[:-1]:
                hop(o, tail).start()
        with scope(f"rsc{l}"):
            for o in later:
                offer(o, 0)
            for o in near:
                k_y(o)
            drains.append((most, rs_s.at[l]))
        with scope(f"own{l}"):
            for o in later:
                osum[o] = paired(o, 0)

        def join(o, at, l=l):
            with scope(f"rsd{l}{o}"):
                hop(o, at).wait_recv()
                own = osum[o, at] + ysr[l, o, at].astype(F32)
                if o:
                    rss[l, o, at] = own.astype(BF16)
                    turn(o, at).start()
                else:
                    osum[o, at] = own

        def finish(at, l=l):
            acc = osum[0, at] + xs[l, me, at].astype(F32)
            with scope(f"rse{l}"):
                parts = rsr.at[l, pl.ds(1, nz - 1), at]
                remote(parts, parts, rz_s, rs_r.at[halves.index(at)], facing).wait_recv()
                for o in near:
                    acc = acc + rsr[l, o, at].astype(F32)
            return acc.astype(BF16)

        for o in order:
            join(o, halves[0])
        with scope(f"cross{l}"):
            cross().wait_recv()
            yss[l, 0, tail] = (osum[nz, tail] + rsr[l, 0, tail].astype(F32)).astype(BF16)
            hop(0, tail).start()
        for o in later[:-1]:
            join(o, tail)
        k_rest()
        with scope(f"update{l}"):
            lax.fori_loop(0, heads, update, 0, unroll=True)
        if l + 1 == layers:
            y_ref[halves[0], :] = finish(halves[0])
            join(0, tail)
            y_ref[tail, :] = finish(tail)
            continue

        first, rest, end = xnear[0], xnear[1:], xnear[-1]
        meet = {0: 0, first: 1, nz: 1, nz + first: 3, nz + end: 3}
        meet.update({o: 2 for o in rest})
        meet.update({nz + o: 4 for o in rest[:-1]})
        rings = []
        clear()
        drains.append((most, ag_s.at[2 * layers + l]))
        for i, at in enumerate(halves):
            rings.append(ring(f"x{l}{i}", xs.at[l + 1], ax_r.at[i], ag_s.at[2 * layers + l], at, (xnear[-1],) if i else (), tuple(xnear[1:-1]) if i else (), xnear, meet))
            if i:
                join(0, tail)
            xs[l + 1, me, at] = finish(at)
            rings[i][0]()
        loads[("q", l + 1, 0)].wait()
        loads[("k", l + 1, 0)].wait()
        loads[("v", l + 1)].wait()
        loads[("g", l + 1)].wait()
        (_, az, ay, _, _), (_, bz, by, _, _) = rings

        def use(*which, l=l):
            o, side = which[0]
            both = xs.at[l + 1, pl.ds(0, len(which))]
            with scope(f"x{l}d{side}{o}"):
                remote(both, both, ag_s.at[2 * layers + l], am_r.at[meet[side * nz + o]], partner).wait_recv()
            with scope(f"x{l}c{which[0][1]}{which[0][0]}"):
                for o, side in which:
                    c = chip_at(o, 1 - yy if side else yy)
                    absorb(l + 1, 2 * c, 2, lambda j: xs[l + 1, j].astype(F32))

        az(first)
        ay(0)
        for o in rest:
            az(o)
        bz(first)
        ay(first)
        by(0)
        use((0, 0))
        for o in rest[:-1]:
            ay(o)
            bz(o)
        ay(end)
        bz(end)
        use((first, 0), (0, 1))
        by(first)
        use(*[(o, 0) for o in rest])
        by(end)
        use((first, 1), (end, 1))
        for o in rest[:-1]:
            by(o)
        use(*[(o, 1) for o in rest[:-1]])

    with scope("drain"):
        for ref, sem in drains:
            remote(ref, ref, sem, st_r.at[0], partner).wait_send()


def store_kernel(y_ref, state_ref, y_out, state_out, yv, sem):
    layers, seqs = state_ref.shape[:2]
    copies = []
    parts = sem.shape[0] - 1
    per = layers * seqs // parts
    for i in range(parts):
        l, s = i * per // seqs, pl.ds(i * per % seqs, per)
        copies.append(pltpu.make_async_copy(state_ref.at[l, s], state_out.at[l, s], sem.at[i]))
    for copy in copies:
        copy.start()
    yv[...] = y_ref[...].astype(F32).reshape(yv.shape).astype(BF16)
    copy = pltpu.make_async_copy(yv, y_out, sem.at[parts])
    copy.start()
    for copy in copies + [copy]:
        copy.wait()


def local(
    stream_in, state_in, norm_gain, query_weight, key_weight,
    value_weight, gate_weight, group_gain, output_weight,
):
    n = lax.axis_size("tp")
    seqs, tok, width = stream_in.shape
    layers, _, heads, e_dim, head_dim = state_in.shape
    cols = query_weight.shape[2]
    rows = seqs * tok
    he = heads * e_dim
    share = width // n
    fits = (
        cols == 128 and head_dim == 256 and he == 128 and heads == 8 and e_dim == 16
        and share % 128 == 0 and n % 4 == 0 and n & (n - 1) == 0 and rows == 128 and 8 % tok == 0
        and n == 2 * heads and seqs % 4 == 0 and share == 2 * cols
    )
    if not fits:
        return plain_local(
            stream_in, state_in, norm_gain, query_weight, key_weight,
            value_weight, gate_weight, group_gain, output_weight,
        )
    nc = n // 2
    be = seqs * e_dim
    hbm = pl.BlockSpec(memory_space=pltpu.HBM)
    vmem = pl.BlockSpec(memory_space=pltpu.VMEM)
    dma = pltpu.SemaphoreType.DMA
    tables = jnp.asarray(rotary_tables(heads, tok, head_dim))
    flat = lambda w: jnp.transpose(w, (0, 2, 3, 1)).reshape(layers, he, width)
    y, new_state = pl.pallas_call(
        functools.partial(kernel, n, head_dim),
        name="retention",
        out_shape=(
            pltpu.VMEM((rows, share), BF16),
            pltpu.VMEM(state_in.shape, F32),
        ),
        in_specs=[hbm] * 10,
        out_specs=(vmem, vmem),
        scratch_shapes=[
            pltpu.VMEM(norm_gain.shape, BF16),
            pltpu.VMEM(group_gain.shape, BF16),
            pltpu.VMEM(tables.shape, F32),
            pltpu.VMEM((seqs, tok, width), BF16),
            pltpu.VMEM((layers, n, rows, share), BF16),
            pltpu.VMEM((rows, width), BF16),
            pltpu.VMEM((layers, width, 2 * cols), BF16),
            pltpu.VMEM((layers, 2 * he, width), BF16),
            pltpu.VMEM((layers, he, width), BF16),
            pltpu.VMEM((layers, n, rows, cols), BF16),
            pltpu.VMEM((layers, n, rows, cols), BF16),
            pltpu.VMEM((layers, heads, 8, rows), F32),
            pltpu.VMEM((he, rows), BF16),
            pltpu.VMEM((tok, rows, he), F32),
            pltpu.VMEM((layers, n, heads, 2 * rows), BF16),
            pltpu.VMEM((layers, nc, rows, share), BF16),
            pltpu.VMEM((layers, nc, rows, share), BF16),
            pltpu.VMEM((layers, nc // 2, rows, share), BF16),
            pltpu.VMEM((layers, nc // 2, rows, share), BF16),
            pltpu.VMEM((layers, nc // 2, rows, share), BF16),
            pltpu.VMEM((layers, nc // 2, rows, share), BF16),
            pltpu.VMEM((rows, be), BF16),
            pltpu.VMEM((be, rows), BF16),
            pltpu.VMEM((be, he), BF16),
            pltpu.VMEM((rows, 128), F32),
            pltpu.VMEM((rows, 2 * cols), F32),
            pltpu.VMEM((rows, 2 * he), F32),
            pltpu.VMEM((nc // 2 + 1, rows, share), F32),
            dma((3 * XPARTS + 6 * layers + 1,)),
            dma((3 * layers - 1,)),
            dma((layers,)),
            dma((layers,)),
            dma((n,)),
            dma((nc + 2,)),
            dma((2, nc)),
            dma((5,)),
            dma((1,)),
            dma((1,)),
            dma((nc,)),
            dma((2, nc // 2)),
            dma((3,)),
        ],
        compiler_params=pltpu.CompilerParams(
            collective_id=0, has_side_effects=True, vmem_limit_bytes=58500000
        ),
    )(
        stream_in, state_in, norm_gain, query_weight, key_weight,
        flat(value_weight), flat(gate_weight), group_gain,
        output_weight.reshape(layers, he, width), tables,
    )
    return pl.pallas_call(
        store_kernel,
        name="store",
        out_shape=(
            jax.ShapeDtypeStruct((seqs, tok, share), BF16),
            jax.ShapeDtypeStruct(state_in.shape, F32),
        ),
        in_specs=[vmem, vmem],
        out_specs=(hbm, hbm),
        scratch_shapes=[pltpu.VMEM((seqs, tok, share), BF16), dma((4 * layers + 1,))],
        compiler_params=pltpu.CompilerParams(vmem_limit_bytes=2 * 2**20),
    )(y, new_state)


def solution(mesh):
    in_specs = (
        P("grp", None, None),
        P(None, "grp", None, "tp", None),
        P(),
        P(None, None, "tp"),
        P(None, None, "tp"),
        P(None, None, None, "tp"),
        P(None, None, None, "tp"),
        P(None, None, "tp"),
        P(None, None, "tp", None),
    )
    out_specs = (P("grp", None, "tp"), P(None, "grp", None, "tp", None))
    return jax.shard_map(local, mesh=mesh, in_specs=in_specs, out_specs=out_specs, check_vma=False)
```

```python
import functools

import jax
import jax.numpy as jnp
import numpy as np
from jax import lax
from jax.experimental import pallas as pl
from jax.experimental.pallas import tpu as pltpu
from jax.sharding import PartitionSpec as P

HEAD_DIM = 256
PAST = 1024


EPS_RMS = 1e-06
EPS_GROUP = 1e-05
ROTARY_BASE = 10000.0


def log_decays(count):
    return jnp.log(1.0 - jnp.power(2.0, -5.0 - jnp.arange(count, dtype=jnp.float32)))


def decay_tables(log_gamma, count):
    steps = jnp.arange(count, dtype=jnp.float32)
    gap = steps[:, None] - steps[None, :]
    intra = jnp.where(
        gap[None] >= 0, jnp.exp(log_gamma[:, None, None] * jnp.maximum(gap, 0.0)[None]), 0.0
    )
    q_decay = jnp.exp(log_gamma[None, :] * (steps[:, None] + 1.0))
    k_decay = jnp.exp(log_gamma[None, :] * (count - 1.0 - steps[:, None]))
    block_decay = jnp.exp(log_gamma * count)
    return (intra, q_decay, k_decay, block_decay)


def rotate(values, offset):
    half_dim = values.shape[-1] // 2
    freqs = jnp.power(
        ROTARY_BASE, -jnp.arange(half_dim, dtype=jnp.float32) * (2.0 / values.shape[-1])
    )
    places = (offset + jnp.arange(values.shape[1])).astype(jnp.float32)
    angles = places[:, None] * freqs[None, :]
    cosine = jnp.cos(angles)[None, :, None, :]
    sine = jnp.sin(angles)[None, :, None, :]
    first = values[..., :half_dim]
    second = values[..., half_dim:]
    return jnp.concatenate(
        [first * cosine - second * sine, second * cosine + first * sine], axis=-1
    )


def plain_local(
    stream_in,
    state_in,
    norm_gain,
    query_weight,
    key_weight,
    value_weight,
    gate_weight,
    group_gain,
    output_weight,
):
    seqs, new_tok, width = stream_in.shape
    heads, local_dim = (value_weight.shape[2], value_weight.shape[3])
    head_dim = HEAD_DIM
    log_gamma = log_decays(heads)
    intra, q_decay, k_decay, block_decay = decay_tables(log_gamma, new_tok)
    highest = lax.Precision.HIGHEST
    share_cols = width // lax.axis_size("tp")
    col_start = lax.axis_index("tp") * share_cols
    layers = state_in.shape[0]
    stream = stream_in
    stream_share = stream_in
    new_states = []
    for layer_no in range(layers):
        stream_f = stream.astype(jnp.float32)
        normed = stream_f * lax.rsqrt(
            jnp.mean(stream_f * stream_f, axis=-1, keepdims=True) + EPS_RMS
        )
        normed = (normed * norm_gain[layer_no].astype(jnp.float32)).astype(jnp.bfloat16)
        flat = normed.reshape(seqs * new_tok, width)
        query_part = jnp.dot(flat, query_weight[layer_no], preferred_element_type=jnp.float32)
        query_part = query_part.astype(jnp.bfloat16).reshape(seqs, new_tok, -1)
        key_part = jnp.dot(flat, key_weight[layer_no], preferred_element_type=jnp.float32)
        key_part = key_part.astype(jnp.bfloat16).reshape(seqs, new_tok, -1)

        def project_local(weight):
            result = jnp.dot(
                flat, weight.reshape(width, heads * local_dim), preferred_element_type=jnp.float32
            )
            result = lax.optimization_barrier(result.astype(jnp.bfloat16))
            return result.astype(jnp.float32).reshape(seqs, new_tok, heads, local_dim)

        values_f = project_local(value_weight[layer_no])
        gates_f = project_local(gate_weight[layer_no])
        queries, key_rows = (
            lax.all_gather(query_part, "tp", axis=2, tiled=True),
            lax.all_gather(key_part, "tp", axis=2, tiled=True),
        )
        queries = queries.astype(jnp.float32).reshape(seqs, new_tok, heads, head_dim)
        key_rows = key_rows.astype(jnp.float32).reshape(seqs, new_tok, heads, head_dim)
        rot_q = rotate(queries, PAST)
        rot_k = rotate(key_rows, PAST) * head_dim ** (-0.5)
        scores = jnp.einsum("bthd,bshd->bhts", rot_q, rot_k, precision=highest) * intra[None]
        inner = jnp.einsum("bhts,bshe->bthe", scores, values_f, precision=highest)
        state = state_in[layer_no]
        carried = (
            jnp.einsum("bthd,bhed->bthe", rot_q, state, precision=highest)
            * q_decay[None, :, :, None]
        )
        mixed = inner + carried
        new_state = state * block_decay[None, :, None, None] + jnp.einsum(
            "bthe,bthd->bhed", values_f, rot_k * k_decay[None, :, :, None], precision=highest
        )
        new_states.append(new_state)
        totals, squares = lax.psum((jnp.sum(mixed, axis=-1), jnp.sum(mixed * mixed, axis=-1)), "tp")
        mean_o = (totals / head_dim)[..., None]
        var_o = (squares / head_dim)[..., None] - mean_o * mean_o
        normal = (
            (mixed - mean_o)
            * lax.rsqrt(var_o + EPS_GROUP)
            * group_gain[layer_no].astype(jnp.float32)[None, None]
        )
        gated = (jax.nn.silu(gates_f) * normal).astype(jnp.bfloat16)
        partial_out = jnp.dot(
            gated.reshape(seqs * new_tok, heads * local_dim),
            output_weight[layer_no].reshape(heads * local_dim, width),
            preferred_element_type=jnp.float32,
        ).reshape(seqs, new_tok, width)
        share_out = lax.psum_scatter(partial_out, "tp", scatter_dimension=2, tiled=True)
        own_cols = lax.dynamic_slice_in_dim(stream, col_start, share_cols, 2)
        stream_share = (own_cols.astype(jnp.float32) + share_out).astype(jnp.bfloat16)
        if layer_no + 1 < layers:
            stream = lax.all_gather(stream_share, "tp", axis=2, tiled=True)
    result = stream_share
    return (result, jnp.stack(new_states))


F32 = jnp.float32
BF16 = jnp.bfloat16
XPARTS = 4
scope = jax.named_scope


def nt_dot(a, b, precision=None):
    return lax.dot_general(
        a, b, (((1,), (1,)), ((), ())), preferred_element_type=F32, precision=precision
    )


def thirds(value, axis):
    high = value.astype(BF16)
    rest = value - high.astype(F32)
    middle = rest.astype(BF16)
    low = (rest - middle.astype(F32)).astype(BF16)
    return jnp.concatenate([high, middle, low], axis=axis)


def log2(value):
    return int(value).bit_length() - 1


def rotary_tables(heads, new_tok, head_dim):
    half = head_dim // 2
    freqs = np.power(
        np.float32(ROTARY_BASE), -np.arange(half, dtype=np.float32) * np.float32(2.0 / head_dim)
    ).astype(np.float32)
    tok = np.arange(8) % new_tok
    places = (PAST + tok).astype(np.float32)
    angles = (places[:, None] * freqs[None, :]).astype(np.float32).astype(np.float64)
    gamma = 1.0 - np.power(2.0, -5.0 - np.arange(heads))
    grow = np.power(gamma[:, None], tok[None, :] + 1.0)[:, :, None]
    shrink = head_dim ** (-0.5) / grow
    cosine, sine = np.cos(angles)[None], np.sin(angles)[None]
    block = np.broadcast_to(np.power(gamma, new_tok)[:, None, None], (heads, 8, half))
    return np.stack(
        [cosine * grow, sine * grow, cosine * shrink, sine * shrink, block]
    ).astype(np.float32)


def kernel(
    n, head_dim,
    x_hbm, st_hbm, ng_hbm, qw_hbm, kw_hbm, vw_hbm, gw_hbm, gg_hbm, ow_hbm, tab_hbm,
    y_ref, stv,
    ng_ref, gg_ref, tab_ref, xr, xs, nv, wqk, wvg, wo, qg, kg, sc, vts, vb, sb, wop, mgs, mgr, yss, ysr, rss, rsr, mkc, mks, fold, sqa, qka, vga, osum,
    lsem, ag_s, st_s, rs_s, aq_r, ak_r, ax_r, am_r, sc_r, st_r, wo_s, mg_s, wo_r, mg_r, ys_r, rs_r,
):
    layers, seqs, heads, e_dim, _ = st_hbm.shape
    tok = x_hbm.shape[1]
    width = x_hbm.shape[2]
    rows = seqs * tok
    share = width // n
    cols = qw_hbm.shape[2]
    he = heads * e_dim
    half = head_dim // 2
    nc = n // 2
    me = lax.axis_index("tp")
    core = lax.rem(me, 2)
    chip = lax.div(me, 2)
    partner = chip * 2 + 1 - core

    nz = nc // 2
    yy = lax.rem(chip, 2)
    zz = lax.div(chip, 2)

    def chip_at(o, y):
        z, bit = zz, 1
        while bit < nz:
            if o & bit:
                z = z + bit - 2 * bit * lax.rem(lax.div(z, bit), 2)
            bit = 2 * bit
        return z * 2 + y

    def at_z(o, y, c):
        return chip_at(o, y) * 2 + c

    facing = at_z(0, 1 - yy, core)
    far = list(range(2, nz)) + [1]
    xnear = list(range(1, nz))
    near = [1] + list(range(nz - 1, 1, -1))

    def remote(src, dst, ssem, rsem, device):
        return pltpu.make_async_remote_copy(
            src_ref=src, dst_ref=dst, send_sem=ssem, recv_sem=rsem,
            device_id={"tp": device}, device_id_type=pl.DeviceIdType.MESH,
        )

    loads = {}
    count = 0

    def load(name, src, dst):
        nonlocal count
        loads[name] = pltpu.make_async_copy(src, dst, lsem.at[count])
        loads[name].start()
        count += 1

    wide = width // XPARTS

    def load_queries(l, deep, j):
        at = pl.ds(j * deep, deep)
        load(("q", l, j), qw_hbm.at[l, at], wqk.at[l, at, pl.ds(0, cols)])
        load(("k", l, j), kw_hbm.at[l, at], wqk.at[l, at, pl.ds(cols, cols)])

    load("ng", ng_hbm, ng_ref)
    for j in range(XPARTS):
        at = pl.ds(j * wide, wide)
        load(("x", j), x_hbm.at[:, :, at], xr.at[:, :, at])
        load_queries(0, wide, j)

    barrier = pltpu.get_barrier_semaphore()
    for o in range(1, n):
        pl.semaphore_signal(
            barrier, inc=1, device_id={"tp": lax.rem(me + o, n)},
            device_id_type=pl.DeviceIdType.MESH,
        )

    def load_rest():
        for l in range(layers):
            if l:
                load_queries(l, width, 0)
            load(("v", l), vw_hbm.at[l], wvg.at[l, pl.ds(0, he)])
            load(("g", l), gw_hbm.at[l], wvg.at[l, pl.ds(he, he)])
            load(("s", l), st_hbm.at[l], stv.at[l])
            if l == 0:
                load("tab", tab_hbm, tab_ref)
                load("gg", gg_hbm, gg_ref)
            load(("o", l), ow_hbm.at[l], wo.at[l])

    be = seqs * e_dim

    def iota(shape, dim, shift=0):
        return jnp.right_shift(lax.broadcasted_iota(jnp.int32, shape, dim), shift)

    te, tt = log2(e_dim), log2(tok)
    low = e_dim - 1
    causal = (
        (iota((rows, rows), 0, tt) == iota((rows, rows), 1, tt))
        & (iota((rows, rows), 0) >= iota((rows, rows), 1))
    ).astype(F32)
    heads_of = (iota((heads, he), 0) == iota((heads, he), 1, te)).astype(F32)
    place = (
        iota((e_dim, he), 0) == jnp.bitwise_and(iota((e_dim, he), 1), low)
    ).astype(F32)
    nth = jnp.concatenate(
        [
            (
                jnp.left_shift(iota((rows, rows), 0, tt), tt) + t == iota((rows, rows), 1)
            ).astype(F32).astype(BF16)
            for t in range(tok)
        ],
        axis=0,
    )
    pick = (
        jnp.bitwise_and(iota((8, rows), 1), tok - 1) == iota((8, rows), 0)
    ).astype(F32).astype(BF16)
    highest = lax.Precision.HIGHEST

    def make_masks():
        mkc[...] = (iota((rows, be), 0, tt) == iota((rows, be), 1, te)).astype(F32).astype(BF16)
        mks[...] = (iota((be, rows), 0, te) == iota((be, rows), 1, tt)).astype(F32).astype(BF16)
        fold[...] = (
            jnp.bitwise_and(iota((be, he), 0), low) == jnp.bitwise_and(iota((be, he), 1), low)
        ).astype(F32).astype(BF16)

    drains = []
    most = xs.at[0, pl.ds(0, n - 1)]
    halves = [pl.ds(i * (rows // 2), rows // 2) for i in range(2)]

    def ring(name, buf, recv, send, at=None, direct=(), twice=(), near=near, meet=None):
        def slot_of(j):
            return buf.at[j] if at is None else buf.at[j, at]

        def sem(k):
            return recv.at[k] if meet is None or k < nc else am_r.at[meet[k - nc]]

        def push(slot, k, device):
            remote(slot, slot, send, sem(k), device).start()

        def arrive(slot, k):
            remote(slot, slot, send, recv.at[k], partner).wait_recv()

        def start(others=True, other_core=True):
            own = slot_of(me)
            if other_core:
                push(own, nc, partner)
            if others:
                push(own, nz, facing)
                for o in near:
                    push(own, o, at_z(o, yy, core))

        def last(k):
            return nc + 1 if recv.shape[0] == nc + 2 and k > nc else k

        def from_z(o):
            with scope(f"{name}z{o}"):
                slot = slot_of(at_z(o, yy, core))
                arrive(slot, o)
                if o not in direct:
                    push(slot, nz + o, facing)
                if o in twice:
                    push(slot, nc + nz + o, at_z(0, 1 - yy, 1 - core))
                push(slot, last(nc + o), partner)

        def from_y(o):
            with scope(f"{name}y{o}"):
                slot = slot_of(at_z(o, 1 - yy, core))
                arrive(slot, nz + o)
                for far_o in direct if o == 0 else ():
                    push(slot, nz + far_o, at_z(far_o, yy, core))
                if o not in twice:
                    push(slot, last(nc + nz + o), partner)

        def done(o, side):
            with scope(f"{name}d{side}{o}"):
                arrive(slot_of(at_z(o, 1 - yy if side else yy, 1 - core)), nc + nz * side + o)

        def done_rest():
            with scope(name + "rest"):
                arrive(slot_of(pl.ds(0, nc - 1)), nc + 1)

        return start, from_z, from_y, done, done_rest

    def in_order(name, from_z, from_y, done, on_chip, early, between, later):
        def use(*which):
            for o, side in which:
                done(o, side)
            with scope(f"{name}c{which[0][1]}{which[0][0]}"):
                on_chip(which)

        use((0, 0))
        from_z(near[0])
        from_y(0)
        early()
        for o in near[1:]:
            from_z(o)
        use((near[0], 0), (0, 1))
        from_y(near[0])
        use(*[(o, 0) for o in near[1:]])
        for o in near[1:-1]:
            from_y(o)
        between()
        from_y(near[-1])
        later()
        use(*[(o, 1) for o in near[:-1]])
        use((near[-1], 1))

    def spread(table):
        return jnp.broadcast_to(table[None], (rows // 8, 8, half)).reshape(rows, half)

    def rotated(buf, l, h, table):
        a, b = buf[l, 2 * h].astype(F32), buf[l, 2 * h + 1].astype(F32)
        cosine, sine = spread(tab_ref[table, h]), spread(tab_ref[table + 1, h])
        return jnp.concatenate([a * cosine - b * sine, b * cosine + a * sine], axis=1).astype(BF16)

    def absorb(l, j, count, block_of):
        at = pl.ds(pl.multiple_of(j * share, share), share * count)
        parts = []
        square = sqa[...]
        for i in range(count):
            block = block_of(j + i)
            for k in range(0, share, 128):
                square = square + block[:, k : k + 128] * block[:, k : k + 128]
            one = pl.ds(pl.multiple_of((j + i) * share, share), share)
            gain = ng_ref[l : l + 1, one].astype(F32)
            scaled = (block * gain).astype(BF16)
            nv[:, one] = scaled
            parts.append(scaled)
        sqa[...] = square
        both = jnp.concatenate(parts, axis=1) if count > 1 else parts[0]
        qka[...] += jnp.dot(both, wqk[l, at, :], preferred_element_type=F32)
        if l:
            vga[...] += nt_dot(both, wvg[l, :, at])

    def unpack(j):
        at = pl.ds(j * share if isinstance(j, int) else pl.multiple_of(j * share, share), share)
        return xr[:, :, at].astype(F32).reshape(rows, share)

    def clear():
        sqa[...] = jnp.zeros_like(sqa)
        qka[...] = jnp.zeros_like(qka)
        vga[...] = jnp.zeros_like(vga)

    for l in range(layers):
        if l == 0:
            with scope("absorb"):
                clear()
                per = n // XPARTS
                loads["ng"].wait()
                for p in range(XPARTS):
                    with scope(f"await{p}"):
                        for name in (("x", p), ("q", 0, p), ("k", 0, p)):
                            loads[name].wait()
                    if p == XPARTS - 1:
                        load_rest()
                    absorb(0, p * per, per, unpack)

        with scope(f"qk{l}"):
            scale = lax.rsqrt(jnp.sum(sqa[...], axis=1, keepdims=True) / width + EPS_RMS)
            both = (qka[...] * scale).astype(BF16)
            qg[l, me] = both[:, :cols]
            kg[l, me] = both[:, cols:]
        if l == 0:
            with scope("bar"):
                pl.semaphore_wait(barrier, n - 1)

        q_start, q_z, q_y, q_done, _ = ring(f"q{l}", qg.at[l], aq_r, ag_s.at[l], None, (), (near[-1],))
        k_start, k_z, k_y, k_done, k_rest = ring(f"k{l}", kg.at[l], ak_r, ag_s.at[l])
        drains.append((most, ag_s.at[l]))
        q_start()
        k_start(others=False)
        if l == 0:
            with scope("masks"):
                make_masks()
                xs[0, me] = unpack(me).astype(BF16)
                loads["tab"].wait()
                loads["gg"].wait()
        q_done(0, 0)
        k_done(0, 0)
        with scope(f"scores{l}"):
            rk = rotated(kg, l, chip, 2)
            scores = (nt_dot(rotated(qg, l, chip, 0), rk) * causal).astype(BF16)
            sc[l, chip] = nt_dot(pick, scores)
            for o, side in [(o, side) for o in far for side in (1, 0)] + [(0, 1)]:
                slot = sc.at[l, chip]
                remote(
                    slot, slot, ag_s.at[layers + l], sc_r.at[0],
                    at_z(o, 1 - yy if side else yy, core),
                ).start()
            drains.append((sc.at[l, pl.ds(0, nc - 1)], ag_s.at[layers + l]))
        k_start(other_core=False)
        for c in range(nc):
            at = pl.ds(pl.multiple_of((2 * c + 1 - core) * share, share), share)
            remote(ow_hbm.at[l, :, at], wop.at[l, c], wo_s.at[l], wo_r.at[0], partner).start()
        drains.append((wop.at[l], wo_s.at[l]))

        with scope(f"vg{l}"):
            if l == 0:
                loads[("v", l)].wait()
                vga[:, :he] = nt_dot(nv[...], wvg[l, :he])
            values = (vga[:, :he] * scale).astype(BF16)
            vts[...] = jnp.transpose(values.astype(F32)).astype(BF16)
            vb[...] = jnp.dot(nth, values, preferred_element_type=F32).reshape(tok, rows, he)
            loads[("s", l)].wait()
        box = {"mixed": jnp.zeros((rows, he), F32)}

        def gate_on(l=l):
            if l == 0:
                with scope(f"gates{l}"):
                    loads[("g", l)].wait()
                    vga[:, he:] = nt_dot(nv[...], wvg[l, he:])

        def carry_one(o, side, l=l):
            h = chip_at(o, 1 - yy if side else yy)
            rq = rotated(qg, l, h, 0)
            state = stv[l, :, h].reshape(be, head_dim).astype(BF16)
            carried = nt_dot(rq, state).astype(BF16) * mkc[...]
            part = jnp.dot(carried, fold[...], preferred_element_type=F32)
            return part * (iota((1, he), 1, te) == h).astype(F32)

        def intra(l=l, box=box):
            with scope(f"intra{l}"):
                others = sc.at[l, pl.ds(0, nc - 1)]
                remote(others, others, ag_s.at[layers + l], sc_r.at[0], partner).wait_recv()
                flat = jnp.concatenate([sc[l, :, t, :] for t in range(tok)], axis=1).astype(BF16)
                wide = lax.dot_general(
                    flat, heads_of.astype(BF16), (((0,), (0,)), ((), ())), preferred_element_type=F32
                )
                box["mixed"] = box["mixed"] + jnp.sum(wide.reshape(tok, rows, he) * vb[...], axis=0)

        def k_on(k_z=k_z, k_y=k_y):
            for o in near:
                k_z(o)
            k_y(0)

        def mix(which, box=box):
            for o, side in which:
                box["mixed"] = box["mixed"] + carry_one(o, side)

        in_order(f"q{l}", q_z, q_y, lambda o, s: None if o == s == 0 else q_done(o, s), mix, gate_on, intra, k_on)
        mixed = box["mixed"]

        with scope(f"sums{l}"):
            both = nt_dot(
                jnp.concatenate([heads_of.astype(BF16)] * 3, axis=1),
                thirds(jnp.concatenate([mixed, mixed * mixed], axis=0), 1),
            )
            sums = both[:, :rows]
            squares = jnp.maximum(both[:, rows:] - sums * sums / e_dim, 0.0)
            sb[l, me] = jnp.concatenate([sums, squares], axis=1).astype(BF16)
            peers = [at_z(o, y, c) for o in far for y in (1 - yy, yy) for c in (core, 1 - core)]
            for device in peers + [at_z(0, 1 - yy, 1 - core), facing, partner]:
                remote(sb.at[l, me], sb.at[l, me], st_s.at[l], st_r.at[0], device).start()
            drains.append((sb.at[l, pl.ds(0, n - 1)], st_s.at[l]))

        def update(h, carry, l=l):
            at = pl.ds(pl.multiple_of(h * e_dim, e_dim), e_dim)
            tall = jnp.broadcast_to(vts[at, :][None], (seqs, e_dim, rows)).reshape(be, rows)
            fresh = jnp.dot(tall * mks[...], rotated(kg, l, h, 2), preferred_element_type=F32)
            row = tab_ref[4, h][0:1, :]
            fade = jnp.concatenate([row, row], axis=1)
            state = stv[l, :, h].reshape(be, head_dim)
            stv[l, :, h] = ((state + fresh) * fade).reshape(seqs, e_dim, head_dim)
            return carry

        with scope(f"silu{l}"):
            gates = (vga[:, he:] * scale).astype(BF16).astype(F32)
            gain = jnp.dot(gg_ref[l].astype(F32), place, preferred_element_type=F32, precision=highest)
            gain = jnp.sum(gain * heads_of, axis=0, keepdims=True)
            gains = gates / (1.0 + jnp.exp(-gates)) * gain
            mgs[l, 0] = mixed
            mgs[l, 1] = gains
            pair = remote(mgs.at[l], mgr.at[l], mg_s.at[l], mg_r.at[0], partner)
            pair.start()
            drains.append((mgs.at[l], mg_s.at[l]))
            loads[("o", l)].wait()
            remote(wop.at[l], wop.at[l], wo_s.at[l], wo_r.at[0], partner).wait_recv()
            pair.wait_recv()

        with scope(f"stwait{l}"):
            others = sb.at[l, pl.ds(0, n - 1)]
            remote(others, others, st_s.at[l], st_r.at[0], partner).wait_recv()

        with scope(f"gated{l}"):
            stats = sb[l].astype(F32)
            sums = stats[:, :, :rows]
            total = jnp.sum(sums, axis=0)
            off = sums - (total / n)[None]
            var = jnp.sum(stats[:, :, rows:] + off * off / e_dim, axis=0) / head_dim
            both = jnp.concatenate([total / head_dim, lax.rsqrt(var + EPS_GROUP)], axis=1)
            both = lax.dot_general(
                thirds(both, 0), jnp.concatenate([heads_of.astype(BF16)] * 3, axis=0),
                (((0,), (0,)), ((), ())), preferred_element_type=F32,
            )
            gated = ((mixed - both[:rows]) * both[rows:] * gains).astype(BF16)
            other = ((mgr[l, 0] - both[:rows]) * both[rows:] * mgr[l, 1]).astype(BF16)

        def paired(o, side, l=l, gated=gated, other=other):
            c = chip_at(o, 1 - yy if side else yy)
            at = pl.ds(pl.multiple_of((2 * c + core) * share, share), share)
            own = jnp.dot(gated, wo[l, :, at], preferred_element_type=F32)
            return own + jnp.dot(other, wop[l, c], preferred_element_type=F32)

        order = list(range(nz - 1, -1, -1))
        ys_s = rz_s = rs_s.at[l]

        early = order[0]
        later = order[1:]
        tail = halves[1]

        def hop(o, at, l=l):
            src, dst = yss.at[l, o, at], ysr.at[l, o, at]
            return remote(src, dst, ys_s, ys_r.at[halves.index(at), o], facing)

        def turn(o, at, l=l):
            src, dst = rss.at[l, o, at], rsr.at[l, o, at]
            return remote(src, dst, rz_s, rs_r.at[halves.index(at)], at_z(o, yy, core))

        def cross(l=l):
            return remote(rss.at[l, 0, tail], rsr.at[l, 0, tail], rz_s, rs_r.at[2], at_z(early, yy, core))

        with scope(f"rsb{l}"):
            both = paired(early, 1).astype(BF16)
            yss[l, early] = both
            hop(early, halves[0]).start()
            rss[l, 0, tail] = both[rows // 2 :]
            cross().start()
            osum[early] = paired(early, 0)
            rss[l, early, tail] = osum[early, tail].astype(BF16)
            turn(early, tail).start()
            for o in later[:-1]:
                yss[l, o] = paired(o, 1).astype(BF16)
                hop(o, halves[0]).start()
            osum[nz] = paired(0, 1)
            yss[l, 0, halves[0]] = osum[nz, halves[0]].astype(BF16)
            hop(0, halves[0]).start()
            for o in later[:-1]:
                hop(o, tail).start()
        with scope(f"rsc{l}"):
            for o in near:
                k_y(o)
            drains.append((xs.at[0, pl.ds(0, 2 * nz - 1)], rs_s.at[l]))
        with scope(f"own{l}"):
            for o in later:
                osum[o] = paired(o, 0)

        def join(o, at, l=l):
            with scope(f"rsd{l}{o}"):
                hop(o, at).wait_recv()
                own = osum[o, at] + ysr[l, o, at].astype(F32)
                if o:
                    rss[l, o, at] = own.astype(BF16)
                    turn(o, at).start()
                else:
                    osum[o, at] = own

        def finish(at, l=l):
            acc = osum[0, at] + xs[l, me, at].astype(F32)
            with scope(f"rse{l}"):
                parts = rsr.at[l, pl.ds(1, nz - 1), at]
                remote(parts, parts, rz_s, rs_r.at[halves.index(at)], facing).wait_recv()
                for o in near:
                    acc = acc + rsr[l, o, at].astype(F32)
            return acc.astype(BF16)

        for o in order:
            join(o, halves[0])
        with scope(f"cross{l}"):
            cross().wait_recv()
            yss[l, 0, tail] = (osum[nz, tail] + rsr[l, 0, tail].astype(F32)).astype(BF16)
            hop(0, tail).start()
        for o in later[:-1]:
            join(o, tail)
        k_rest()
        with scope(f"update{l}"):
            lax.fori_loop(0, heads, update, 0, unroll=True)
        if l + 1 == layers:
            y_ref[halves[0], :] = finish(halves[0])
            join(0, tail)
            y_ref[tail, :] = finish(tail)
            continue

        first, rest, end = xnear[0], xnear[1:], xnear[-1]
        meet = {0: 0, first: 1, nz: 1, nz + first: 3, nz + end: 3}
        meet.update({o: 2 for o in rest})
        meet.update({nz + o: 4 for o in rest[:-1]})
        rings = []
        clear()
        drains.append((most, ag_s.at[2 * layers + l]))
        for i, at in enumerate(halves):
            rings.append(ring(f"x{l}{i}", xs.at[l + 1], ax_r.at[i], ag_s.at[2 * layers + l], at, (xnear[-1],) if i else (), tuple(xnear[1:-1]) if i else (), xnear, meet))
            if i:
                join(0, tail)
            xs[l + 1, me, at] = finish(at)
            rings[i][0]()
        loads[("q", l + 1, 0)].wait()
        loads[("k", l + 1, 0)].wait()
        loads[("v", l + 1)].wait()
        loads[("g", l + 1)].wait()
        (_, az, ay, _, _), (_, bz, by, _, _) = rings

        def use(*which, l=l):
            o, side = which[0]
            both = xs.at[l + 1, pl.ds(0, len(which))]
            with scope(f"x{l}d{side}{o}"):
                remote(both, both, ag_s.at[2 * layers + l], am_r.at[meet[side * nz + o]], partner).wait_recv()
            with scope(f"x{l}c{which[0][1]}{which[0][0]}"):
                for o, side in which:
                    c = chip_at(o, 1 - yy if side else yy)
                    absorb(l + 1, 2 * c, 2, lambda j: xs[l + 1, j].astype(F32))

        az(first)
        ay(0)
        for o in rest:
            az(o)
        bz(first)
        ay(first)
        by(0)
        use((0, 0))
        for o in rest[:-1]:
            ay(o)
            bz(o)
        ay(end)
        bz(end)
        use((first, 0), (0, 1))
        by(first)
        use(*[(o, 0) for o in rest])
        by(end)
        use((first, 1), (end, 1))
        for o in rest[:-1]:
            by(o)
        use(*[(o, 1) for o in rest[:-1]])

    with scope("drain"):
        for ref, sem in drains:
            remote(ref, ref, sem, st_r.at[0], partner).wait_send()


def store_kernel(y_ref, state_ref, y_out, state_out, yv, sem):
    layers, seqs = state_ref.shape[:2]
    copies = []
    parts = sem.shape[0] - 1
    per = layers * seqs // parts
    for i in range(parts):
        l, s = i * per // seqs, pl.ds(i * per % seqs, per)
        copies.append(pltpu.make_async_copy(state_ref.at[l, s], state_out.at[l, s], sem.at[i]))
    for copy in copies:
        copy.start()
    yv[...] = y_ref[...].astype(F32).reshape(yv.shape).astype(BF16)
    copy = pltpu.make_async_copy(yv, y_out, sem.at[parts])
    copy.start()
    for copy in copies + [copy]:
        copy.wait()


def local(
    stream_in, state_in, norm_gain, query_weight, key_weight,
    value_weight, gate_weight, group_gain, output_weight,
):
    n = lax.axis_size("tp")
    seqs, tok, width = stream_in.shape
    layers, _, heads, e_dim, head_dim = state_in.shape
    cols = query_weight.shape[2]
    rows = seqs * tok
    he = heads * e_dim
    share = width // n
    fits = (
        cols == 128 and head_dim == 256 and he == 128 and heads == 8 and e_dim == 16
        and share % 128 == 0 and n % 4 == 0 and n & (n - 1) == 0 and rows == 128 and 8 % tok == 0
        and n == 2 * heads and seqs % 4 == 0 and share == 2 * cols
    )
    if not fits:
        return plain_local(
            stream_in, state_in, norm_gain, query_weight, key_weight,
            value_weight, gate_weight, group_gain, output_weight,
        )
    nc = n // 2
    be = seqs * e_dim
    hbm = pl.BlockSpec(memory_space=pltpu.HBM)
    vmem = pl.BlockSpec(memory_space=pltpu.VMEM)
    dma = pltpu.SemaphoreType.DMA
    tables = jnp.asarray(rotary_tables(heads, tok, head_dim))
    flat = lambda w: jnp.transpose(w, (0, 2, 3, 1)).reshape(layers, he, width)
    y, new_state = pl.pallas_call(
        functools.partial(kernel, n, head_dim),
        name="retention",
        out_shape=(
            pltpu.VMEM((rows, share), BF16),
            pltpu.VMEM(state_in.shape, F32),
        ),
        in_specs=[hbm] * 10,
        out_specs=(vmem, vmem),
        scratch_shapes=[
            pltpu.VMEM(norm_gain.shape, BF16),
            pltpu.VMEM(group_gain.shape, BF16),
            pltpu.VMEM(tables.shape, F32),
            pltpu.VMEM((seqs, tok, width), BF16),
            pltpu.VMEM((layers, n, rows, share), BF16),
            pltpu.VMEM((rows, width), BF16),
            pltpu.VMEM((layers, width, 2 * cols), BF16),
            pltpu.VMEM((layers, 2 * he, width), BF16),
            pltpu.VMEM((layers, he, width), BF16),
            pltpu.VMEM((layers, n, rows, cols), BF16),
            pltpu.VMEM((layers, n, rows, cols), BF16),
            pltpu.VMEM((layers, heads, 8, rows), F32),
            pltpu.VMEM((he, rows), BF16),
            pltpu.VMEM((tok, rows, he), F32),
            pltpu.VMEM((layers, n, heads, 2 * rows), BF16),
            pltpu.VMEM((layers, nc, he, share), BF16),
            pltpu.VMEM((layers, 2, rows, he), F32),
            pltpu.VMEM((layers, 2, rows, he), F32),
            pltpu.VMEM((layers, nc // 2, rows, share), BF16),
            pltpu.VMEM((layers, nc // 2, rows, share), BF16),
            pltpu.VMEM((layers, nc // 2, rows, share), BF16),
            pltpu.VMEM((layers, nc // 2, rows, share), BF16),
            pltpu.VMEM((rows, be), BF16),
            pltpu.VMEM((be, rows), BF16),
            pltpu.VMEM((be, he), BF16),
            pltpu.VMEM((rows, 128), F32),
            pltpu.VMEM((rows, 2 * cols), F32),
            pltpu.VMEM((rows, 2 * he), F32),
            pltpu.VMEM((nc // 2 + 1, rows, share), F32),
            dma((3 * XPARTS + 6 * layers + 1,)),
            dma((3 * layers - 1,)),
            dma((layers,)),
            dma((layers,)),
            dma((n,)),
            dma((nc + 2,)),
            dma((2, nc)),
            dma((5,)),
            dma((1,)),
            dma((1,)),
            dma((layers,)),
            dma((layers,)),
            dma((1,)),
            dma((1,)),
            dma((2, nc // 2)),
            dma((3,)),
        ],
        compiler_params=pltpu.CompilerParams(
            collective_id=0, has_side_effects=True, vmem_limit_bytes=58500000
        ),
    )(
        stream_in, state_in, norm_gain, query_weight, key_weight,
        flat(value_weight), flat(gate_weight), group_gain,
        output_weight.reshape(layers, he, width), tables,
    )
    return pl.pallas_call(
        store_kernel,
        name="store",
        out_shape=(
            jax.ShapeDtypeStruct((seqs, tok, share), BF16),
            jax.ShapeDtypeStruct(state_in.shape, F32),
        ),
        in_specs=[vmem, vmem],
        out_specs=(hbm, hbm),
        scratch_shapes=[pltpu.VMEM((seqs, tok, share), BF16), dma((4 * layers + 1,))],
        compiler_params=pltpu.CompilerParams(vmem_limit_bytes=2 * 2**20),
    )(y, new_state)


def solution(mesh):
    in_specs = (
        P("grp", None, None),
        P(None, "grp", None, "tp", None),
        P(),
        P(None, None, "tp"),
        P(None, None, "tp"),
        P(None, None, None, "tp"),
        P(None, None, None, "tp"),
        P(None, None, "tp"),
        P(None, None, "tp", None),
    )
    out_specs = (P("grp", None, "tp"), P(None, "grp", None, "tp", None))
    return jax.shard_map(local, mesh=mesh, in_specs=in_specs, out_specs=out_specs, check_vma=False)
```

```python
import functools

import jax
import jax.numpy as jnp
import numpy as np
from jax import lax
from jax.experimental import pallas as pl
from jax.experimental.pallas import tpu as pltpu
from jax.sharding import PartitionSpec as P

HEAD_DIM = 256
PAST = 1024


EPS_RMS = 1e-06
EPS_GROUP = 1e-05
ROTARY_BASE = 10000.0


def log_decays(count):
    return jnp.log(1.0 - jnp.power(2.0, -5.0 - jnp.arange(count, dtype=jnp.float32)))


def decay_tables(log_gamma, count):
    steps = jnp.arange(count, dtype=jnp.float32)
    gap = steps[:, None] - steps[None, :]
    intra = jnp.where(
        gap[None] >= 0, jnp.exp(log_gamma[:, None, None] * jnp.maximum(gap, 0.0)[None]), 0.0
    )
    q_decay = jnp.exp(log_gamma[None, :] * (steps[:, None] + 1.0))
    k_decay = jnp.exp(log_gamma[None, :] * (count - 1.0 - steps[:, None]))
    block_decay = jnp.exp(log_gamma * count)
    return (intra, q_decay, k_decay, block_decay)


def rotate(values, offset):
    half_dim = values.shape[-1] // 2
    freqs = jnp.power(
        ROTARY_BASE, -jnp.arange(half_dim, dtype=jnp.float32) * (2.0 / values.shape[-1])
    )
    places = (offset + jnp.arange(values.shape[1])).astype(jnp.float32)
    angles = places[:, None] * freqs[None, :]
    cosine = jnp.cos(angles)[None, :, None, :]
    sine = jnp.sin(angles)[None, :, None, :]
    first = values[..., :half_dim]
    second = values[..., half_dim:]
    return jnp.concatenate(
        [first * cosine - second * sine, second * cosine + first * sine], axis=-1
    )


def plain_local(
    stream_in,
    state_in,
    norm_gain,
    query_weight,
    key_weight,
    value_weight,
    gate_weight,
    group_gain,
    output_weight,
):
    seqs, new_tok, width = stream_in.shape
    heads, local_dim = (value_weight.shape[2], value_weight.shape[3])
    head_dim = HEAD_DIM
    log_gamma = log_decays(heads)
    intra, q_decay, k_decay, block_decay = decay_tables(log_gamma, new_tok)
    highest = lax.Precision.HIGHEST
    share_cols = width // lax.axis_size("tp")
    col_start = lax.axis_index("tp") * share_cols
    layers = state_in.shape[0]
    stream = stream_in
    stream_share = stream_in
    new_states = []
    for layer_no in range(layers):
        stream_f = stream.astype(jnp.float32)
        normed = stream_f * lax.rsqrt(
            jnp.mean(stream_f * stream_f, axis=-1, keepdims=True) + EPS_RMS
        )
        normed = (normed * norm_gain[layer_no].astype(jnp.float32)).astype(jnp.bfloat16)
        flat = normed.reshape(seqs * new_tok, width)
        query_part = jnp.dot(flat, query_weight[layer_no], preferred_element_type=jnp.float32)
        query_part = query_part.astype(jnp.bfloat16).reshape(seqs, new_tok, -1)
        key_part = jnp.dot(flat, key_weight[layer_no], preferred_element_type=jnp.float32)
        key_part = key_part.astype(jnp.bfloat16).reshape(seqs, new_tok, -1)

        def project_local(weight):
            result = jnp.dot(
                flat, weight.reshape(width, heads * local_dim), preferred_element_type=jnp.float32
            )
            result = lax.optimization_barrier(result.astype(jnp.bfloat16))
            return result.astype(jnp.float32).reshape(seqs, new_tok, heads, local_dim)

        values_f = project_local(value_weight[layer_no])
        gates_f = project_local(gate_weight[layer_no])
        queries, key_rows = (
            lax.all_gather(query_part, "tp", axis=2, tiled=True),
            lax.all_gather(key_part, "tp", axis=2, tiled=True),
        )
        queries = queries.astype(jnp.float32).reshape(seqs, new_tok, heads, head_dim)
        key_rows = key_rows.astype(jnp.float32).reshape(seqs, new_tok, heads, head_dim)
        rot_q = rotate(queries, PAST)
        rot_k = rotate(key_rows, PAST) * head_dim ** (-0.5)
        scores = jnp.einsum("bthd,bshd->bhts", rot_q, rot_k, precision=highest) * intra[None]
        inner = jnp.einsum("bhts,bshe->bthe", scores, values_f, precision=highest)
        state = state_in[layer_no]
        carried = (
            jnp.einsum("bthd,bhed->bthe", rot_q, state, precision=highest)
            * q_decay[None, :, :, None]
        )
        mixed = inner + carried
        new_state = state * block_decay[None, :, None, None] + jnp.einsum(
            "bthe,bthd->bhed", values_f, rot_k * k_decay[None, :, :, None], precision=highest
        )
        new_states.append(new_state)
        totals, squares = lax.psum((jnp.sum(mixed, axis=-1), jnp.sum(mixed * mixed, axis=-1)), "tp")
        mean_o = (totals / head_dim)[..., None]
        var_o = (squares / head_dim)[..., None] - mean_o * mean_o
        normal = (
            (mixed - mean_o)
            * lax.rsqrt(var_o + EPS_GROUP)
            * group_gain[layer_no].astype(jnp.float32)[None, None]
        )
        gated = (jax.nn.silu(gates_f) * normal).astype(jnp.bfloat16)
        partial_out = jnp.dot(
            gated.reshape(seqs * new_tok, heads * local_dim),
            output_weight[layer_no].reshape(heads * local_dim, width),
            preferred_element_type=jnp.float32,
        ).reshape(seqs, new_tok, width)
        share_out = lax.psum_scatter(partial_out, "tp", scatter_dimension=2, tiled=True)
        own_cols = lax.dynamic_slice_in_dim(stream, col_start, share_cols, 2)
        stream_share = (own_cols.astype(jnp.float32) + share_out).astype(jnp.bfloat16)
        if layer_no + 1 < layers:
            stream = lax.all_gather(stream_share, "tp", axis=2, tiled=True)
    result = stream_share
    return (result, jnp.stack(new_states))


F32 = jnp.float32
BF16 = jnp.bfloat16
XPARTS = 4
scope = jax.named_scope


def nt_dot(a, b, precision=None):
    return lax.dot_general(
        a, b, (((1,), (1,)), ((), ())), preferred_element_type=F32, precision=precision
    )


def thirds(value, axis):
    high = value.astype(BF16)
    rest = value - high.astype(F32)
    middle = rest.astype(BF16)
    low = (rest - middle.astype(F32)).astype(BF16)
    return jnp.concatenate([high, middle, low], axis=axis)


def log2(value):
    return int(value).bit_length() - 1


def rotary_tables(heads, new_tok, head_dim):
    half = head_dim // 2
    freqs = np.power(
        np.float32(ROTARY_BASE), -np.arange(half, dtype=np.float32) * np.float32(2.0 / head_dim)
    ).astype(np.float32)
    tok = np.arange(8) % new_tok
    places = (PAST + tok).astype(np.float32)
    angles = (places[:, None] * freqs[None, :]).astype(np.float32).astype(np.float64)
    gamma = 1.0 - np.power(2.0, -5.0 - np.arange(heads))
    grow = np.power(gamma[:, None], tok[None, :] + 1.0)[:, :, None]
    shrink = head_dim ** (-0.5) / grow
    cosine, sine = np.cos(angles)[None], np.sin(angles)[None]
    block = np.broadcast_to(np.power(gamma, new_tok)[:, None, None], (heads, 8, half))
    return np.stack(
        [cosine * grow, sine * grow, cosine * shrink, sine * shrink, block]
    ).astype(np.float32)


def kernel(
    n, head_dim,
    x_hbm, st_hbm, ng_hbm, qw_hbm, kw_hbm, vw_hbm, gw_hbm, gg_hbm, ow_hbm, tab_hbm,
    y_ref, stv,
    ng_ref, gg_ref, tab_ref, xr, xs, nv, wqk, wvg, wo, qg, kg, sc, vts, vb, sb, wop, mgs, mgr, yss, ysr, rss, rsr, mkc, mks, fold, sqa, qka, vga, osum,
    lsem, ag_s, st_s, rs_s, aq_r, ak_r, ax_r, am_r, sc_r, st_r, wo_s, mg_s, wo_r, mg_r, ys_r, rs_r,
):
    layers, seqs, heads, e_dim, _ = st_hbm.shape
    tok = x_hbm.shape[1]
    width = x_hbm.shape[2]
    rows = seqs * tok
    share = width // n
    cols = qw_hbm.shape[2]
    he = heads * e_dim
    half = head_dim // 2
    nc = n // 2
    me = lax.axis_index("tp")
    core = lax.rem(me, 2)
    chip = lax.div(me, 2)
    partner = chip * 2 + 1 - core

    nz = nc // 2
    yy = lax.rem(chip, 2)
    zz = lax.div(chip, 2)

    def chip_at(o, y):
        z, bit = zz, 1
        while bit < nz:
            if o & bit:
                z = z + bit - 2 * bit * lax.rem(lax.div(z, bit), 2)
            bit = 2 * bit
        return z * 2 + y

    def at_z(o, y, c):
        return chip_at(o, y) * 2 + c

    facing = at_z(0, 1 - yy, core)
    far = list(range(2, nz)) + [1]
    xnear = list(range(1, nz))
    near = [1] + list(range(nz - 1, 1, -1))

    def remote(src, dst, ssem, rsem, device):
        return pltpu.make_async_remote_copy(
            src_ref=src, dst_ref=dst, send_sem=ssem, recv_sem=rsem,
            device_id={"tp": device}, device_id_type=pl.DeviceIdType.MESH,
        )

    loads = {}
    count = 0

    def load(name, src, dst):
        nonlocal count
        loads[name] = pltpu.make_async_copy(src, dst, lsem.at[count])
        loads[name].start()
        count += 1

    wide = width // XPARTS

    def load_queries(l, deep, j):
        at = pl.ds(j * deep, deep)
        load(("q", l, j), qw_hbm.at[l, at], wqk.at[l, at, pl.ds(0, cols)])
        load(("k", l, j), kw_hbm.at[l, at], wqk.at[l, at, pl.ds(cols, cols)])

    load("ng", ng_hbm, ng_ref)
    for j in range(XPARTS):
        at = pl.ds(j * wide, wide)
        load(("x", j), x_hbm.at[:, :, at], xr.at[:, :, at])
        load_queries(0, wide, j)

    barrier = pltpu.get_barrier_semaphore()
    for o in range(1, n):
        pl.semaphore_signal(
            barrier, inc=1, device_id={"tp": lax.rem(me + o, n)},
            device_id_type=pl.DeviceIdType.MESH,
        )

    def load_rest():
        for l in range(layers):
            if l:
                load_queries(l, width, 0)
            load(("v", l), vw_hbm.at[l], wvg.at[l, pl.ds(0, he)])
            load(("g", l), gw_hbm.at[l], wvg.at[l, pl.ds(he, he)])
            load(("s", l), st_hbm.at[l], stv.at[l])
            if l == 0:
                load("tab", tab_hbm, tab_ref)
                load("gg", gg_hbm, gg_ref)
            load(("o", l), ow_hbm.at[l], wo.at[l])

    be = seqs * e_dim

    def iota(shape, dim, shift=0):
        return jnp.right_shift(lax.broadcasted_iota(jnp.int32, shape, dim), shift)

    te, tt = log2(e_dim), log2(tok)
    low = e_dim - 1
    causal = (
        (iota((rows, rows), 0, tt) == iota((rows, rows), 1, tt))
        & (iota((rows, rows), 0) >= iota((rows, rows), 1))
    ).astype(F32)
    heads_of = (iota((heads, he), 0) == iota((heads, he), 1, te)).astype(F32)
    place = (
        iota((e_dim, he), 0) == jnp.bitwise_and(iota((e_dim, he), 1), low)
    ).astype(F32)
    nth = jnp.concatenate(
        [
            (
                jnp.left_shift(iota((rows, rows), 0, tt), tt) + t == iota((rows, rows), 1)
            ).astype(F32).astype(BF16)
            for t in range(tok)
        ],
        axis=0,
    )
    pick = (
        jnp.bitwise_and(iota((8, rows), 1), tok - 1) == iota((8, rows), 0)
    ).astype(F32).astype(BF16)
    highest = lax.Precision.HIGHEST

    def make_masks():
        mkc[...] = (iota((rows, be), 0, tt) == iota((rows, be), 1, te)).astype(F32).astype(BF16)
        mks[...] = (iota((be, rows), 0, te) == iota((be, rows), 1, tt)).astype(F32).astype(BF16)
        fold[...] = (
            jnp.bitwise_and(iota((be, he), 0), low) == jnp.bitwise_and(iota((be, he), 1), low)
        ).astype(F32).astype(BF16)

    drains = []
    most = xs.at[0, pl.ds(0, n - 1)]
    halves = [pl.ds(i * (rows // 2), rows // 2) for i in range(2)]

    def ring(name, buf, recv, send, at=None, direct=(), twice=(), near=near, meet=None):
        def slot_of(j):
            return buf.at[j] if at is None else buf.at[j, at]

        def sem(k):
            return recv.at[k] if meet is None or k < nc else am_r.at[meet[k - nc]]

        def push(slot, k, device):
            remote(slot, slot, send, sem(k), device).start()

        def arrive(slot, k):
            remote(slot, slot, send, recv.at[k], partner).wait_recv()

        def start(others=True, other_core=True):
            own = slot_of(me)
            if other_core:
                push(own, nc, partner)
            if others:
                push(own, nz, facing)
                for o in near:
                    push(own, o, at_z(o, yy, core))

        def last(k):
            return nc + 1 if recv.shape[0] == nc + 2 and k > nc else k

        def from_z(o):
            with scope(f"{name}z{o}"):
                slot = slot_of(at_z(o, yy, core))
                arrive(slot, o)
                if o not in direct:
                    push(slot, nz + o, facing)
                if o in twice:
                    push(slot, nc + nz + o, at_z(0, 1 - yy, 1 - core))
                push(slot, last(nc + o), partner)

        def from_y(o):
            with scope(f"{name}y{o}"):
                slot = slot_of(at_z(o, 1 - yy, core))
                arrive(slot, nz + o)
                for far_o in direct if o == 0 else ():
                    push(slot, nz + far_o, at_z(far_o, yy, core))
                if o not in twice:
                    push(slot, last(nc + nz + o), partner)

        def done(o, side):
            with scope(f"{name}d{side}{o}"):
                arrive(slot_of(at_z(o, 1 - yy if side else yy, 1 - core)), nc + nz * side + o)

        def done_rest():
            with scope(name + "rest"):
                arrive(slot_of(pl.ds(0, nc - 1)), nc + 1)

        return start, from_z, from_y, done, done_rest

    def in_order(name, from_z, from_y, done, on_chip, early, between, later):
        def use(*which):
            for o, side in which:
                done(o, side)
            with scope(f"{name}c{which[0][1]}{which[0][0]}"):
                on_chip(which)

        use((0, 0))
        from_z(near[0])
        from_y(0)
        early()
        for o in near[1:-1]:
            from_z(o)
        use((near[0], 0), (0, 1))
        from_z(near[-1])
        from_y(near[0])
        use(*[(o, 0) for o in near[1:]])
        for o in near[1:-1]:
            from_y(o)
        between()
        use(*[(o, 1) for o in near[:-1]])
        later()
        from_y(near[-1])
        use((near[-1], 1))

    def spread(table):
        return jnp.broadcast_to(table[None], (rows // 8, 8, half)).reshape(rows, half)

    def rotated(buf, l, h, table):
        a, b = buf[l, 2 * h].astype(F32), buf[l, 2 * h + 1].astype(F32)
        cosine, sine = spread(tab_ref[table, h]), spread(tab_ref[table + 1, h])
        return jnp.concatenate([a * cosine - b * sine, b * cosine + a * sine], axis=1).astype(BF16)

    def absorb(l, j, count, block_of):
        at = pl.ds(pl.multiple_of(j * share, share), share * count)
        parts = []
        square = sqa[...]
        for i in range(count):
            block = block_of(j + i)
            for k in range(0, share, 128):
                square = square + block[:, k : k + 128] * block[:, k : k + 128]
            one = pl.ds(pl.multiple_of((j + i) * share, share), share)
            gain = ng_ref[l : l + 1, one].astype(F32)
            scaled = (block * gain).astype(BF16)
            nv[:, one] = scaled
            parts.append(scaled)
        sqa[...] = square
        both = jnp.concatenate(parts, axis=1) if count > 1 else parts[0]
        qka[...] += jnp.dot(both, wqk[l, at, :], preferred_element_type=F32)
        if l:
            vga[...] += nt_dot(both, wvg[l, :, at])

    def unpack(j):
        at = pl.ds(j * share if isinstance(j, int) else pl.multiple_of(j * share, share), share)
        return xr[:, :, at].astype(F32).reshape(rows, share)

    def clear():
        sqa[...] = jnp.zeros_like(sqa)
        qka[...] = jnp.zeros_like(qka)
        vga[...] = jnp.zeros_like(vga)

    for l in range(layers):
        if l == 0:
            with scope("absorb"):
                clear()
                per = n // XPARTS
                loads["ng"].wait()
                for p in range(XPARTS):
                    with scope(f"await{p}"):
                        for name in (("x", p), ("q", 0, p), ("k", 0, p)):
                            loads[name].wait()
                    if p == XPARTS - 1:
                        load_rest()
                    absorb(0, p * per, per, unpack)

        with scope(f"qk{l}"):
            scale = lax.rsqrt(jnp.sum(sqa[...], axis=1, keepdims=True) / width + EPS_RMS)
            both = (qka[...] * scale).astype(BF16)
            qg[l, me] = both[:, :cols]
            kg[l, me] = both[:, cols:]
        if l == 0:
            with scope("bar"):
                pl.semaphore_wait(barrier, n - 1)

        q_start, q_z, q_y, q_done, _ = ring(f"q{l}", qg.at[l], aq_r, ag_s.at[l], None, (), (near[-1],))
        k_start, k_z, k_y, k_done, k_rest = ring(f"k{l}", kg.at[l], ak_r, ag_s.at[l])
        drains.append((most, ag_s.at[l]))
        q_start()
        k_start(others=False)
        if l == 0:
            with scope("masks"):
                make_masks()
                xs[0, me] = unpack(me).astype(BF16)
                loads["tab"].wait()
                loads["gg"].wait()
        q_done(0, 0)
        k_done(0, 0)
        with scope(f"scores{l}"):
            rk = rotated(kg, l, chip, 2)
            scores = (nt_dot(rotated(qg, l, chip, 0), rk) * causal).astype(BF16)
            sc[l, chip] = nt_dot(pick, scores)
            for o, side in [(o, side) for o in far for side in (1, 0)] + [(0, 1)]:
                slot = sc.at[l, chip]
                remote(
                    slot, slot, ag_s.at[layers + l], sc_r.at[0],
                    at_z(o, 1 - yy if side else yy, core),
                ).start()
            drains.append((sc.at[l, pl.ds(0, nc - 1)], ag_s.at[layers + l]))
        k_start(other_core=False)
        for c in range(nc):
            at = pl.ds(pl.multiple_of((2 * c + 1 - core) * share, share), share)
            remote(ow_hbm.at[l, :, at], wop.at[l, c], wo_s.at[l], wo_r.at[0], partner).start()
        drains.append((wop.at[l], wo_s.at[l]))

        with scope(f"vg{l}"):
            if l == 0:
                loads[("v", l)].wait()
                vga[:, :he] = nt_dot(nv[...], wvg[l, :he])
            values = (vga[:, :he] * scale).astype(BF16)
            vts[...] = jnp.transpose(values.astype(F32)).astype(BF16)
            vb[...] = jnp.dot(nth, values, preferred_element_type=F32).reshape(tok, rows, he)
            loads[("s", l)].wait()
        box = {"mixed": jnp.zeros((rows, he), F32)}

        def gate_on(l=l):
            if l == 0:
                with scope(f"gates{l}"):
                    loads[("g", l)].wait()
                    vga[:, he:] = nt_dot(nv[...], wvg[l, he:])

        def carry_one(o, side, l=l):
            h = chip_at(o, 1 - yy if side else yy)
            rq = rotated(qg, l, h, 0)
            state = stv[l, :, h].reshape(be, head_dim).astype(BF16)
            carried = nt_dot(rq, state).astype(BF16) * mkc[...]
            part = jnp.dot(carried, fold[...], preferred_element_type=F32)
            return part * (iota((1, he), 1, te) == h).astype(F32)

        def intra(l=l, box=box):
            with scope(f"intra{l}"):
                others = sc.at[l, pl.ds(0, nc - 1)]
                remote(others, others, ag_s.at[layers + l], sc_r.at[0], partner).wait_recv()
                flat = jnp.concatenate([sc[l, :, t, :] for t in range(tok)], axis=1).astype(BF16)
                wide = lax.dot_general(
                    flat, heads_of.astype(BF16), (((0,), (0,)), ((), ())), preferred_element_type=F32
                )
                box["mixed"] = box["mixed"] + jnp.sum(wide.reshape(tok, rows, he) * vb[...], axis=0)

        def k_on(k_z=k_z, k_y=k_y):
            for o in near[:-1]:
                k_z(o)
            k_y(0)

        def mix(which, box=box):
            for o, side in which:
                box["mixed"] = box["mixed"] + carry_one(o, side)

        in_order(f"q{l}", q_z, q_y, lambda o, s: None if o == s == 0 else q_done(o, s), mix, gate_on, intra, k_on)
        mixed = box["mixed"]

        with scope(f"sums{l}"):
            both = nt_dot(
                jnp.concatenate([heads_of.astype(BF16)] * 3, axis=1),
                thirds(jnp.concatenate([mixed, mixed * mixed], axis=0), 1),
            )
            sums = both[:, :rows]
            squares = jnp.maximum(both[:, rows:] - sums * sums / e_dim, 0.0)
            sb[l, me] = jnp.concatenate([sums, squares], axis=1).astype(BF16)
            peers = [at_z(o, y, c) for o in far for y in (1 - yy, yy) for c in (core, 1 - core)]
            for device in peers + [at_z(0, 1 - yy, 1 - core), facing, partner]:
                remote(sb.at[l, me], sb.at[l, me], st_s.at[l], st_r.at[0], device).start()
            drains.append((sb.at[l, pl.ds(0, n - 1)], st_s.at[l]))

        def update(h, carry, l=l):
            at = pl.ds(pl.multiple_of(h * e_dim, e_dim), e_dim)
            tall = jnp.broadcast_to(vts[at, :][None], (seqs, e_dim, rows)).reshape(be, rows)
            fresh = jnp.dot(tall * mks[...], rotated(kg, l, h, 2), preferred_element_type=F32)
            row = tab_ref[4, h][0:1, :]
            fade = jnp.concatenate([row, row], axis=1)
            state = stv[l, :, h].reshape(be, head_dim)
            stv[l, :, h] = ((state + fresh) * fade).reshape(seqs, e_dim, head_dim)
            return carry

        k_z(near[-1])
        with scope(f"silu{l}"):
            gates = (vga[:, he:] * scale).astype(BF16).astype(F32)
            gain = jnp.dot(gg_ref[l].astype(F32), place, preferred_element_type=F32, precision=highest)
            gain = jnp.sum(gain * heads_of, axis=0, keepdims=True)
            gains = gates / (1.0 + jnp.exp(-gates)) * gain
            mgs[l, 0] = mixed
            mgs[l, 1] = gains
            pair = remote(mgs.at[l], mgr.at[l], mg_s.at[l], mg_r.at[0], partner)
            pair.start()
            drains.append((mgs.at[l], mg_s.at[l]))
            loads[("o", l)].wait()
            remote(wop.at[l], wop.at[l], wo_s.at[l], wo_r.at[0], partner).wait_recv()
            pair.wait_recv()

        with scope(f"stwait{l}"):
            others = sb.at[l, pl.ds(0, n - 1)]
            remote(others, others, st_s.at[l], st_r.at[0], partner).wait_recv()

        with scope(f"gated{l}"):
            stats = sb[l].astype(F32)
            sums = stats[:, :, :rows]
            total = jnp.sum(sums, axis=0)
            off = sums - (total / n)[None]
            var = jnp.sum(stats[:, :, rows:] + off * off / e_dim, axis=0) / head_dim
            both = jnp.concatenate([total / head_dim, lax.rsqrt(var + EPS_GROUP)], axis=1)
            both = lax.dot_general(
                thirds(both, 0), jnp.concatenate([heads_of.astype(BF16)] * 3, axis=0),
                (((0,), (0,)), ((), ())), preferred_element_type=F32,
            )
            gated = ((mixed - both[:rows]) * both[rows:] * gains).astype(BF16)
            other = ((mgr[l, 0] - both[:rows]) * both[rows:] * mgr[l, 1]).astype(BF16)

        def paired(o, side, l=l, gated=gated, other=other):
            c = chip_at(o, 1 - yy if side else yy)
            at = pl.ds(pl.multiple_of((2 * c + core) * share, share), share)
            own = jnp.dot(gated, wo[l, :, at], preferred_element_type=F32)
            return own + jnp.dot(other, wop[l, c], preferred_element_type=F32)

        order = list(range(nz - 1, -1, -1))
        ys_s = rz_s = rs_s.at[l]

        early = order[0]
        later = order[1:]
        tail = halves[1]

        def hop(o, at, l=l):
            src, dst = yss.at[l, o, at], ysr.at[l, o, at]
            return remote(src, dst, ys_s, ys_r.at[halves.index(at), o], facing)

        def turn(o, at, l=l):
            src, dst = rss.at[l, o, at], rsr.at[l, o, at]
            return remote(src, dst, rz_s, rs_r.at[halves.index(at)], at_z(o, yy, core))

        def cross(l=l):
            return remote(rss.at[l, 0, tail], rsr.at[l, 0, tail], rz_s, rs_r.at[2], at_z(early, yy, core))

        with scope(f"rsb{l}"):
            both = paired(early, 1).astype(BF16)
            yss[l, early] = both
            hop(early, halves[0]).start()
            rss[l, 0, tail] = both[rows // 2 :]
            cross().start()
            osum[early] = paired(early, 0)
            rss[l, early, tail] = osum[early, tail].astype(BF16)
            turn(early, tail).start()
            for o in later[:-1]:
                yss[l, o] = paired(o, 1).astype(BF16)
                hop(o, halves[0]).start()
            osum[nz] = paired(0, 1)
            yss[l, 0, halves[0]] = osum[nz, halves[0]].astype(BF16)
            hop(0, halves[0]).start()
            for o in later[:-1]:
                hop(o, tail).start()
        with scope(f"rsc{l}"):
            for o in near:
                k_y(o)
            drains.append((xs.at[0, pl.ds(0, 2 * nz - 1)], rs_s.at[l]))
        with scope(f"own{l}"):
            for o in later:
                osum[o] = paired(o, 0)

        def join(o, at, l=l):
            with scope(f"rsd{l}{o}"):
                hop(o, at).wait_recv()
                own = osum[o, at] + ysr[l, o, at].astype(F32)
                if o:
                    rss[l, o, at] = own.astype(BF16)
                    turn(o, at).start()
                else:
                    osum[o, at] = own

        def finish(at, l=l):
            acc = osum[0, at] + xs[l, me, at].astype(F32)
            with scope(f"rse{l}"):
                parts = rsr.at[l, pl.ds(1, nz - 1), at]
                remote(parts, parts, rz_s, rs_r.at[halves.index(at)], facing).wait_recv()
                for o in near:
                    acc = acc + rsr[l, o, at].astype(F32)
            return acc.astype(BF16)

        k_rest()
        with scope(f"update{l}"):
            lax.fori_loop(0, heads, update, 0, unroll=True)
        for o in order:
            join(o, halves[0])
        with scope(f"cross{l}"):
            cross().wait_recv()
            yss[l, 0, tail] = (osum[nz, tail] + rsr[l, 0, tail].astype(F32)).astype(BF16)
            hop(0, tail).start()
        for o in later[:-1]:
            join(o, tail)
        if l + 1 == layers:
            y_ref[halves[0], :] = finish(halves[0])
            join(0, tail)
            y_ref[tail, :] = finish(tail)
            continue

        first, rest, end = xnear[0], xnear[1:], xnear[-1]
        meet = {0: 0, first: 1, nz: 1, nz + first: 3, nz + end: 3}
        meet.update({o: 2 for o in rest})
        meet.update({nz + o: 4 for o in rest[:-1]})
        rings = []
        clear()
        drains.append((most, ag_s.at[2 * layers + l]))
        for i, at in enumerate(halves):
            rings.append(ring(f"x{l}{i}", xs.at[l + 1], ax_r.at[i], ag_s.at[2 * layers + l], at, (xnear[-1],) if i else (), tuple(xnear[1:-1]) if i else (), xnear, meet))
            if i:
                join(0, tail)
            xs[l + 1, me, at] = finish(at)
            rings[i][0]()
        loads[("q", l + 1, 0)].wait()
        loads[("k", l + 1, 0)].wait()
        loads[("v", l + 1)].wait()
        loads[("g", l + 1)].wait()
        (_, az, ay, _, _), (_, bz, by, _, _) = rings

        def use(*which, l=l):
            o, side = which[0]
            both = xs.at[l + 1, pl.ds(0, len(which))]
            with scope(f"x{l}d{side}{o}"):
                remote(both, both, ag_s.at[2 * layers + l], am_r.at[meet[side * nz + o]], partner).wait_recv()
            with scope(f"x{l}c{which[0][1]}{which[0][0]}"):
                for o, side in which:
                    c = chip_at(o, 1 - yy if side else yy)
                    absorb(l + 1, 2 * c, 2, lambda j: xs[l + 1, j].astype(F32))

        az(first)
        ay(0)
        for o in rest:
            az(o)
        bz(first)
        ay(first)
        by(0)
        use((0, 0))
        for o in rest[:-1]:
            ay(o)
            bz(o)
        ay(end)
        bz(end)
        use((first, 0), (0, 1))
        by(first)
        use(*[(o, 0) for o in rest])
        by(end)
        use((first, 1), (end, 1))
        for o in rest[:-1]:
            by(o)
        use(*[(o, 1) for o in rest[:-1]])

    with scope("drain"):
        for ref, sem in drains:
            remote(ref, ref, sem, st_r.at[0], partner).wait_send()


def store_kernel(y_ref, state_ref, y_out, state_out, yv, sem):
    layers, seqs = state_ref.shape[:2]
    copies = []
    parts = sem.shape[0] - 1
    per = layers * seqs // parts
    for i in range(parts):
        l, s = i * per // seqs, pl.ds(i * per % seqs, per)
        copies.append(pltpu.make_async_copy(state_ref.at[l, s], state_out.at[l, s], sem.at[i]))
    for copy in copies:
        copy.start()
    yv[...] = y_ref[...].astype(F32).reshape(yv.shape).astype(BF16)
    copy = pltpu.make_async_copy(yv, y_out, sem.at[parts])
    copy.start()
    for copy in copies + [copy]:
        copy.wait()


def local(
    stream_in, state_in, norm_gain, query_weight, key_weight,
    value_weight, gate_weight, group_gain, output_weight,
):
    n = lax.axis_size("tp")
    seqs, tok, width = stream_in.shape
    layers, _, heads, e_dim, head_dim = state_in.shape
    cols = query_weight.shape[2]
    rows = seqs * tok
    he = heads * e_dim
    share = width // n
    fits = (
        cols == 128 and head_dim == 256 and he == 128 and heads == 8 and e_dim == 16
        and share % 128 == 0 and n % 4 == 0 and n & (n - 1) == 0 and rows == 128 and 8 % tok == 0
        and n == 2 * heads and seqs % 4 == 0 and share == 2 * cols
    )
    if not fits:
        return plain_local(
            stream_in, state_in, norm_gain, query_weight, key_weight,
            value_weight, gate_weight, group_gain, output_weight,
        )
    nc = n // 2
    be = seqs * e_dim
    hbm = pl.BlockSpec(memory_space=pltpu.HBM)
    vmem = pl.BlockSpec(memory_space=pltpu.VMEM)
    dma = pltpu.SemaphoreType.DMA
    tables = jnp.asarray(rotary_tables(heads, tok, head_dim))
    flat = lambda w: jnp.transpose(w, (0, 2, 3, 1)).reshape(layers, he, width)
    y, new_state = pl.pallas_call(
        functools.partial(kernel, n, head_dim),
        name="retention",
        out_shape=(
            pltpu.VMEM((rows, share), BF16),
            pltpu.VMEM(state_in.shape, F32),
        ),
        in_specs=[hbm] * 10,
        out_specs=(vmem, vmem),
        scratch_shapes=[
            pltpu.VMEM(norm_gain.shape, BF16),
            pltpu.VMEM(group_gain.shape, BF16),
            pltpu.VMEM(tables.shape, F32),
            pltpu.VMEM((seqs, tok, width), BF16),
            pltpu.VMEM((layers, n, rows, share), BF16),
            pltpu.VMEM((rows, width), BF16),
            pltpu.VMEM((layers, width, 2 * cols), BF16),
            pltpu.VMEM((layers, 2 * he, width), BF16),
            pltpu.VMEM((layers, he, width), BF16),
            pltpu.VMEM((layers, n, rows, cols), BF16),
            pltpu.VMEM((layers, n, rows, cols), BF16),
            pltpu.VMEM((layers, heads, 8, rows), F32),
            pltpu.VMEM((he, rows), BF16),
            pltpu.VMEM((tok, rows, he), F32),
            pltpu.VMEM((layers, n, heads, 2 * rows), BF16),
            pltpu.VMEM((layers, nc, he, share), BF16),
            pltpu.VMEM((layers, 2, rows, he), F32),
            pltpu.VMEM((layers, 2, rows, he), F32),
            pltpu.VMEM((layers, nc // 2, rows, share), BF16),
            pltpu.VMEM((layers, nc // 2, rows, share), BF16),
            pltpu.VMEM((layers, nc // 2, rows, share), BF16),
            pltpu.VMEM((layers, nc // 2, rows, share), BF16),
            pltpu.VMEM((rows, be), BF16),
            pltpu.VMEM((be, rows), BF16),
            pltpu.VMEM((be, he), BF16),
            pltpu.VMEM((rows, 128), F32),
            pltpu.VMEM((rows, 2 * cols), F32),
            pltpu.VMEM((rows, 2 * he), F32),
            pltpu.VMEM((nc // 2 + 1, rows, share), F32),
            dma((3 * XPARTS + 6 * layers + 1,)),
            dma((3 * layers - 1,)),
            dma((layers,)),
            dma((layers,)),
            dma((n,)),
            dma((nc + 2,)),
            dma((2, nc)),
            dma((5,)),
            dma((1,)),
            dma((1,)),
            dma((layers,)),
            dma((layers,)),
            dma((1,)),
            dma((1,)),
            dma((2, nc // 2)),
            dma((3,)),
        ],
        compiler_params=pltpu.CompilerParams(
            collective_id=0, has_side_effects=True, vmem_limit_bytes=58500000
        ),
    )(
        stream_in, state_in, norm_gain, query_weight, key_weight,
        flat(value_weight), flat(gate_weight), group_gain,
        output_weight.reshape(layers, he, width), tables,
    )
    return pl.pallas_call(
        store_kernel,
        name="store",
        out_shape=(
            jax.ShapeDtypeStruct((seqs, tok, share), BF16),
            jax.ShapeDtypeStruct(state_in.shape, F32),
        ),
        in_specs=[vmem, vmem],
        out_specs=(hbm, hbm),
        scratch_shapes=[pltpu.VMEM((seqs, tok, share), BF16), dma((4 * layers + 1,))],
        compiler_params=pltpu.CompilerParams(vmem_limit_bytes=2 * 2**20),
    )(y, new_state)


def solution(mesh):
    in_specs = (
        P("grp", None, None),
        P(None, "grp", None, "tp", None),
        P(),
        P(None, None, "tp"),
        P(None, None, "tp"),
        P(None, None, None, "tp"),
        P(None, None, None, "tp"),
        P(None, None, "tp"),
        P(None, None, "tp", None),
    )
    out_specs = (P("grp", None, "tp"), P(None, "grp", None, "tp", None))
    return jax.shard_map(local, mesh=mesh, in_specs=in_specs, out_specs=out_specs, check_vma=False)
```

```python
import functools

import jax
import jax.numpy as jnp
import numpy as np
from jax import lax
from jax.experimental import pallas as pl
from jax.experimental.pallas import tpu as pltpu
from jax.sharding import PartitionSpec as P

HEAD_DIM = 256
PAST = 1024


EPS_RMS = 1e-06
EPS_GROUP = 1e-05
ROTARY_BASE = 10000.0


def log_decays(count):
    return jnp.log(1.0 - jnp.power(2.0, -5.0 - jnp.arange(count, dtype=jnp.float32)))


def decay_tables(log_gamma, count):
    steps = jnp.arange(count, dtype=jnp.float32)
    gap = steps[:, None] - steps[None, :]
    intra = jnp.where(
        gap[None] >= 0, jnp.exp(log_gamma[:, None, None] * jnp.maximum(gap, 0.0)[None]), 0.0
    )
    q_decay = jnp.exp(log_gamma[None, :] * (steps[:, None] + 1.0))
    k_decay = jnp.exp(log_gamma[None, :] * (count - 1.0 - steps[:, None]))
    block_decay = jnp.exp(log_gamma * count)
    return (intra, q_decay, k_decay, block_decay)


def rotate(values, offset):
    half_dim = values.shape[-1] // 2
    freqs = jnp.power(
        ROTARY_BASE, -jnp.arange(half_dim, dtype=jnp.float32) * (2.0 / values.shape[-1])
    )
    places = (offset + jnp.arange(values.shape[1])).astype(jnp.float32)
    angles = places[:, None] * freqs[None, :]
    cosine = jnp.cos(angles)[None, :, None, :]
    sine = jnp.sin(angles)[None, :, None, :]
    first = values[..., :half_dim]
    second = values[..., half_dim:]
    return jnp.concatenate(
        [first * cosine - second * sine, second * cosine + first * sine], axis=-1
    )


def plain_local(
    stream_in,
    state_in,
    norm_gain,
    query_weight,
    key_weight,
    value_weight,
    gate_weight,
    group_gain,
    output_weight,
):
    seqs, new_tok, width = stream_in.shape
    heads, local_dim = (value_weight.shape[2], value_weight.shape[3])
    head_dim = HEAD_DIM
    log_gamma = log_decays(heads)
    intra, q_decay, k_decay, block_decay = decay_tables(log_gamma, new_tok)
    highest = lax.Precision.HIGHEST
    share_cols = width // lax.axis_size("tp")
    col_start = lax.axis_index("tp") * share_cols
    layers = state_in.shape[0]
    stream = stream_in
    stream_share = stream_in
    new_states = []
    for layer_no in range(layers):
        stream_f = stream.astype(jnp.float32)
        normed = stream_f * lax.rsqrt(
            jnp.mean(stream_f * stream_f, axis=-1, keepdims=True) + EPS_RMS
        )
        normed = (normed * norm_gain[layer_no].astype(jnp.float32)).astype(jnp.bfloat16)
        flat = normed.reshape(seqs * new_tok, width)
        query_part = jnp.dot(flat, query_weight[layer_no], preferred_element_type=jnp.float32)
        query_part = query_part.astype(jnp.bfloat16).reshape(seqs, new_tok, -1)
        key_part = jnp.dot(flat, key_weight[layer_no], preferred_element_type=jnp.float32)
        key_part = key_part.astype(jnp.bfloat16).reshape(seqs, new_tok, -1)

        def project_local(weight):
            result = jnp.dot(
                flat, weight.reshape(width, heads * local_dim), preferred_element_type=jnp.float32
            )
            result = lax.optimization_barrier(result.astype(jnp.bfloat16))
            return result.astype(jnp.float32).reshape(seqs, new_tok, heads, local_dim)

        values_f = project_local(value_weight[layer_no])
        gates_f = project_local(gate_weight[layer_no])
        queries, key_rows = (
            lax.all_gather(query_part, "tp", axis=2, tiled=True),
            lax.all_gather(key_part, "tp", axis=2, tiled=True),
        )
        queries = queries.astype(jnp.float32).reshape(seqs, new_tok, heads, head_dim)
        key_rows = key_rows.astype(jnp.float32).reshape(seqs, new_tok, heads, head_dim)
        rot_q = rotate(queries, PAST)
        rot_k = rotate(key_rows, PAST) * head_dim ** (-0.5)
        scores = jnp.einsum("bthd,bshd->bhts", rot_q, rot_k, precision=highest) * intra[None]
        inner = jnp.einsum("bhts,bshe->bthe", scores, values_f, precision=highest)
        state = state_in[layer_no]
        carried = (
            jnp.einsum("bthd,bhed->bthe", rot_q, state, precision=highest)
            * q_decay[None, :, :, None]
        )
        mixed = inner + carried
        new_state = state * block_decay[None, :, None, None] + jnp.einsum(
            "bthe,bthd->bhed", values_f, rot_k * k_decay[None, :, :, None], precision=highest
        )
        new_states.append(new_state)
        totals, squares = lax.psum((jnp.sum(mixed, axis=-1), jnp.sum(mixed * mixed, axis=-1)), "tp")
        mean_o = (totals / head_dim)[..., None]
        var_o = (squares / head_dim)[..., None] - mean_o * mean_o
        normal = (
            (mixed - mean_o)
            * lax.rsqrt(var_o + EPS_GROUP)
            * group_gain[layer_no].astype(jnp.float32)[None, None]
        )
        gated = (jax.nn.silu(gates_f) * normal).astype(jnp.bfloat16)
        partial_out = jnp.dot(
            gated.reshape(seqs * new_tok, heads * local_dim),
            output_weight[layer_no].reshape(heads * local_dim, width),
            preferred_element_type=jnp.float32,
        ).reshape(seqs, new_tok, width)
        share_out = lax.psum_scatter(partial_out, "tp", scatter_dimension=2, tiled=True)
        own_cols = lax.dynamic_slice_in_dim(stream, col_start, share_cols, 2)
        stream_share = (own_cols.astype(jnp.float32) + share_out).astype(jnp.bfloat16)
        if layer_no + 1 < layers:
            stream = lax.all_gather(stream_share, "tp", axis=2, tiled=True)
    result = stream_share
    return (result, jnp.stack(new_states))


F32 = jnp.float32
BF16 = jnp.bfloat16
XPARTS = 4
scope = jax.named_scope


def nt_dot(a, b, precision=None):
    return lax.dot_general(
        a, b, (((1,), (1,)), ((), ())), preferred_element_type=F32, precision=precision
    )


def thirds(value, axis):
    high = value.astype(BF16)
    rest = value - high.astype(F32)
    middle = rest.astype(BF16)
    low = (rest - middle.astype(F32)).astype(BF16)
    return jnp.concatenate([high, middle, low], axis=axis)


def log2(value):
    return int(value).bit_length() - 1


def rotary_tables(heads, new_tok, head_dim):
    half = head_dim // 2
    freqs = np.power(
        np.float32(ROTARY_BASE), -np.arange(half, dtype=np.float32) * np.float32(2.0 / head_dim)
    ).astype(np.float32)
    tok = np.arange(8) % new_tok
    places = (PAST + tok).astype(np.float32)
    angles = (places[:, None] * freqs[None, :]).astype(np.float32).astype(np.float64)
    gamma = 1.0 - np.power(2.0, -5.0 - np.arange(heads))
    grow = np.power(gamma[:, None], tok[None, :] + 1.0)[:, :, None]
    shrink = head_dim ** (-0.5) / grow
    cosine, sine = np.cos(angles)[None], np.sin(angles)[None]
    block = np.broadcast_to(np.power(gamma, new_tok)[:, None, None], (heads, 8, half))
    return np.stack(
        [cosine * grow, sine * grow, cosine * shrink, sine * shrink, block]
    ).astype(np.float32)


def kernel(
    n, head_dim,
    x_hbm, st_hbm, ng_hbm, qw_hbm, kw_hbm, vw_hbm, gw_hbm, gg_hbm, ow_hbm, tab_hbm,
    y_ref, stv,
    ng_ref, gg_ref, tab_ref, xr, xs, nv, wqk, wvg, wo, qg, kg, sc, vts, vb, sb, wop, mgs, mgr, yss, ysr, rss, rsr, mkc, mks, fold, sqa, qka, vga, osum,
    lsem, ag_s, st_s, rs_s, aq_r, ak_r, ax_r, am_r, sc_r, st_r, wo_s, mg_s, wo_r, mg_r, ys_r, rs_r,
):
    layers, seqs, heads, e_dim, _ = st_hbm.shape
    tok = x_hbm.shape[1]
    width = x_hbm.shape[2]
    rows = seqs * tok
    share = width // n
    cols = qw_hbm.shape[2]
    he = heads * e_dim
    half = head_dim // 2
    nc = n // 2
    me = lax.axis_index("tp")
    core = lax.rem(me, 2)
    chip = lax.div(me, 2)
    partner = chip * 2 + 1 - core

    nz = nc // 2
    yy = lax.rem(chip, 2)
    zz = lax.div(chip, 2)

    def chip_at(o, y):
        z, bit = zz, 1
        while bit < nz:
            if o & bit:
                z = z + bit - 2 * bit * lax.rem(lax.div(z, bit), 2)
            bit = 2 * bit
        return z * 2 + y

    def at_z(o, y, c):
        return chip_at(o, y) * 2 + c

    facing = at_z(0, 1 - yy, core)
    far = list(range(2, nz)) + [1]
    xnear = list(range(1, nz))
    near = [1] + list(range(nz - 1, 1, -1))

    def remote(src, dst, ssem, rsem, device):
        return pltpu.make_async_remote_copy(
            src_ref=src, dst_ref=dst, send_sem=ssem, recv_sem=rsem,
            device_id={"tp": device}, device_id_type=pl.DeviceIdType.MESH,
        )

    loads = {}
    count = 0

    def load(name, src, dst):
        nonlocal count
        loads[name] = pltpu.make_async_copy(src, dst, lsem.at[count])
        loads[name].start()
        count += 1

    wide = width // XPARTS

    def load_queries(l, deep, j):
        at = pl.ds(j * deep, deep)
        load(("q", l, j), qw_hbm.at[l, at], wqk.at[l, at, pl.ds(0, cols)])
        load(("k", l, j), kw_hbm.at[l, at], wqk.at[l, at, pl.ds(cols, cols)])

    load("ng", ng_hbm, ng_ref)
    for j in range(XPARTS):
        at = pl.ds(j * wide, wide)
        load(("x", j), x_hbm.at[:, :, at], xr.at[:, :, at])
        load_queries(0, wide, j)

    barrier = pltpu.get_barrier_semaphore()
    for o in range(1, n):
        pl.semaphore_signal(
            barrier, inc=1, device_id={"tp": lax.rem(me + o, n)},
            device_id_type=pl.DeviceIdType.MESH,
        )

    def load_rest():
        for l in range(layers):
            if l:
                load_queries(l, width, 0)
            load(("v", l), vw_hbm.at[l], wvg.at[l, pl.ds(0, he)])
            load(("g", l), gw_hbm.at[l], wvg.at[l, pl.ds(he, he)])
            load(("s", l), st_hbm.at[l], stv.at[l])
            if l == 0:
                load("tab", tab_hbm, tab_ref)
                load("gg", gg_hbm, gg_ref)
            load(("o", l), ow_hbm.at[l], wo.at[l])

    be = seqs * e_dim

    def iota(shape, dim, shift=0):
        return jnp.right_shift(lax.broadcasted_iota(jnp.int32, shape, dim), shift)

    te, tt = log2(e_dim), log2(tok)
    low = e_dim - 1
    causal = (
        (iota((rows, rows), 0, tt) == iota((rows, rows), 1, tt))
        & (iota((rows, rows), 0) >= iota((rows, rows), 1))
    ).astype(F32)
    heads_of = (iota((heads, he), 0) == iota((heads, he), 1, te)).astype(F32)
    place = (
        iota((e_dim, he), 0) == jnp.bitwise_and(iota((e_dim, he), 1), low)
    ).astype(F32)
    nth = jnp.concatenate(
        [
            (
                jnp.left_shift(iota((rows, rows), 0, tt), tt) + t == iota((rows, rows), 1)
            ).astype(F32).astype(BF16)
            for t in range(tok)
        ],
        axis=0,
    )
    pick = (
        jnp.bitwise_and(iota((8, rows), 1), tok - 1) == iota((8, rows), 0)
    ).astype(F32).astype(BF16)
    highest = lax.Precision.HIGHEST

    def make_masks():
        mkc[...] = (iota((rows, be), 0, tt) == iota((rows, be), 1, te)).astype(F32).astype(BF16)
        mks[...] = (iota((be, rows), 0, te) == iota((be, rows), 1, tt)).astype(F32).astype(BF16)
        fold[...] = (
            jnp.bitwise_and(iota((be, he), 0), low) == jnp.bitwise_and(iota((be, he), 1), low)
        ).astype(F32).astype(BF16)

    drains = []
    most = xs.at[0, pl.ds(0, n - 1)]
    halves = [pl.ds(i * (rows // 2), rows // 2) for i in range(2)]

    def ring(name, buf, recv, send, at=None, direct=(), twice=(), near=near, meet=None):
        def slot_of(j):
            return buf.at[j] if at is None else buf.at[j, at]

        def sem(k):
            return recv.at[k] if meet is None or k < nc else am_r.at[meet[k - nc]]

        def push(slot, k, device):
            remote(slot, slot, send, sem(k), device).start()

        def arrive(slot, k):
            remote(slot, slot, send, recv.at[k], partner).wait_recv()

        def start(others=True, other_core=True):
            own = slot_of(me)
            if other_core:
                push(own, nc, partner)
            if others:
                push(own, nz, facing)
                for o in near:
                    push(own, o, at_z(o, yy, core))

        def last(k):
            return nc + 1 if recv.shape[0] == nc + 2 and k > nc else k

        def from_z(o):
            with scope(f"{name}z{o}"):
                slot = slot_of(at_z(o, yy, core))
                arrive(slot, o)
                if o not in direct:
                    push(slot, nz + o, facing)
                if o in twice:
                    push(slot, nc + nz + o, at_z(0, 1 - yy, 1 - core))
                push(slot, last(nc + o), partner)

        def from_y(o):
            with scope(f"{name}y{o}"):
                slot = slot_of(at_z(o, 1 - yy, core))
                arrive(slot, nz + o)
                for far_o in direct if o == 0 else ():
                    push(slot, nz + far_o, at_z(far_o, yy, core))
                if o not in twice:
                    push(slot, last(nc + nz + o), partner)

        def done(o, side):
            with scope(f"{name}d{side}{o}"):
                arrive(slot_of(at_z(o, 1 - yy if side else yy, 1 - core)), nc + nz * side + o)

        def done_rest():
            with scope(name + "rest"):
                arrive(slot_of(pl.ds(0, nc - 1)), nc + 1)

        return start, from_z, from_y, done, done_rest

    def in_order(name, from_z, from_y, done, on_chip, early, between, later):
        def use(*which):
            for o, side in which:
                done(o, side)
            with scope(f"{name}c{which[0][1]}{which[0][0]}"):
                on_chip(which)

        use((0, 0))
        from_z(near[0])
        from_y(0)
        early()
        for o in near[1:-1]:
            from_z(o)
        use((near[0], 0), (0, 1))
        from_z(near[-1])
        from_y(near[0])
        use(*[(o, 0) for o in near[1:]])
        for o in near[1:-1]:
            from_y(o)
        between()
        use(*[(o, 1) for o in near[:-1]])
        later()
        from_y(near[-1])
        use((near[-1], 1))

    def spread(table):
        return jnp.broadcast_to(table[None], (rows // 8, 8, half)).reshape(rows, half)

    def rotated(buf, l, h, table):
        a, b = buf[l, 2 * h].astype(F32), buf[l, 2 * h + 1].astype(F32)
        cosine, sine = spread(tab_ref[table, h]), spread(tab_ref[table + 1, h])
        return jnp.concatenate([a * cosine - b * sine, b * cosine + a * sine], axis=1).astype(BF16)

    def absorb(l, j, count, block_of):
        at = pl.ds(pl.multiple_of(j * share, share), share * count)
        parts = []
        square = sqa[...]
        for i in range(count):
            block = block_of(j + i)
            for k in range(0, share, 128):
                square = square + block[:, k : k + 128] * block[:, k : k + 128]
            one = pl.ds(pl.multiple_of((j + i) * share, share), share)
            gain = ng_ref[l : l + 1, one].astype(F32)
            scaled = (block * gain).astype(BF16)
            nv[:, one] = scaled
            parts.append(scaled)
        sqa[...] = square
        both = jnp.concatenate(parts, axis=1) if count > 1 else parts[0]
        qka[...] += jnp.dot(both, wqk[l, at, :], preferred_element_type=F32)
        if l:
            vga[...] += nt_dot(both, wvg[l, :, at])

    def unpack(j):
        at = pl.ds(j * share if isinstance(j, int) else pl.multiple_of(j * share, share), share)
        return xr[:, :, at].astype(F32).reshape(rows, share)

    def clear():
        sqa[...] = jnp.zeros_like(sqa)
        qka[...] = jnp.zeros_like(qka)
        vga[...] = jnp.zeros_like(vga)

    def send_rows(l):
        for c in range(nc):
            at = pl.ds(pl.multiple_of((2 * c + 1 - core) * share, share), share)
            remote(ow_hbm.at[l, :, at], wop.at[l, c], wo_s.at[l], wo_r.at[l], partner).start()

    for l in range(layers):
        if l == 0:
            with scope("absorb"):
                clear()
                per = n // XPARTS
                loads["ng"].wait()
                for p in range(XPARTS):
                    with scope(f"await{p}"):
                        for name in (("x", p), ("q", 0, p), ("k", 0, p)):
                            loads[name].wait()
                    if p == XPARTS - 1:
                        load_rest()
                    absorb(0, p * per, per, unpack)

        with scope(f"qk{l}"):
            scale = lax.rsqrt(jnp.sum(sqa[...], axis=1, keepdims=True) / width + EPS_RMS)
            both = (qka[...] * scale).astype(BF16)
            qg[l, me] = both[:, :cols]
            kg[l, me] = both[:, cols:]
        if l == 0:
            with scope("bar"):
                pl.semaphore_wait(barrier, n - 1)

        q_start, q_z, q_y, q_done, _ = ring(f"q{l}", qg.at[l], aq_r, ag_s.at[l], None, (), (near[-1],))
        k_start, k_z, k_y, k_done, k_rest = ring(f"k{l}", kg.at[l], ak_r, ag_s.at[l])
        drains.append((most, ag_s.at[l]))
        q_start()
        k_start(others=False)
        if l == 0:
            with scope("masks"):
                make_masks()
                xs[0, me] = unpack(me).astype(BF16)
                loads["tab"].wait()
                loads["gg"].wait()
        q_done(0, 0)
        k_done(0, 0)
        with scope(f"scores{l}"):
            rk = rotated(kg, l, chip, 2)
            scores = (nt_dot(rotated(qg, l, chip, 0), rk) * causal).astype(BF16)
            sc[l, chip] = nt_dot(pick, scores)
            for o, side in [(o, side) for o in far for side in (1, 0)] + [(0, 1)]:
                slot = sc.at[l, chip]
                remote(
                    slot, slot, ag_s.at[layers + l], sc_r.at[0],
                    at_z(o, 1 - yy if side else yy, core),
                ).start()
            drains.append((sc.at[l, pl.ds(0, nc - 1)], ag_s.at[layers + l]))
        k_start(other_core=False)
        if l == 0:
            send_rows(0)
        drains.append((wop.at[l], wo_s.at[l]))

        with scope(f"vg{l}"):
            if l == 0:
                loads[("v", l)].wait()
                vga[:, :he] = nt_dot(nv[...], wvg[l, :he])
            values = (vga[:, :he] * scale).astype(BF16)
            vts[...] = jnp.transpose(values.astype(F32)).astype(BF16)
            vb[...] = jnp.dot(nth, values, preferred_element_type=F32).reshape(tok, rows, he)
            loads[("s", l)].wait()
        box = {"mixed": jnp.zeros((rows, he), F32)}

        def gate_on(l=l):
            if l == 0:
                with scope(f"gates{l}"):
                    loads[("g", l)].wait()
                    vga[:, he:] = nt_dot(nv[...], wvg[l, he:])

        def carry_one(o, side, l=l):
            h = chip_at(o, 1 - yy if side else yy)
            rq = rotated(qg, l, h, 0)
            state = stv[l, :, h].reshape(be, head_dim).astype(BF16)
            carried = nt_dot(rq, state).astype(BF16) * mkc[...]
            part = jnp.dot(carried, fold[...], preferred_element_type=F32)
            return part * (iota((1, he), 1, te) == h).astype(F32)

        def intra(l=l, box=box):
            with scope(f"intra{l}"):
                others = sc.at[l, pl.ds(0, nc - 1)]
                remote(others, others, ag_s.at[layers + l], sc_r.at[0], partner).wait_recv()
                flat = jnp.concatenate([sc[l, :, t, :] for t in range(tok)], axis=1).astype(BF16)
                wide = lax.dot_general(
                    flat, heads_of.astype(BF16), (((0,), (0,)), ((), ())), preferred_element_type=F32
                )
                box["mixed"] = box["mixed"] + jnp.sum(wide.reshape(tok, rows, he) * vb[...], axis=0)

        def k_on(k_z=k_z, k_y=k_y):
            for o in near[:-1]:
                k_z(o)
            k_y(0)

        def mix(which, box=box):
            for o, side in which:
                box["mixed"] = box["mixed"] + carry_one(o, side)

        in_order(f"q{l}", q_z, q_y, lambda o, s: None if o == s == 0 else q_done(o, s), mix, gate_on, intra, k_on)
        mixed = box["mixed"]

        with scope(f"sums{l}"):
            both = nt_dot(
                jnp.concatenate([heads_of.astype(BF16)] * 3, axis=1),
                thirds(jnp.concatenate([mixed, mixed * mixed], axis=0), 1),
            )
            sums = both[:, :rows]
            squares = jnp.maximum(both[:, rows:] - sums * sums / e_dim, 0.0)
            sb[l, me] = jnp.concatenate([sums, squares], axis=1).astype(BF16)
            peers = [at_z(o, y, c) for o in far for y in (1 - yy, yy) for c in (core, 1 - core)]
            for device in peers + [at_z(0, 1 - yy, 1 - core), facing, partner]:
                remote(sb.at[l, me], sb.at[l, me], st_s.at[l], st_r.at[0], device).start()
            drains.append((sb.at[l, pl.ds(0, n - 1)], st_s.at[l]))

        def update(h, carry, l=l):
            at = pl.ds(pl.multiple_of(h * e_dim, e_dim), e_dim)
            tall = jnp.broadcast_to(vts[at, :][None], (seqs, e_dim, rows)).reshape(be, rows)
            fresh = jnp.dot(tall * mks[...], rotated(kg, l, h, 2), preferred_element_type=F32)
            row = tab_ref[4, h][0:1, :]
            fade = jnp.concatenate([row, row], axis=1)
            state = stv[l, :, h].reshape(be, head_dim)
            stv[l, :, h] = ((state + fresh) * fade).reshape(seqs, e_dim, head_dim)
            return carry

        k_z(near[-1])
        with scope(f"silu{l}"):
            gates = (vga[:, he:] * scale).astype(BF16).astype(F32)
            gain = jnp.dot(gg_ref[l].astype(F32), place, preferred_element_type=F32, precision=highest)
            gain = jnp.sum(gain * heads_of, axis=0, keepdims=True)
            gains = gates / (1.0 + jnp.exp(-gates)) * gain
            mgs[l, 0] = mixed
            mgs[l, 1] = gains
            pair = remote(mgs.at[l], mgr.at[l], mg_s.at[l], mg_r.at[0], partner)
            pair.start()
            drains.append((mgs.at[l], mg_s.at[l]))
            loads[("o", l)].wait()
            remote(wop.at[l], wop.at[l], wo_s.at[l], wo_r.at[l], partner).wait_recv()
            pair.wait_recv()

        with scope(f"stwait{l}"):
            others = sb.at[l, pl.ds(0, n - 1)]
            remote(others, others, st_s.at[l], st_r.at[0], partner).wait_recv()

        with scope(f"gated{l}"):
            stats = sb[l].astype(F32)
            sums = stats[:, :, :rows]
            total = jnp.sum(sums, axis=0)
            off = sums - (total / n)[None]
            var = jnp.sum(stats[:, :, rows:] + off * off / e_dim, axis=0) / head_dim
            both = jnp.concatenate([total / head_dim, lax.rsqrt(var + EPS_GROUP)], axis=1)
            both = lax.dot_general(
                thirds(both, 0), jnp.concatenate([heads_of.astype(BF16)] * 3, axis=0),
                (((0,), (0,)), ((), ())), preferred_element_type=F32,
            )
            gated = ((mixed - both[:rows]) * both[rows:] * gains).astype(BF16)
            other = ((mgr[l, 0] - both[:rows]) * both[rows:] * mgr[l, 1]).astype(BF16)

        def paired(o, side, l=l, gated=gated, other=other):
            c = chip_at(o, 1 - yy if side else yy)
            at = pl.ds(pl.multiple_of((2 * c + core) * share, share), share)
            own = jnp.dot(gated, wo[l, :, at], preferred_element_type=F32)
            return own + jnp.dot(other, wop[l, c], preferred_element_type=F32)

        order = list(range(nz - 1, -1, -1))
        ys_s = rz_s = rs_s.at[l]

        early = order[0]
        later = order[1:]
        tail = halves[1]

        def hop(o, at, l=l):
            src, dst = yss.at[l, o, at], ysr.at[l, o, at]
            return remote(src, dst, ys_s, ys_r.at[halves.index(at), o], facing)

        def turn(o, at, l=l):
            src, dst = rss.at[l, o, at], rsr.at[l, o, at]
            return remote(src, dst, rz_s, rs_r.at[halves.index(at)], at_z(o, yy, core))

        def cross(l=l):
            return remote(rss.at[l, 0, tail], rsr.at[l, 0, tail], rz_s, rs_r.at[2], at_z(early, yy, core))

        with scope(f"rsb{l}"):
            both = paired(early, 1).astype(BF16)
            yss[l, early] = both
            hop(early, halves[0]).start()
            rss[l, 0, tail] = both[rows // 2 :]
            cross().start()
            osum[early] = paired(early, 0)
            rss[l, early, tail] = osum[early, tail].astype(BF16)
            turn(early, tail).start()
            for o in later[:-1]:
                yss[l, o] = paired(o, 1).astype(BF16)
                hop(o, halves[0]).start()
            osum[nz] = paired(0, 1)
            yss[l, 0, halves[0]] = osum[nz, halves[0]].astype(BF16)
            hop(0, halves[0]).start()
            for o in later[:-1]:
                hop(o, tail).start()
        with scope(f"rsc{l}"):
            for o in near:
                k_y(o)
            drains.append((xs.at[0, pl.ds(0, 2 * nz - 1)], rs_s.at[l]))
        if l + 1 < layers:
            send_rows(l + 1)
        with scope(f"own{l}"):
            for o in later:
                osum[o] = paired(o, 0)

        def join(o, at, l=l):
            with scope(f"rsd{l}{o}"):
                hop(o, at).wait_recv()
                own = osum[o, at] + ysr[l, o, at].astype(F32)
                if o:
                    rss[l, o, at] = own.astype(BF16)
                    turn(o, at).start()
                else:
                    osum[o, at] = own

        def finish(at, l=l):
            acc = osum[0, at] + xs[l, me, at].astype(F32)
            with scope(f"rse{l}"):
                parts = rsr.at[l, pl.ds(1, nz - 1), at]
                remote(parts, parts, rz_s, rs_r.at[halves.index(at)], facing).wait_recv()
                for o in near:
                    acc = acc + rsr[l, o, at].astype(F32)
            return acc.astype(BF16)

        k_rest()
        with scope(f"update{l}"):
            lax.fori_loop(0, heads, update, 0, unroll=True)
        for o in order:
            join(o, halves[0])
        with scope(f"cross{l}"):
            cross().wait_recv()
            yss[l, 0, tail] = (osum[nz, tail] + rsr[l, 0, tail].astype(F32)).astype(BF16)
            hop(0, tail).start()
        for o in later[:-1]:
            join(o, tail)
        if l + 1 == layers:
            y_ref[halves[0], :] = finish(halves[0])
            join(0, tail)
            y_ref[tail, :] = finish(tail)
            continue

        first, rest, end = xnear[0], xnear[1:], xnear[-1]
        meet = {0: 0, first: 1, nz: 1, nz + first: 3, nz + end: 3}
        meet.update({o: 2 for o in rest})
        meet.update({nz + o: 4 for o in rest[:-1]})
        rings = []
        clear()
        drains.append((most, ag_s.at[2 * layers + l]))
        for i, at in enumerate(halves):
            rings.append(ring(f"x{l}{i}", xs.at[l + 1], ax_r.at[i], ag_s.at[2 * layers + l], at, (xnear[-1],) if i else (), tuple(xnear[1:-1]) if i else (), xnear, meet))
            if i:
                join(0, tail)
            xs[l + 1, me, at] = finish(at)
            rings[i][0]()
        loads[("q", l + 1, 0)].wait()
        loads[("k", l + 1, 0)].wait()
        loads[("v", l + 1)].wait()
        loads[("g", l + 1)].wait()
        (_, az, ay, _, _), (_, bz, by, _, _) = rings

        def use(*which, l=l):
            o, side = which[0]
            both = xs.at[l + 1, pl.ds(0, len(which))]
            with scope(f"x{l}d{side}{o}"):
                remote(both, both, ag_s.at[2 * layers + l], am_r.at[meet[side * nz + o]], partner).wait_recv()
            with scope(f"x{l}c{which[0][1]}{which[0][0]}"):
                for o, side in which:
                    c = chip_at(o, 1 - yy if side else yy)
                    absorb(l + 1, 2 * c, 2, lambda j: xs[l + 1, j].astype(F32))

        az(first)
        ay(0)
        for o in rest:
            az(o)
        bz(first)
        ay(first)
        by(0)
        use((0, 0))
        for o in rest[:-1]:
            ay(o)
            bz(o)
        ay(end)
        bz(end)
        use((first, 0), (0, 1))
        by(first)
        use(*[(o, 0) for o in rest])
        by(end)
        use((first, 1), (end, 1))
        for o in rest[:-1]:
            by(o)
        use(*[(o, 1) for o in rest[:-1]])

    with scope("drain"):
        for ref, sem in drains:
            remote(ref, ref, sem, st_r.at[0], partner).wait_send()


def store_kernel(y_ref, state_ref, y_out, state_out, yv, sem):
    layers, seqs = state_ref.shape[:2]
    copies = []
    parts = sem.shape[0] - 1
    per = layers * seqs // parts
    for i in range(parts):
        l, s = i * per // seqs, pl.ds(i * per % seqs, per)
        copies.append(pltpu.make_async_copy(state_ref.at[l, s], state_out.at[l, s], sem.at[i]))
    for copy in copies:
        copy.start()
    yv[...] = y_ref[...].astype(F32).reshape(yv.shape).astype(BF16)
    copy = pltpu.make_async_copy(yv, y_out, sem.at[parts])
    copy.start()
    for copy in copies + [copy]:
        copy.wait()


def local(
    stream_in, state_in, norm_gain, query_weight, key_weight,
    value_weight, gate_weight, group_gain, output_weight,
):
    n = lax.axis_size("tp")
    seqs, tok, width = stream_in.shape
    layers, _, heads, e_dim, head_dim = state_in.shape
    cols = query_weight.shape[2]
    rows = seqs * tok
    he = heads * e_dim
    share = width // n
    fits = (
        cols == 128 and head_dim == 256 and he == 128 and heads == 8 and e_dim == 16
        and share % 128 == 0 and n % 4 == 0 and n & (n - 1) == 0 and rows == 128 and 8 % tok == 0
        and n == 2 * heads and seqs % 4 == 0 and share == 2 * cols
    )
    if not fits:
        return plain_local(
            stream_in, state_in, norm_gain, query_weight, key_weight,
            value_weight, gate_weight, group_gain, output_weight,
        )
    nc = n // 2
    be = seqs * e_dim
    hbm = pl.BlockSpec(memory_space=pltpu.HBM)
    vmem = pl.BlockSpec(memory_space=pltpu.VMEM)
    dma = pltpu.SemaphoreType.DMA
    tables = jnp.asarray(rotary_tables(heads, tok, head_dim))
    flat = lambda w: jnp.transpose(w, (0, 2, 3, 1)).reshape(layers, he, width)
    y, new_state = pl.pallas_call(
        functools.partial(kernel, n, head_dim),
        name="retention",
        out_shape=(
            pltpu.VMEM((rows, share), BF16),
            pltpu.VMEM(state_in.shape, F32),
        ),
        in_specs=[hbm] * 10,
        out_specs=(vmem, vmem),
        scratch_shapes=[
            pltpu.VMEM(norm_gain.shape, BF16),
            pltpu.VMEM(group_gain.shape, BF16),
            pltpu.VMEM(tables.shape, F32),
            pltpu.VMEM((seqs, tok, width), BF16),
            pltpu.VMEM((layers, n, rows, share), BF16),
            pltpu.VMEM((rows, width), BF16),
            pltpu.VMEM((layers, width, 2 * cols), BF16),
            pltpu.VMEM((layers, 2 * he, width), BF16),
            pltpu.VMEM((layers, he, width), BF16),
            pltpu.VMEM((layers, n, rows, cols), BF16),
            pltpu.VMEM((layers, n, rows, cols), BF16),
            pltpu.VMEM((layers, heads, 8, rows), F32),
            pltpu.VMEM((he, rows), BF16),
            pltpu.VMEM((tok, rows, he), F32),
            pltpu.VMEM((layers, n, heads, 2 * rows), BF16),
            pltpu.VMEM((layers, nc, he, share), BF16),
            pltpu.VMEM((layers, 2, rows, he), F32),
            pltpu.VMEM((layers, 2, rows, he), F32),
            pltpu.VMEM((layers, nc // 2, rows, share), BF16),
            pltpu.VMEM((layers, nc // 2, rows, share), BF16),
            pltpu.VMEM((layers, nc // 2, rows, share), BF16),
            pltpu.VMEM((layers, nc // 2, rows, share), BF16),
            pltpu.VMEM((rows, be), BF16),
            pltpu.VMEM((be, rows), BF16),
            pltpu.VMEM((be, he), BF16),
            pltpu.VMEM((rows, 128), F32),
            pltpu.VMEM((rows, 2 * cols), F32),
            pltpu.VMEM((rows, 2 * he), F32),
            pltpu.VMEM((nc // 2 + 1, rows, share), F32),
            dma((3 * XPARTS + 6 * layers + 1,)),
            dma((3 * layers - 1,)),
            dma((layers,)),
            dma((layers,)),
            dma((n,)),
            dma((nc + 2,)),
            dma((2, nc)),
            dma((5,)),
            dma((1,)),
            dma((1,)),
            dma((layers,)),
            dma((layers,)),
            dma((layers,)),
            dma((1,)),
            dma((2, nc // 2)),
            dma((3,)),
        ],
        compiler_params=pltpu.CompilerParams(
            collective_id=0, has_side_effects=True, vmem_limit_bytes=58500000
        ),
    )(
        stream_in, state_in, norm_gain, query_weight, key_weight,
        flat(value_weight), flat(gate_weight), group_gain,
        output_weight.reshape(layers, he, width), tables,
    )
    return pl.pallas_call(
        store_kernel,
        name="store",
        out_shape=(
            jax.ShapeDtypeStruct((seqs, tok, share), BF16),
            jax.ShapeDtypeStruct(state_in.shape, F32),
        ),
        in_specs=[vmem, vmem],
        out_specs=(hbm, hbm),
        scratch_shapes=[pltpu.VMEM((seqs, tok, share), BF16), dma((4 * layers + 1,))],
        compiler_params=pltpu.CompilerParams(vmem_limit_bytes=2 * 2**20),
    )(y, new_state)


def solution(mesh):
    in_specs = (
        P("grp", None, None),
        P(None, "grp", None, "tp", None),
        P(),
        P(None, None, "tp"),
        P(None, None, "tp"),
        P(None, None, None, "tp"),
        P(None, None, None, "tp"),
        P(None, None, "tp"),
        P(None, None, "tp", None),
    )
    out_specs = (P("grp", None, "tp"), P(None, "grp", None, "tp", None))
    return jax.shard_map(local, mesh=mesh, in_specs=in_specs, out_specs=out_specs, check_vma=False)
```
